256 devices in a mesh: sp: 64 (over z, x, core), tp: 4 (over y).
Axes of the slice: x: 4, y: 4, z: 8, core: 2. Of those that a mesh axis runs over, the one named last changes fastest.
Arguments:
- stream: bfloat16 [32768, 2048], P(('sp', 'tp')), may hold values from -6 to 6
- queries: bfloat16 [32768, 512], P('sp', 'tp'), may hold values from -6 to 6
- key_rows: bfloat16 [32768, 512], P('sp', 'tp'), may hold values from -6 to 6
- values: bfloat16 [32768, 1024], P('sp', 'tp'), may hold values from -6 to 6
- out_gate: bfloat16 [32768, 1024], P('sp', 'tp'), may hold values from -6 to 6
- fwd_decay: float32 [32768, 512], P('sp', 'tp'), may hold values from -14 to 14
- bwd_decay: float32 [32768, 512], P('sp', 'tp'), may hold values from -14 to 14
- head_gain: float32 [1024], P('tp'), may hold values from 0.1 to 1.9
- out_proj: bfloat16 [1024, 2048], replicated, may hold values from -0.1875 to 0.1875
- mix_gain: float32 [2048], replicated, may hold values from 0.1 to 1.9
- ffn_gain: float32 [2048], replicated, may hold values from 0.1 to 1.9
- moe_gain: float32 [2048], replicated, may hold values from 0.1 to 1.9
- routes: int32 [32768, 2], P(('sp', 'tp')), may hold values from 0 to 63, all different within a row; in each aligned block of 128 rows (0 to 127, 128 to 255, ...) at most 6 rows name the same one
- route_weight: float32 [32768, 2], P(('sp', 'tp')), may hold values from 0.25 to 2.5
- expert_gate: bfloat16 [64, 2048, 1024], P('sp', None, 'tp'), may hold values from -0.125 to 0.125
- expert_up: bfloat16 [64, 2048, 1024], P('sp', None, 'tp'), may hold values from -0.125 to 0.125
- expert_down: bfloat16 [64, 1024, 2048], P('sp', 'tp'), may hold values from -0.1875 to 0.1875
- shared_gate: bfloat16 [2048, 512], P(None, 'tp'), may hold values from -0.125 to 0.125
- shared_up: bfloat16 [2048, 512], P(None, 'tp'), may hold values from -0.125 to 0.125
- shared_down: bfloat16 [512, 2048], P('tp'), may hold values from -0.25 to 0.25
Outputs:
- updated: bfloat16 [32768, 2048], P(('sp', 'tp'))
The draws below stay inside these ranges and needn't reach their ends.
Inputs may be any that keep to these rules, and one draw needn't show every extreme that they name: `routes`: each row names 2 different experts. Among the rows of one device no expert is named more than 6 times, and in every draw some device names some expert exactly 6 times.
All inputs are finite; a program needn't handle non-finite values.
Results may differ from the reference program's by a relative error of at most 0.023.
Values may be sent and summed in bfloat16 or wider, within the bound.
A program may use at most 128 MiB of HBM per device.

```python
import math
import jax
import jax.numpy as jnp
import numpy as np
from jax import lax

D = 2048
HEAD_TOTAL = 8
KEY_CHANNELS = 64
DV = 128
BLK = 64
FE = 1024
SH = 512
TOPK = 2
TOK_DEV = 128
TOKEN_COUNT = 32768
HV = 1024
EXPERTS = 64
CAP = 6
PARTS_SIZE = 4


def decay_law(key):
    head_key, chan_key, dev_key, jitter_key, position_key, fraction_key = jax.random.split(key, 6)
    slow_share = 0.5
    slow_heads = jax.random.uniform(head_key, (HEAD_TOTAL,)) < slow_share
    head_rate = jnp.where(slow_heads, 0.6 / TOKEN_COUNT, 2.5 / BLK)
    channel_rate = jnp.repeat(head_rate, KEY_CHANNELS) * jnp.exp(jax.random.uniform(chan_key, (HEAD_TOTAL * KEY_CHANNELS,), minval=-0.5, maxval=0.5))
    device_factor = jnp.exp(jax.random.uniform(dev_key, (TOKEN_COUNT // TOK_DEV, 1), minval=-0.7, maxval=0.7))
    rates = jnp.repeat(device_factor, TOK_DEV, axis=0) * channel_rate[None, :]
    preactivation = -jnp.log(jnp.expm1(16.0 * rates))
    preactivation = preactivation + jax.random.uniform(jitter_key, (TOKEN_COUNT, HEAD_TOTAL * KEY_CHANNELS), minval=-1.0, maxval=1.0)
    spike_rows = jax.random.randint(position_key, (2,), 0, TOKEN_COUNT)
    spike_fraction = jax.random.uniform(fraction_key, (2, HEAD_TOTAL * KEY_CHANNELS), minval=0.2, maxval=0.5)
    spike_preactivation = -jnp.log(jnp.expm1(-16.0 * jnp.log(1.0 - spike_fraction)))
    preactivation = preactivation.at[spike_rows].set(spike_preactivation)
    return jnp.clip(preactivation, -14.0, 14.0).astype(jnp.float32)


def draw_fwd_decay(key, part):
    return decay_law(jax.random.fold_in(key, 11))


def draw_bwd_decay(key, part):
    return decay_law(jax.random.fold_in(key, 23))


def levels(own_key, dims, cuts, low, high):
    gain = 1.0
    for dim, blocks in cuts:
        draws = jax.random.uniform(jax.random.fold_in(jax.random.fold_in(own_key, 6), dim), (blocks,), jnp.float32, low / len(cuts), high / len(cuts))
        gain = gain * jnp.repeat(jnp.exp(draws), dims[dim] // blocks).reshape((-1,) + (1,) * (len(dims) - 1 - dim))
    return gain


def deal_out(key, own, number, rows, amount, top, most, lean):
    sequence = jax.random.permutation(key, amount)
    heavy_load, ordinary = portions_of(amount, rows * top, most, lean, True), portions_of(amount, rows * top, most, lean, False)
    places = jnp.arange(amount)

    def named(tallies, rotation):
        used = int((tallies > 0).sum())
        fixed = max(1, used // 4)
        shifted = fixed + (places - fixed + rotation * (used - fixed)) % max(1, amount - fixed)
        return jnp.zeros((amount,), jnp.int32).at[sequence[jnp.where(places < fixed, places, shifted)]].set(jnp.asarray(tallies, jnp.int32))

    tallies = jnp.where(number % 4 == 0, named(heavy_load, number // 4), named(ordinary, number - number // 4 - 1))
    mixed = jax.random.permutation(jax.random.fold_in(own, 3), amount)
    giver, taker = mixed[0:amount // 2 * 2:2], mixed[1:amount // 2 * 2:2]
    room = jnp.minimum(tallies[giver] - 1, most - tallies[taker]) // 2
    room = jnp.where((giver == sequence[0]) | (taker == sequence[0]) | (tallies[taker] == 0), 0, jnp.maximum(room, 0))
    shifted = jax.random.randint(jax.random.fold_in(own, 4), (amount // 2,), 0, 1 << 20) % (room + 1)
    tallies = tallies.at[giver].add(-shifted).at[taker].add(shifted)
    members = jnp.searchsorted(jnp.cumsum(tallies), jnp.arange(rows * top), side="right").astype(jnp.int32)
    listing = members.reshape(top, rows).T
    listing = listing[jax.random.permutation(jax.random.fold_in(own, 1), rows)]
    rotation = jax.random.randint(jax.random.fold_in(own, 2), (rows, 1), 0, top)
    return jnp.take_along_axis(listing, (jnp.arange(top)[None, :] + rotation) % top, axis=1)


def portions_of(count, total, reach, skew, full):
    weights = [(1 << 20) // math.isqrt(standing ** skew) + 1 for standing in range(1, count + 1)]
    largest = reach if full else min(reach, max(-(-total // count), total * weights[0] // sum(weights)))
    least = 1 if total - largest >= count - 1 else 0
    given, surplus = [largest] + [least] * (count - 1), total - largest - least * (count - 1)
    while surplus > 0:
        free = [i for i in range(1, count) if given[i] < largest] or [i for i in range(1, count) if given[i] < reach]
        mass, left = sum([weights[i] for i in free]), surplus
        for i in free:
            extra = min(reach - given[i], max(1, left * weights[i] // mass), surplus)
            given[i] = given[i] + extra
            surplus = surplus - extra
    return np.array(given)


def bell_draw(own_key, dims, width, most, cuts=(), kind=jnp.bfloat16):
    drawn = jax.random.normal(own_key, dims, jnp.float32) * width
    if len(cuts) > 0:
        drawn = levels(own_key, dims, cuts, -0.22, 0.18) * drawn
    return jnp.clip(drawn, min=-most, max=most).astype(kind)


def setup_inputs(seed: int = 0) -> dict:
    arg_keys = jax.random.split(jax.random.key(seed), 21)
    stream = bell_draw(arg_keys[0], (TOKEN_COUNT, D), 1.0, 6.0, ((0, 256),))
    queries = bell_draw(arg_keys[1], (TOKEN_COUNT, HEAD_TOTAL * KEY_CHANNELS), 1.0, 6.0, ((0, 64), (1, 4)))
    key_rows = bell_draw(arg_keys[2], (TOKEN_COUNT, HEAD_TOTAL * KEY_CHANNELS), 1.0, 6.0, ((0, 64), (1, 4)))
    values = bell_draw(arg_keys[3], (TOKEN_COUNT, HV), 1.0, 6.0, ((0, 64), (1, 4)))
    out_gate = bell_draw(arg_keys[4], (TOKEN_COUNT, HV), 1.0, 6.0, ((0, 64), (1, 4)))
    fwd_decay = draw_fwd_decay(jax.random.fold_in(arg_keys[20], 71), 0)
    bwd_decay = draw_bwd_decay(jax.random.fold_in(arg_keys[20], 71), 0)
    head_gain = jnp.clip(1.0 + 0.18 * jax.random.normal(arg_keys[7], (HV,), jnp.float32), 0.1, 1.9)
    out_proj = bell_draw(arg_keys[8], (HV, D), HV ** -0.5, 0.1875)
    mix_gain = jnp.clip(1.0 + 0.18 * jax.random.normal(arg_keys[9], (D,), jnp.float32), 0.1, 1.9)
    ffn_gain = jnp.clip(1.0 + 0.18 * jax.random.normal(arg_keys[10], (D,), jnp.float32), 0.1, 1.9)
    moe_gain = jnp.clip(1.0 + 0.18 * jax.random.normal(arg_keys[11], (D,), jnp.float32), 0.1, 1.9)
    routes_keys = jax.random.split(jax.random.fold_in(arg_keys[12], 1), TOKEN_COUNT // TOK_DEV)
    routes_turns = jax.random.permutation(jax.random.fold_in(arg_keys[12], 3), TOKEN_COUNT // TOK_DEV)
    routes = jax.vmap(lambda own, number: deal_out(jax.random.fold_in(arg_keys[12], 2), own, number, TOK_DEV, EXPERTS, TOPK, CAP, 1))(routes_keys, routes_turns).reshape((TOKEN_COUNT, TOPK))
    route_weight = jnp.clip(jnp.exp(math.log(2.5) - 2.3025851 * jax.random.uniform(arg_keys[13], (TOKEN_COUNT, TOPK), jnp.float32) ** levels(arg_keys[13], (TOKEN_COUNT, TOPK), ((0, 256),), -0.2, 0.2)), 0.25, 2.5)
    expert_gate = bell_draw(arg_keys[14], (EXPERTS, D, FE), D ** -0.5, 0.125, ((0, 64), (2, 4)))
    expert_up = bell_draw(arg_keys[15], (EXPERTS, D, FE), D ** -0.5, 0.125, ((0, 64), (2, 4)))
    expert_down = bell_draw(arg_keys[16], (EXPERTS, FE, D), FE ** -0.5, 0.1875, ((0, 64), (1, 4)))
    shared_gate = bell_draw(arg_keys[17], (D, SH), D ** -0.5, 0.125, ((1, 4),))
    shared_up = bell_draw(arg_keys[18], (D, SH), D ** -0.5, 0.125, ((1, 4),))
    shared_down = bell_draw(arg_keys[19], (SH, D), SH ** -0.5, 0.25, ((0, 4),))
    return {"stream": stream, "queries": queries, "key_rows": key_rows, "values": values, "out_gate": out_gate, "fwd_decay": fwd_decay, "bwd_decay": bwd_decay, "head_gain": head_gain, "out_proj": out_proj, "mix_gain": mix_gain, "ffn_gain": ffn_gain, "moe_gain": moe_gain, "routes": routes, "route_weight": route_weight, "expert_gate": expert_gate, "expert_up": expert_up, "expert_down": expert_down, "shared_gate": shared_gate, "shared_up": shared_up, "shared_down": shared_down}


EPS = 1e-06
GATE_NORM = 16.0
ROPE_BASE = 10000.0
TOP_PRECISION = lax.Precision.HIGHEST

def normalize(tensor):
    return tensor * lax.rsqrt(lax.optimization_barrier(jnp.mean(tensor * tensor, axis=-1, keepdims=True)) + EPS)

def rotate(tensor, positions):
    half_width = tensor.shape[-1] // 2
    frequency = ROPE_BASE ** (-jnp.arange(half_width, dtype=jnp.float32) / half_width)
    angles = positions[:, None] * frequency[None, :]
    cosine = jnp.cos(angles)[:, None, :]
    sine_part = jnp.sin(angles)[:, None, :]
    front_half = tensor[..., :half_width]
    back_half = tensor[..., half_width:]
    return jnp.concatenate([front_half * cosine - back_half * sine_part, front_half * sine_part + back_half * cosine], axis=-1)

def blockwise(query_rows, key_data, value_matrix, log_decay, start_state):
    length, head_count, key_width = query_rows.shape
    value_width = value_matrix.shape[-1]
    block_count = length // BLK
    query_blocks = query_rows.reshape(block_count, BLK, head_count, key_width)
    key_blocks = key_data.reshape(block_count, BLK, head_count, key_width)
    value_blocks = value_matrix.reshape(block_count, BLK, head_count, value_width)
    cumul = jnp.cumsum(log_decay.reshape(block_count, BLK, head_count, key_width), axis=1)
    middle = cumul[:, BLK // 2 - 1:BLK // 2]
    query_scaled = query_blocks * jnp.exp(cumul - middle)
    key_scaled = key_blocks * jnp.exp(middle - cumul)
    scores = jnp.einsum('nthk,nshk->nhts', query_scaled, key_scaled, precision=TOP_PRECISION)
    lower_mask = jnp.arange(BLK)[:, None] >= jnp.arange(BLK)[None, :]
    scores = jnp.where(lower_mask, scores, 0.0)
    within = jnp.einsum('nhts,nshv->nthv', scores, value_blocks, precision=TOP_PRECISION)
    last_cumul = cumul[:, -1:]
    query_in = query_blocks * jnp.exp(cumul)
    key_out = key_blocks * jnp.exp(last_cumul - cumul)
    block_decay = jnp.exp(last_cumul[:, 0])

    def advance(carried_state, pieces):
        query_segment, key_segment, value_segment, decay_segment = pieces
        across_blocks = jnp.einsum('asu,sun->asn', query_segment, carried_state, precision=TOP_PRECISION)
        carried_state = carried_state * decay_segment[:, :, None] + jnp.einsum('jco,jcm->com', key_segment, value_segment, precision=TOP_PRECISION)
        return (carried_state, across_blocks)
    final_state, across_blocks = lax.scan(advance, start_state, (query_in, key_out, value_blocks, block_decay))
    return ((within + across_blocks).reshape(length, head_count, value_width), final_state)

def reference(stream, queries, key_rows, values, out_gate, fwd_decay, bwd_decay, head_gain, out_proj, mix_gain, ffn_gain, moe_gain, routes, route_weight, expert_gate, expert_up, expert_down, shared_gate, shared_up, shared_down):
    positions = jnp.arange(TOKEN_COUNT, dtype=jnp.int32).astype(jnp.float32)
    query_rows = rotate(queries.astype(jnp.float32).reshape(TOKEN_COUNT, HEAD_TOTAL, KEY_CHANNELS) * KEY_CHANNELS ** (-0.5), positions)
    key_data = rotate(key_rows.astype(jnp.float32).reshape(TOKEN_COUNT, HEAD_TOTAL, KEY_CHANNELS), positions)
    value_matrix = values.astype(jnp.float32).reshape(TOKEN_COUNT, HEAD_TOTAL, DV)
    fwd_log = jax.nn.log_sigmoid(fwd_decay).reshape(TOKEN_COUNT, HEAD_TOTAL, KEY_CHANNELS) / GATE_NORM
    bwd_log = jax.nn.log_sigmoid(bwd_decay).reshape(TOKEN_COUNT, HEAD_TOTAL, KEY_CHANNELS) / GATE_NORM
    zero_state = jnp.zeros((HEAD_TOTAL, KEY_CHANNELS, DV), jnp.float32)
    fwd_out, _ = blockwise(query_rows, key_data, value_matrix, fwd_log, zero_state)
    bwd_out, _ = blockwise(query_rows[::-1], key_data[::-1], value_matrix[::-1], bwd_log[::-1], zero_state)
    combined = normalize(fwd_out + bwd_out[::-1]) * head_gain.reshape(HEAD_TOTAL, DV)
    mixed_out = (combined.reshape(TOKEN_COUNT, HV) * jax.nn.silu(out_gate.astype(jnp.float32))).astype(jnp.bfloat16)
    projected = jnp.dot(mixed_out, out_proj, preferred_element_type=jnp.float32)
    residual = (stream.astype(jnp.float32) + normalize(projected) * mix_gain).astype(jnp.bfloat16)
    normed = (normalize(residual.astype(jnp.float32)) * ffn_gain).astype(jnp.bfloat16)
    shared_hidden = (jax.nn.silu(jnp.dot(normed, shared_gate, preferred_element_type=jnp.float32)) * jnp.dot(normed, shared_up, preferred_element_type=jnp.float32)).astype(jnp.bfloat16)
    group_width = SH // PARTS_SIZE
    shared_out = jnp.zeros((TOKEN_COUNT, D), jnp.float32)
    for quarter in range(PARTS_SIZE):
        piece = jnp.dot(shared_hidden[:, quarter * group_width:(quarter + 1) * group_width], shared_down[quarter * group_width:(quarter + 1) * group_width], preferred_element_type=jnp.float32)
        shared_out = shared_out + lax.optimization_barrier(piece.astype(jnp.bfloat16)).astype(jnp.float32)
    row_block = 256
    flat_ids = routes.reshape(-1)
    grand_total = flat_ids.shape[0]
    token_index = jnp.arange(grand_total, dtype=jnp.int32) // TOPK
    sort_order = jnp.argsort(flat_ids, stable=True)
    sorted_expert = flat_ids[sort_order]
    sorted_token = token_index[sort_order]
    sorted_weight = route_weight.reshape(-1)[sort_order]
    counts = lax.optimization_barrier(jnp.sum((flat_ids[:, None] == jnp.arange(EXPERTS, dtype=jnp.int32)[None, :]).astype(jnp.int32), axis=0))
    starts = jnp.cumsum(counts) - counts
    padded = (counts + row_block - 1) // row_block * row_block
    block_ends = jnp.cumsum(padded)
    padded_starts = block_ends - padded
    position = (padded_starts[sorted_expert] + jnp.arange(grand_total, dtype=jnp.int32) - starts[sorted_expert]).astype(jnp.int32)
    block_total = -(-(grand_total + EXPERTS * (row_block - 1)) // row_block)
    slot_token = jnp.zeros((block_total * row_block,), jnp.int32).at[position].set(sorted_token)
    slot_weight = jnp.zeros((block_total * row_block,), jnp.float32).at[position].set(sorted_weight)
    block_expert = jnp.minimum(jnp.searchsorted(block_ends, jnp.arange(block_total, dtype=jnp.int32) * row_block, side='right'), EXPERTS - 1).astype(jnp.int32)
    expert_width = FE // PARTS_SIZE

    def add_block(totals, block_item):
        token_ids, slot_wts, expert = block_item
        row_data = normed[token_ids]
        gate_mat = lax.dynamic_index_in_dim(expert_gate, expert, 0, keepdims=False)
        up_mat = lax.dynamic_index_in_dim(expert_up, expert, 0, keepdims=False)
        down_mat = lax.dynamic_index_in_dim(expert_down, expert, 0, keepdims=False)
        hidden = (jax.nn.silu(jnp.dot(row_data, gate_mat, preferred_element_type=jnp.float32)) * jnp.dot(row_data, up_mat, preferred_element_type=jnp.float32)).astype(jnp.bfloat16)
        quarter_sums = jnp.einsum('rqf,qfd->qrd', hidden.astype(jnp.float32).reshape(row_block, PARTS_SIZE, expert_width), down_mat.astype(jnp.float32).reshape(PARTS_SIZE, expert_width, D), precision=TOP_PRECISION)
        rounded = lax.optimization_barrier(quarter_sums.astype(jnp.bfloat16)).astype(jnp.float32)
        result = lax.optimization_barrier(lax.optimization_barrier(jnp.sum(rounded, axis=0)).astype(jnp.bfloat16)).astype(jnp.float32)
        return (totals.at[token_ids].add(result * slot_wts[:, None]), None)
    routed_sum, _ = lax.scan(add_block, jnp.zeros((TOKEN_COUNT, D), jnp.float32), (slot_token.reshape(block_total, row_block), slot_weight.reshape(block_total, row_block), block_expert))
    mixture = shared_out + routed_sum
    return (residual.astype(jnp.float32) + normalize(mixture) * moe_gain).astype(jnp.bfloat16)
```

```python
import functools

import jax
import jax.numpy as jnp
from jax import lax
from jax.experimental import pallas as pl
from jax.experimental.pallas import tpu as pltpu
from jax.sharding import PartitionSpec as P

KEY_CHANNELS = 64
DV = 128
BLK = 64
TOPK = 2
PLANE = 8


EPS = 1e-06
GATE_NORM = 16.0
ROPE_BASE = 10000.0
TOP_PRECISION = lax.Precision.HIGHEST
MESH = pl.DeviceIdType.MESH


def normalize(tensor):
    return tensor * lax.rsqrt(jnp.mean(tensor * tensor, axis=-1, keepdims=True) + EPS)


def dot_nt(left, right):
    return lax.dot_general(
        left, right, (((1,), (1,)), ((), ())), preferred_element_type=jnp.float32
    )


def dot_tn(left, right):
    return lax.dot_general(
        left, right, (((0,), (0,)), ((), ())), preferred_element_type=jnp.float32
    )


def fused_kernel(
    sp_count,
    tp_count,
    q_ref,
    k_ref,
    v_ref,
    gate_ref,
    fwd_ref,
    bwd_ref,
    cos_ref,
    sin_ref,
    gain_ref,
    stream_ref,
    mix_gain_ref,
    ffn_gain_ref,
    moe_gain_ref,
    slot_ref,
    weight_ref,
    proj_hbm,
    eg_hbm,
    eu_hbm,
    ed_hbm,
    gu_hbm,
    sd_hbm,
    out_ref,
    mixed_ref,
    land_ref,
    within_ref,
    key_ref,
    sums_f,
    sums_b,
    near_out,
    near_in,
    far_out,
    far_in,
    carry_out,
    carry_in,
    proj_w,
    gate_w,
    up_w,
    down_w,
    gu_w,
    sd_w,
    resid_ref,
    normed_ref,
    outgoing_ref,
    arrived_ref,
    rows_ref,
    hidden_ref,
    done_ref,
    back_ref,
    pair_in,
    part_out,
    part_in,
    local_sem,
    near_send,
    near_recv,
    far_send,
    far_recv,
    carry_send,
    carry_recv,
    row_send,
    row_recv,
    own_send,
    own_recv,
    relay_send,
    relay_recv,
    sh_send,
    sh_recv,
    shr_send,
    shr_recv,
    block_send,
    block_recv,
    back_send,
    back_recv,
    pair_send,
    pair_recv,
):
    span, lanes = q_ref.shape
    width = v_ref.shape[1]
    heads = lanes // KEY_CHANNELS
    blocks = span // BLK
    rows_out = span // tp_count
    planes = sp_count // PLANE
    piece = DV // PLANE
    model = stream_ref.shape[1]
    quarter = model // 4
    units = eg_hbm.shape[2]
    depth = eg_hbm.shape[1]
    sp_me = lax.axis_index("sp")
    tp_me = lax.axis_index("tp")
    z_me = sp_me // PLANE
    p_me = lax.rem(sp_me, PLANE)
    pair = sp_me + 1 - 2 * lax.rem(sp_me, 2)
    up_y = lax.rem(tp_me + 1, tp_count)
    down_y = lax.rem(tp_me + tp_count - 1, tp_count)
    far_y = lax.rem(tp_me + 2, tp_count)

    barrier = pltpu.get_barrier_semaphore()
    for step in range(1, sp_count):
        pl.semaphore_signal(
            barrier,
            inc=1,
            device_id=(lax.rem(sp_me + step, sp_count), tp_me),
            device_id_type=MESH,
        )
    for step in range(1, tp_count):
        pl.semaphore_signal(
            barrier,
            inc=1,
            device_id=(sp_me, lax.rem(tp_me + step, tp_count)),
            device_id_type=MESH,
        )

    def remote(source, target, send, recv, device):
        copy = pltpu.make_async_remote_copy(
            src_ref=source,
            dst_ref=target,
            send_sem=send,
            recv_sem=recv,
            device_id=device,
            device_id_type=MESH,
        )
        copy.start()
        return copy

    own_cut = pl.ds(pl.multiple_of(tp_me * units, units), units)
    sd_rows = sd_hbm.shape[0]
    sd_cut = pl.ds(pl.multiple_of(tp_me * sd_rows, sd_rows), sd_rows)
    local = []
    for index, (source, target) in enumerate(
        (
            (proj_hbm, proj_w),
            (eg_hbm.at[0], gate_w.at[tp_me]),
            (eu_hbm.at[0], up_w.at[tp_me]),
            (ed_hbm.at[0], down_w.at[own_cut]),
            (gu_hbm, gu_w.at[tp_me]),
            (sd_hbm, sd_w.at[sd_cut]),
        )
    ):
        copy = pltpu.make_async_copy(source, target, local_sem.at[index])
        copy.start()
        local.append(copy)

    row = lax.broadcasted_iota(jnp.int32, (BLK, BLK), 0)
    column = lax.broadcasted_iota(jnp.int32, (BLK, BLK), 1)
    lower = row >= column
    upper = row <= column
    lower_ones = lower.astype(jnp.float32)
    upper_ones = upper.astype(jnp.float32)
    from_lane = lax.broadcasted_iota(jnp.int32, (lanes, lanes), 0)
    to_lane = lax.broadcasted_iota(jnp.int32, (lanes, lanes), 1)
    half = KEY_CHANNELS // 2
    partner = jnp.where(lax.rem(to_lane, KEY_CHANNELS) < half, to_lane + half, to_lane - half)
    swap = (from_lane == partner).astype(jnp.bfloat16)
    own_head = (
        lax.broadcasted_iota(jnp.int32, (width, lanes), 0) // DV
        == lax.broadcasted_iota(jnp.int32, (width, lanes), 1) // KEY_CHANNELS
    )
    lane_head = lax.broadcasted_iota(jnp.int32, (BLK, lanes), 1) // KEY_CHANNELS

    def rotated(tensor, rows):
        swapped = jnp.dot(tensor, swap, preferred_element_type=jnp.float32)
        return tensor.astype(jnp.float32) * cos_ref[rows, :] + swapped * sin_ref[rows, :]

    pl.semaphore_wait(barrier, sp_count - 1 + tp_count - 1)
    ups, downs = (sp_me, up_y), (sp_me, down_y)
    own_copies = []

    def send_own(item):
        middle = depth // 2
        parts = (
            (eg_hbm.at[0], gate_w.at[tp_me]),
            (eu_hbm.at[0, pl.ds(0, middle)], up_w.at[tp_me, pl.ds(0, middle)]),
            (eu_hbm.at[0, pl.ds(middle, middle)], up_w.at[tp_me, pl.ds(middle, middle)]),
            (ed_hbm.at[0], down_w.at[own_cut]),
        )
        source, target = parts[item]
        own_copies.append(
            tuple(
                remote(source, target, own_send.at[way, item], own_recv.at[way, item], device)
                for way, device in enumerate((ups, downs))
            )
        )

    send_own(0)
    send_own(1)

    cumul_f, cumul_b, decay_f, decay_b = [], [], [], []
    for block in range(blocks):
        rows = pl.ds(block * BLK, BLK)
        total_f = jnp.dot(
            lower_ones, fwd_ref[rows, :], precision=TOP_PRECISION, preferred_element_type=jnp.float32
        )
        total_b = jnp.dot(
            upper_ones, bwd_ref[rows, :], precision=TOP_PRECISION, preferred_element_type=jnp.float32
        )
        last_f = total_f[BLK - 1 : BLK]
        last_b = total_b[0:1]
        keys = rotated(k_ref[rows, :], rows)
        key_ref[rows, :] = keys
        value_rows = v_ref[rows, :]
        out_f = (keys * jnp.exp(last_f - total_f)).astype(jnp.bfloat16)
        out_b = (keys * jnp.exp(last_b - total_b)).astype(jnp.bfloat16)
        sums_f[block] = jnp.where(own_head, dot_tn(value_rows, out_f), 0.0)
        sums_b[block] = jnp.where(own_head, dot_tn(value_rows, out_b), 0.0)
        cumul_f.append(total_f)
        cumul_b.append(total_b)
        decay_f.append(jnp.exp(last_f))
        decay_b.append(jnp.exp(last_b))

    def packed(total):
        return sum(total[h * DV : (h + 1) * DV] for h in range(heads))

    total = sums_f[0]
    through_f = decay_f[0]
    for block in range(1, blocks):
        total = total * decay_f[block] + sums_f[block]
        through_f = through_f * decay_f[block]
    state_f = packed(total)
    total = sums_b[blocks - 1]
    through_b = decay_b[blocks - 1]
    for block in range(blocks - 2, -1, -1):
        total = total * decay_b[block] + sums_b[block]
        through_b = through_b * decay_b[block]
    state_b = packed(total)

    def put_state(ref, first, second, through_first, through_second):
        ref[0:piece] = first
        ref[piece : 2 * piece] = second
        ref[2 * piece : 2 * piece + 8] = jnp.concatenate(
            [
                jnp.broadcast_to(through_first, (4, lanes)),
                jnp.broadcast_to(through_second, (4, lanes)),
            ],
            axis=0,
        )

    for p in range(PLANE):
        cut = slice(p * piece, (p + 1) * piece)
        put_state(near_out.at[p], state_f[cut], state_b[cut], through_f, through_b)
    near_copies = []
    for step in range(1, PLANE):
        target = lax.rem(p_me + step, PLANE)
        near_copies.append(
            remote(
                near_out.at[target],
                near_in.at[p_me],
                near_send.at[step],
                near_recv.at[step],
                (z_me * PLANE + target, tp_me),
            )
        )
    near_in[p_me] = near_out[p_me]

    query_f, query_b = [], []

    def within(block):
        rows = pl.ds(block * BLK, BLK)
        queries = rotated(q_ref[rows, :], rows) * KEY_CHANNELS ** (-0.5)
        keys = key_ref[rows, :]
        total_f, total_b = cumul_f[block], cumul_b[block]
        middle_f = total_f[BLK // 2 - 1 : BLK // 2]
        middle_b = total_b[BLK // 2 : BLK // 2 + 1]
        scaled_qf = queries * jnp.exp(total_f - middle_f)
        scaled_qb = queries * jnp.exp(total_b - middle_b)
        scaled_kf = (keys * jnp.exp(middle_f - total_f)).astype(jnp.bfloat16)
        scaled_kb = (keys * jnp.exp(middle_b - total_b)).astype(jnp.bfloat16)
        query_f.append((queries * jnp.exp(total_f)).astype(jnp.bfloat16))
        query_b.append((queries * jnp.exp(total_b)).astype(jnp.bfloat16))
        for h in range(heads):
            mine = lane_head == h
            scores_f = dot_nt(jnp.where(mine, scaled_qf, 0.0).astype(jnp.bfloat16), scaled_kf)
            scores_b = dot_nt(jnp.where(mine, scaled_qb, 0.0).astype(jnp.bfloat16), scaled_kb)
            scores = jnp.where(lower, scores_f, 0.0) + jnp.where(upper, scores_b, 0.0)
            within_ref[rows, h * DV : (h + 1) * DV] = jnp.dot(
                scores.astype(jnp.bfloat16),
                v_ref[rows, h * DV : (h + 1) * DV],
                preferred_element_type=jnp.float32,
            )

    third = blocks // 3
    for block in range(third):
        within(block)
    for copy in near_copies:
        copy.wait()

    def near(p):
        return (
            near_in[p, 0:piece],
            near_in[p, piece : 2 * piece],
            near_in[p, 2 * piece : 2 * piece + 1],
            near_in[p, 2 * piece + 4 : 2 * piece + 5],
        )

    def fold(orders, visit):
        state = jnp.zeros((piece, lanes), jnp.float32)
        through = jnp.ones((1, lanes), jnp.float32)
        first = orders[0] == 0
        for p in orders:
            visit(p, state, through)
            fwd_state, bwd_state, fwd_through, bwd_through = near(p)
            state = state * (fwd_through if first else bwd_through) + (
                fwd_state if first else bwd_state
            )
            through = through * (fwd_through if first else bwd_through)
        return state, through

    ahead = list(range(PLANE))
    behind = ahead[::-1]
    plane_f, plane_df = fold(ahead, lambda p, state, through: None)
    plane_b, plane_db = fold(behind, lambda p, state, through: None)
    put_state(far_out, plane_f, plane_b, plane_df, plane_db)
    far_copies = []
    for step in range(1, planes):
        target = lax.rem(z_me + step, planes)
        far_copies.append(
            remote(
                far_out,
                far_in.at[z_me],
                far_send.at[step],
                far_recv.at[step],
                (target * PLANE + p_me, tp_me),
            )
        )
    far_in[z_me] = far_out[...]
    for block in range(third, blocks - third):
        within(block)
    for copy in far_copies:
        copy.wait()
    enter_f = jnp.zeros((piece, lanes), jnp.float32)
    enter_b = jnp.zeros((piece, lanes), jnp.float32)
    for z in range(planes):
        step_f = enter_f * far_in[z, 2 * piece : 2 * piece + 1] + far_in[z, 0:piece]
        enter_f = jnp.where(z < z_me, step_f, enter_f)
    for z in range(planes - 1, -1, -1):
        step_b = enter_b * far_in[z, 2 * piece + 4 : 2 * piece + 5] + far_in[z, piece : 2 * piece]
        enter_b = jnp.where(z > z_me, step_b, enter_b)

    def emit_f(p, state, through):
        carry_out[p, 0:piece] = enter_f * through + state

    def emit_b(p, state, through):
        carry_out[p, piece : 2 * piece] = enter_b * through + state

    fold(ahead, emit_f)
    fold(behind, emit_b)
    carry_copies = []
    for step in range(1, PLANE):
        target = lax.rem(p_me + step, PLANE)
        carry_copies.append(
            remote(
                carry_out.at[target],
                carry_in.at[p_me],
                carry_send.at[step],
                carry_recv.at[step],
                (z_me * PLANE + target, tp_me),
            )
        )
    carry_in[p_me] = carry_out[p_me]
    for block in range(blocks - third, blocks):
        within(block)
    for copy in carry_copies:
        copy.wait()

    def unpacked(first):
        carry = jnp.concatenate([carry_in[p, first : first + piece] for p in range(PLANE)], axis=0)
        return jnp.where(own_head, jnp.concatenate([carry] * heads, axis=0), 0.0)

    state = unpacked(0)
    for block in range(blocks):
        rows = pl.ds(block * BLK, BLK)
        within_ref[rows, :] += dot_nt(query_f[block], state.astype(jnp.bfloat16))
        if block < blocks - 1:
            state = state * decay_f[block] + sums_f[block]
    state = unpacked(piece)
    for block in range(blocks - 1, -1, -1):
        rows = pl.ds(block * BLK, BLK)
        attended = within_ref[rows, :] + dot_nt(query_b[block], state.astype(jnp.bfloat16))
        if block > 0:
            state = state * decay_b[block] + sums_b[block]
        for h in range(heads):
            part = attended[:, h * DV : (h + 1) * DV]
            square = jnp.mean(part * part, axis=-1, keepdims=True)
            gate = gate_ref[rows, h * DV : (h + 1) * DV].astype(jnp.float32)
            mixed_ref[rows, h * DV : (h + 1) * DV] = (
                part
                * lax.rsqrt(square + EPS)
                * gain_ref[:, h * DV : (h + 1) * DV]
                * (gate / (1.0 + jnp.exp(-gate)))
            ).astype(jnp.bfloat16)

    row_copies = []
    for step in range(1, tp_count):
        target = lax.rem(tp_me + step, tp_count)
        row_copies.append(
            remote(
                mixed_ref.at[pl.ds(pl.multiple_of(target * rows_out, rows_out), rows_out)],
                land_ref.at[tp_me],
                row_send.at[step],
                row_recv.at[step],
                (sp_me, target),
            )
        )
    send_own(2)
    send_own(3)
    land_ref[tp_me] = mixed_ref[pl.ds(pl.multiple_of(tp_me * rows_out, rows_out), rows_out), :]

    slot_lane = lax.broadcasted_iota(jnp.int32, (rows_out, sp_count * 8), 1)
    mains = [slot_ref[:, k : k + 1] == slot_lane for k in range(TOPK)]
    tails = [slot_ref[:, TOPK + k : TOPK + k + 1] == slot_lane for k in range(TOPK)]

    def tail_hit(k, b):
        return jnp.logical_and(tails[k], slot_ref[:, 2 * TOPK + k : 2 * TOPK + k + 1] == b)

    def chosen(first, second):
        return jnp.where(jnp.logical_or(first, second), 1.0, 0.0).astype(jnp.bfloat16)

    local[0].wait()
    for copy in row_copies:
        copy.wait()
    mixed_all = jnp.concatenate([land_ref[source] for source in range(tp_count)], axis=1)
    projected = jnp.dot(mixed_all, proj_w[...], preferred_element_type=jnp.float32)
    residual = (
        stream_ref[...].astype(jnp.float32) + normalize(projected) * mix_gain_ref[...]
    ).astype(jnp.bfloat16)
    resid_ref[...] = residual
    normed = (normalize(residual.astype(jnp.float32)) * ffn_gain_ref[...]).astype(jnp.bfloat16)
    normed_ref[...] = normed
    pick_main = chosen(mains[0], mains[1])
    for b in range(3):
        picks = jnp.concatenate([pick_main, chosen(tail_hit(0, b), tail_hit(1, b))], axis=0)
        source = jnp.concatenate(
            [normed[:, b * quarter : (b + 1) * quarter], normed[:, 3 * quarter :]], axis=0
        )
        outgoing_ref[:, :, b * quarter : (b + 1) * quarter] = (
            dot_tn(picks, source).reshape(sp_count, 8, quarter).astype(jnp.bfloat16)
        )
    block_copies = []
    for step in range(1, sp_count):
        target = lax.rem(sp_me + step, sp_count)
        block_copies.append(
            remote(
                outgoing_ref.at[target],
                arrived_ref.at[sp_me],
                block_send.at[step],
                block_recv.at[step],
                (target, tp_me),
            )
        )
    arrived_ref[sp_me] = outgoing_ref[sp_me]
    pair_copy = remote(normed_ref, pair_in, pair_send.at[0], pair_recv.at[0], (pair, tp_me))

    relay_copies = []
    middle = depth // 2
    middle_units = units // 2

    def relay_rows(item, slot, way):
        if item < 2:
            ref = (gate_w, up_w)[item]
            return ref.at[slot, pl.ds(way * middle, middle)]
        start = pl.multiple_of(slot * units + way * middle_units, middle_units)
        return down_w.at[pl.ds(start, middle_units)]

    for item in range(3):
        for index in ((0,), (1, 2), (3,))[item]:
            for copy in own_copies[index]:
                copy.wait()
        for way, (slot, device) in enumerate(((down_y, ups), (up_y, downs))):
            ref = relay_rows(item, slot, way)
            relay_copies.append(
                remote(ref, ref, relay_send.at[way, item], relay_recv.at[way, item], device)
            )
    sh_copies = []
    local[4].wait()
    local[5].wait()
    for way, device in enumerate((ups, downs)):
        ref = gu_w.at[tp_me]
        sh_copies.append(remote(ref, ref, sh_send.at[way, 0], sh_recv.at[way, 0], device))
        ref = sd_w.at[sd_cut]
        sh_copies.append(remote(ref, ref, sh_send.at[way, 1], sh_recv.at[way, 1], device))
    for index in (1, 2, 3):
        local[index].wait()

    group = 128
    spot = lax.broadcasted_iota(jnp.int32, (group, group), 0)
    origin = lax.broadcasted_iota(jnp.int32, (group, group), 1)
    same = spot // 8 == origin // 8

    def spread(target, source, b):
        rank = lax.rem(target, 8)
        hit = jnp.logical_and(rank < 6, lax.rem(rank, 3) == b)
        hit = jnp.logical_and(hit, lax.rem(source, 8) == 6 + rank // 3)
        return jnp.where(jnp.logical_and(same, hit), 1.0, 0.0).astype(jnp.bfloat16)

    for copy in block_copies:
        copy.wait()
    for part in range(sp_count * 8 // group):
        cut = slice(part * group, (part + 1) * group)
        tail = jnp.zeros((group, quarter), jnp.float32)
        for b in range(3):
            block = arrived_ref[
                part * group // 8 : (part + 1) * group // 8, :, b * quarter : (b + 1) * quarter
            ].reshape(group, quarter)
            rows_ref[cut, b * quarter : (b + 1) * quarter] = block
            tail = tail + jnp.dot(
                spread(spot, origin, b), block, preferred_element_type=jnp.float32
            )
        rows_ref[cut, 3 * quarter :] = tail.astype(jnp.bfloat16)

    def hidden_of(slot):
        hidden_ref[:, pl.ds(pl.multiple_of(slot * units, units), units)] = (
            jax.nn.silu(jnp.dot(rows_ref[...], gate_w[slot], preferred_element_type=jnp.float32))
            * jnp.dot(rows_ref[...], up_w[slot], preferred_element_type=jnp.float32)
        ).astype(jnp.bfloat16)

    hidden_of(tp_me)
    hidden_of(down_y)
    hidden_of(up_y)
    for copy in relay_copies:
        copy.wait()
    hidden_of(far_y)
    last = jnp.dot(
        hidden_ref[...], down_w[:, 3 * quarter :], preferred_element_type=jnp.float32
    ).astype(jnp.bfloat16)
    keep = lax.rem(lax.broadcasted_iota(jnp.int32, (sp_count * 8, quarter), 0), 8) < 6
    for b in range(3):
        value = jnp.dot(
            hidden_ref[...],
            down_w[:, b * quarter : (b + 1) * quarter],
            preferred_element_type=jnp.float32,
        )
        gather = spread(origin, spot, b)
        moved = jnp.concatenate(
            [
                jnp.dot(
                    gather,
                    last[part * group : (part + 1) * group],
                    preferred_element_type=jnp.float32,
                )
                for part in range(sp_count * 8 // group)
            ],
            axis=0,
        )
        done_ref[:, :, b * quarter : (b + 1) * quarter] = (
            jnp.where(keep, value, moved).reshape(sp_count, 8, quarter).astype(jnp.bfloat16)
        )
    back_copies = []
    for step in range(1, sp_count):
        target = lax.rem(sp_me + step, sp_count)
        back_copies.append(
            remote(
                done_ref.at[target],
                back_ref.at[sp_me],
                back_send.at[step],
                back_recv.at[step],
                (target, tp_me),
            )
        )
    back_ref[sp_me] = done_ref[sp_me]

    for copy in sh_copies:
        copy.wait()
    shr_copies = []
    for way, (slot, device) in enumerate(((down_y, ups), (up_y, downs))):
        ref = gu_w.at[slot, pl.ds(way * middle, middle)]
        shr_copies.append(remote(ref, ref, shr_send.at[way, 0], shr_recv.at[way, 0], device))
        start = pl.multiple_of(slot * sd_rows + way * (sd_rows // 2), sd_rows // 2)
        ref = sd_w.at[pl.ds(start, sd_rows // 2)]
        shr_copies.append(remote(ref, ref, shr_send.at[way, 1], shr_recv.at[way, 1], device))
    pair_copy.wait()
    for copy in shr_copies:
        copy.wait()
    tokens = jnp.concatenate([normed_ref[...], pair_in[...]], axis=0)
    lane = lax.broadcasted_iota(jnp.int32, (2 * rows_out, 2 * sd_rows), 1)
    units_of = []
    for slot in range(tp_count):
        both = jnp.dot(tokens, gu_w[slot], preferred_element_type=jnp.float32)
        units_of.append(jax.nn.silu(both) * pltpu.roll(both, sd_rows, 1))
    hidden = jnp.concatenate(
        [
            jnp.where(lane < sd_rows, units_of[s], pltpu.roll(units_of[s + 1], sd_rows, 1))
            for s in range(0, tp_count, 2)
        ],
        axis=1,
    ).astype(jnp.bfloat16)
    part_out[...] = jnp.dot(
        hidden[rows_out:], sd_w[...], preferred_element_type=jnp.float32
    ).astype(jnp.bfloat16)
    part_copy = remote(part_out, part_in, pair_send.at[1], pair_recv.at[1], (pair, tp_me))
    shared = jnp.dot(hidden[:rows_out], sd_w[...], preferred_element_type=jnp.float32)

    weights = [weight_ref[:, k : k + 1] for k in range(TOPK)]

    def split(hits):
        full = jnp.where(hits[0], weights[0], 0.0) + jnp.where(hits[1], weights[1], 0.0)
        high = full.astype(jnp.bfloat16)
        return [high, (full - high.astype(jnp.float32)).astype(jnp.bfloat16)]

    main_split = split(mains)
    sides = [
        jnp.concatenate(main_split + split([tail_hit(0, b), tail_hit(1, b)]), axis=0)
        for b in range(3)
    ]
    part_copy.wait()
    for copy in back_copies:
        copy.wait()
    shared = shared + part_in[...].astype(jnp.float32)
    pieces = []
    tail = jnp.zeros((rows_out, quarter), jnp.float32)
    for b in range(3):
        block = back_ref[:, :, b * quarter : (b + 1) * quarter].reshape(sp_count * 8, quarter)
        value = jnp.dot(sides[b], block, preferred_element_type=jnp.float32)
        pieces.append(value[0:rows_out] + value[rows_out : 2 * rows_out])
        tail = tail + value[2 * rows_out : 3 * rows_out] + value[3 * rows_out :]
    mixture = shared + jnp.concatenate(pieces + [tail], axis=1)
    square = jnp.mean(mixture * mixture, axis=-1, keepdims=True)
    out_ref[...] = (
        resid_ref[...].astype(jnp.float32)
        + mixture * lax.rsqrt(square + EPS) * moe_gain_ref[...]
    ).astype(out_ref.dtype)


def fused(vmem_args, hbm_args):
    sp_count = lax.axis_size("sp")
    tp_count = lax.axis_size("tp")
    queries, _, values = vmem_args[:3]
    stream = vmem_args[9]
    _, expert_gate, _, expert_down, pair_gate, pair_down = hbm_args
    span, lanes = queries.shape
    width = values.shape[1]
    rows_out = span // tp_count
    blocks = span // BLK
    planes = sp_count // PLANE
    piece = DV // PLANE
    model = stream.shape[1]
    units = expert_gate.shape[2]
    vmem = pl.BlockSpec(memory_space=pltpu.VMEM)
    hbm = pl.BlockSpec(memory_space=pl.ANY)
    bf16, f32 = jnp.bfloat16, jnp.float32
    packets = pltpu.VMEM((sp_count, 8, 3 * model // 4), bf16)
    tokens = pltpu.VMEM(stream.shape, bf16)
    dma = pltpu.SemaphoreType.DMA
    return pl.pallas_call(
        functools.partial(fused_kernel, sp_count, tp_count),
        out_shape=jax.ShapeDtypeStruct(stream.shape, stream.dtype),
        in_specs=[vmem] * len(vmem_args) + [hbm] * len(hbm_args),
        out_specs=vmem,
        scratch_shapes=[
            pltpu.VMEM((span, width), bf16),
            pltpu.VMEM((tp_count, rows_out, width), bf16),
            pltpu.VMEM((span, width), f32),
            pltpu.VMEM((span, lanes), f32),
            pltpu.VMEM((blocks, width, lanes), f32),
            pltpu.VMEM((blocks, width, lanes), f32),
            pltpu.VMEM((PLANE, 2 * piece + 8, lanes), f32),
            pltpu.VMEM((PLANE, 2 * piece + 8, lanes), f32),
            pltpu.VMEM((2 * piece + 8, lanes), f32),
            pltpu.VMEM((planes, 2 * piece + 8, lanes), f32),
            pltpu.VMEM((PLANE, 2 * piece, lanes), f32),
            pltpu.VMEM((PLANE, 2 * piece, lanes), f32),
            pltpu.VMEM((tp_count * width, model), bf16),
            pltpu.VMEM((tp_count, model, units), bf16),
            pltpu.VMEM((tp_count, model, units), bf16),
            pltpu.VMEM((tp_count * units, model), bf16),
            pltpu.VMEM((tp_count,) + pair_gate.shape, bf16),
            pltpu.VMEM((tp_count * pair_down.shape[0], model), bf16),
            tokens,
            tokens,
            packets,
            packets,
            pltpu.VMEM((sp_count * 8, model), bf16),
            pltpu.VMEM((sp_count * 8, tp_count * units), bf16),
            packets,
            packets,
            tokens,
            tokens,
            tokens,
            dma((6,)),
            dma((PLANE,)),
            dma((PLANE,)),
            dma((planes,)),
            dma((planes,)),
            dma((PLANE,)),
            dma((PLANE,)),
            dma((tp_count,)),
            dma((tp_count,)),
            dma((2, 4)),
            dma((2, 4)),
            dma((2, 3)),
            dma((2, 3)),
            dma((2, 2)),
            dma((2, 2)),
            dma((2, 2)),
            dma((2, 2)),
            dma((sp_count,)),
            dma((sp_count,)),
            dma((sp_count,)),
            dma((sp_count,)),
            dma((2,)),
            dma((2,)),
        ],
        compiler_params=pltpu.CompilerParams(
            collective_id=0, has_side_effects=True, vmem_limit_bytes=60 * 1024 * 1024
        ),
    )(*vmem_args, *hbm_args)


def slot_ranks(route_block, experts):
    flat_ids = route_block.reshape(-1)
    total = flat_ids.shape[0]
    onehot = (flat_ids[:, None] == jnp.arange(experts, dtype=jnp.int32)[None, :]).astype(
        jnp.bfloat16
    )
    earlier = (jnp.arange(total)[:, None] > jnp.arange(total)[None, :]).astype(jnp.bfloat16)
    before = jnp.dot(earlier, onehot, preferred_element_type=jnp.float32)
    ranks = jnp.sum(before * onehot.astype(jnp.float32), axis=1).astype(jnp.int32)
    return ranks.reshape(route_block.shape)


def body(
    stream,
    queries,
    key_rows,
    values,
    out_gate,
    fwd_decay,
    bwd_decay,
    head_gain,
    out_proj,
    mix_gain,
    ffn_gain,
    moe_gain,
    routes,
    route_weight,
    expert_gate,
    expert_up,
    expert_down,
    shared_gate,
    shared_up,
    shared_down,
):
    span_rows, lanes = queries.shape
    experts = lax.axis_size("sp")
    ranks = slot_ranks(routes, experts)
    slots = jnp.concatenate(
        [
            routes * 8 + ranks,
            routes * 8 + 6 + ranks // 3,
            ranks % 3,
            jnp.zeros_like(ranks),
        ],
        axis=1,
    )
    offset = lax.axis_index("sp") * span_rows
    positions = (offset + jnp.arange(span_rows, dtype=jnp.int32)).astype(jnp.float32)
    half = KEY_CHANNELS // 2
    lane = jnp.arange(lanes, dtype=jnp.int32) % KEY_CHANNELS
    frequency = ROPE_BASE ** (-(lane % half).astype(jnp.float32) / half)
    angles = positions[:, None] * frequency[None, :]
    sine = jnp.sin(angles)
    core = lax.rem(lax.axis_index("sp"), 2)
    part = shared_gate.shape[1] // 2
    pair_gate = jnp.concatenate(
        [
            lax.dynamic_slice_in_dim(shared_gate, core * part, part, axis=1),
            lax.dynamic_slice_in_dim(shared_up, core * part, part, axis=1),
        ],
        axis=1,
    )
    pair_down = lax.dynamic_slice_in_dim(shared_down, core * part, part, axis=0)
    return fused(
        (
            queries,
            key_rows,
            values,
            out_gate,
            jax.nn.log_sigmoid(fwd_decay) / GATE_NORM,
            jax.nn.log_sigmoid(bwd_decay) / GATE_NORM,
            jnp.cos(angles),
            jnp.where(lane[None, :] < half, -sine, sine),
            head_gain.reshape(1, -1),
            stream,
            mix_gain.reshape(1, -1),
            ffn_gain.reshape(1, -1),
            moe_gain.reshape(1, -1),
            slots,
            route_weight,
        ),
        (out_proj, expert_gate, expert_up, expert_down, pair_gate, pair_down),
    )


def solution(mesh):
    return jax.shard_map(
        body,
        mesh=mesh,
        in_specs=(
            P(("sp", "tp"), None),
            P("sp", "tp"),
            P("sp", "tp"),
            P("sp", "tp"),
            P("sp", "tp"),
            P("sp", "tp"),
            P("sp", "tp"),
            P("tp"),
            P(),
            P(),
            P(),
            P(),
            P(("sp", "tp"), None),
            P(("sp", "tp"), None),
            P("sp", None, "tp"),
            P("sp", None, "tp"),
            P("sp", "tp", None),
            P(None, "tp"),
            P(None, "tp"),
            P("tp", None),
        ),
        out_specs=P(("sp", "tp"), None),
        check_vma=False,
    )
```

```python
import functools

import jax
import jax.numpy as jnp
from jax import lax
from jax.experimental import pallas as pl
from jax.experimental.pallas import tpu as pltpu
from jax.sharding import PartitionSpec as P

KEY_CHANNELS = 64
DV = 128
BLK = 64
TOPK = 2
PLANE = 8


EPS = 1e-06
GATE_NORM = 16.0
ROPE_BASE = 10000.0
TOP_PRECISION = lax.Precision.HIGHEST
MESH = pl.DeviceIdType.MESH


def normalize(tensor):
    return tensor * lax.rsqrt(jnp.mean(tensor * tensor, axis=-1, keepdims=True) + EPS)


def dot_nt(left, right):
    return lax.dot_general(
        left, right, (((1,), (1,)), ((), ())), preferred_element_type=jnp.float32
    )


def dot_tn(left, right):
    return lax.dot_general(
        left, right, (((0,), (0,)), ((), ())), preferred_element_type=jnp.float32
    )


def fused_kernel(
    sp_count,
    tp_count,
    q_ref,
    k_ref,
    v_ref,
    gate_ref,
    fwd_ref,
    bwd_ref,
    cos_ref,
    sin_ref,
    gain_ref,
    stream_ref,
    mix_gain_ref,
    ffn_gain_ref,
    moe_gain_ref,
    route_ref,
    weight_ref,
    proj_hbm,
    eg_hbm,
    eu_hbm,
    ed_hbm,
    sg_hbm,
    su_hbm,
    sd_hbm,
    out_ref,
    mixed_ref,
    land_ref,
    within_ref,
    key_ref,
    sums_f,
    sums_b,
    near_out,
    near_in,
    far_out,
    far_in,
    carry_out,
    carry_in,
    proj_w,
    gate_w,
    up_w,
    down_w,
    sg_ref,
    su_ref,
    gu_w,
    sd_w,
    resid_ref,
    normed_ref,
    outgoing_ref,
    arrived_ref,
    lent_ref,
    rows_ref,
    hidden_ref,
    lent_out,
    lent_back,
    kept_ref,
    done_ref,
    back_ref,
    pair_in,
    part_out,
    part_in,
    local_sem,
    near_send,
    near_recv,
    far_send,
    far_recv,
    carry_send,
    carry_recv,
    row_send,
    row_recv,
    own_send,
    own_recv,
    sh_send,
    sh_recv,
    lend_send,
    lend_recv,
    give_send,
    give_recv,
    block_send,
    block_recv,
    back_send,
    back_recv,
    pair_send,
    pair_recv,
):
    span, lanes = q_ref.shape
    width = v_ref.shape[1]
    heads = lanes // KEY_CHANNELS
    blocks = span // BLK
    rows_out = span // tp_count
    planes = sp_count // PLANE
    piece = DV // PLANE
    model = stream_ref.shape[1]
    quarter = model // 4
    units = eg_hbm.shape[2]
    depth = eg_hbm.shape[1]
    sp_me = lax.axis_index("sp")
    tp_me = lax.axis_index("tp")
    z_me = sp_me // PLANE
    p_me = lax.rem(sp_me, PLANE)
    pair = sp_me + 1 - 2 * lax.rem(sp_me, 2)
    core = lax.rem(sp_me, 2)
    holder = (sp_me, tp_me + 1 - 2 * lax.rem(tp_me, 2))
    mate = (sp_me, tp_count - 1 - tp_me)
    ways = [0]
    for step in range(1, planes // 2):
        ways += [step, planes - step]
    ways.append(planes // 2)

    barrier = pltpu.get_barrier_semaphore()
    for step in range(1, sp_count):
        pl.semaphore_signal(
            barrier,
            inc=1,
            device_id=(lax.rem(sp_me + step, sp_count), tp_me),
            device_id_type=MESH,
        )
    for step in range(1, tp_count):
        pl.semaphore_signal(
            barrier,
            inc=1,
            device_id=(sp_me, lax.rem(tp_me + step, tp_count)),
            device_id_type=MESH,
        )

    def remote(source, target, send, recv, device):
        copy = pltpu.make_async_remote_copy(
            src_ref=source,
            dst_ref=target,
            send_sem=send,
            recv_sem=recv,
            device_id=device,
            device_id_type=MESH,
        )
        copy.start()
        return copy

    sd_rows = sd_hbm.shape[0] // 2
    local = []
    for index, (source, target) in enumerate(
        (
            (sg_hbm, sg_ref),
            (su_hbm, su_ref),
            (
                sd_hbm.at[pl.ds(pl.multiple_of(core * sd_rows, sd_rows), sd_rows)],
                sd_w.at[pl.ds(0, sd_rows)],
            ),
            (proj_hbm, proj_w),
            (eg_hbm.at[0], gate_w.at[0]),
            (eu_hbm.at[0], up_w.at[0]),
            (ed_hbm.at[0], down_w.at[pl.ds(0, units)]),
        )
    ):
        copy = pltpu.make_async_copy(source, target, local_sem.at[index])
        copy.start()
        local.append(copy)

    row = lax.broadcasted_iota(jnp.int32, (BLK, BLK), 0)
    column = lax.broadcasted_iota(jnp.int32, (BLK, BLK), 1)
    lower = row >= column
    upper = row <= column
    lower_ones = lower.astype(jnp.float32)
    upper_ones = upper.astype(jnp.float32)
    from_lane = lax.broadcasted_iota(jnp.int32, (lanes, lanes), 0)
    to_lane = lax.broadcasted_iota(jnp.int32, (lanes, lanes), 1)
    half = KEY_CHANNELS // 2
    partner = jnp.where(lax.rem(to_lane, KEY_CHANNELS) < half, to_lane + half, to_lane - half)
    swap = (from_lane == partner).astype(jnp.bfloat16)
    own_head = (
        lax.broadcasted_iota(jnp.int32, (width, lanes), 0) // DV
        == lax.broadcasted_iota(jnp.int32, (width, lanes), 1) // KEY_CHANNELS
    )
    lane_head = lax.broadcasted_iota(jnp.int32, (BLK, lanes), 1) // KEY_CHANNELS

    lane_low = lax.rem(lax.broadcasted_iota(jnp.int32, (BLK, lanes), 1), KEY_CHANNELS) < half

    def rotated(tensor, block):
        swapped = jnp.dot(tensor, swap, preferred_element_type=jnp.float32)
        cos_block, sin_block = cos_ref[block : block + 1], sin_ref[block : block + 1]
        cos_row, sin_row = cos_ref[blocks : blocks + BLK], sin_ref[blocks : blocks + BLK]
        cosine = cos_block * cos_row - sin_block * sin_row
        sine = sin_block * cos_row + cos_block * sin_row
        return tensor.astype(jnp.float32) * cosine + swapped * jnp.where(lane_low, -sine, sine)

    cumul_f, cumul_b, decay_f, decay_b = [], [], [], []
    for block in range(blocks):
        rows = pl.ds(block * BLK, BLK)
        total_f = jnp.dot(
            lower_ones,
            jax.nn.log_sigmoid(fwd_ref[rows, :]) / GATE_NORM,
            precision=TOP_PRECISION,
            preferred_element_type=jnp.float32,
        )
        total_b = jnp.dot(
            upper_ones,
            jax.nn.log_sigmoid(bwd_ref[rows, :]) / GATE_NORM,
            precision=TOP_PRECISION,
            preferred_element_type=jnp.float32,
        )
        last_f = total_f[BLK - 1 : BLK]
        last_b = total_b[0:1]
        keys = rotated(k_ref[rows, :], block)
        key_ref[rows, :] = keys
        value_rows = v_ref[rows, :]
        out_f = (keys * jnp.exp(last_f - total_f)).astype(jnp.bfloat16)
        out_b = (keys * jnp.exp(last_b - total_b)).astype(jnp.bfloat16)
        sums_f[block] = jnp.where(own_head, dot_tn(value_rows, out_f), 0.0)
        sums_b[block] = jnp.where(own_head, dot_tn(value_rows, out_b), 0.0)
        cumul_f.append(total_f)
        cumul_b.append(total_b)
        decay_f.append(jnp.exp(last_f))
        decay_b.append(jnp.exp(last_b))

    local[0].wait()
    local[1].wait()
    local[2].wait()
    shared_low = lax.broadcasted_iota(jnp.int32, sg_ref.shape, 1) < sd_rows
    gate_rows = sg_ref[...].astype(jnp.float32)
    up_rows = su_ref[...].astype(jnp.float32)
    first = jnp.where(core == 0, gate_rows, pltpu.roll(gate_rows, sd_rows, 1))
    second = jnp.where(core == 0, pltpu.roll(up_rows, sd_rows, 1), up_rows)
    gu_w[0] = jnp.where(shared_low, first, second).astype(jnp.bfloat16)

    pl.semaphore_wait(barrier, sp_count - 1 + tp_count - 1)
    own_copies = []

    def send_own(item):
        source, target = (
            (eg_hbm.at[0], gate_w.at[1]),
            (eu_hbm.at[0], up_w.at[1]),
            (ed_hbm.at[0], down_w.at[pl.ds(units, units)]),
        )[item]
        own_copies.append(remote(source, target, own_send.at[item], own_recv.at[item], holder))

    send_own(0)

    def packed(total):
        return sum(total[h * DV : (h + 1) * DV] for h in range(heads))

    total = sums_f[0]
    through_f = decay_f[0]
    for block in range(1, blocks):
        total = total * decay_f[block] + sums_f[block]
        through_f = through_f * decay_f[block]
    state_f = packed(total)
    total = sums_b[blocks - 1]
    through_b = decay_b[blocks - 1]
    for block in range(blocks - 2, -1, -1):
        total = total * decay_b[block] + sums_b[block]
        through_b = through_b * decay_b[block]
    state_b = packed(total)

    def put_state(ref, first, second, through_first, through_second):
        ref[0:piece] = first.astype(jnp.bfloat16)
        ref[piece : 2 * piece] = second.astype(jnp.bfloat16)
        high = [t.astype(jnp.bfloat16).astype(jnp.float32) for t in (through_first, through_second)]
        ref[2 * piece : 2 * piece + 8] = jnp.concatenate(
            [
                high[0],
                through_first - high[0],
                high[1],
                through_second - high[1],
                jnp.zeros((4, lanes), jnp.float32),
            ],
            axis=0,
        ).astype(jnp.bfloat16)

    def get_state(ref, index):
        block = ref[index].astype(jnp.float32)
        cut = 2 * piece
        return (
            block[0:piece],
            block[piece:cut],
            block[cut : cut + 1] + block[cut + 1 : cut + 2],
            block[cut + 2 : cut + 3] + block[cut + 3 : cut + 4],
        )

    for p in range(PLANE):
        cut = slice(p * piece, (p + 1) * piece)
        put_state(near_out.at[p], state_f[cut], state_b[cut], through_f, through_b)
    near_copies = []
    for step in range(1, PLANE):
        target = lax.rem(p_me + step, PLANE)
        near_copies.append(
            remote(
                near_out.at[target],
                near_in.at[p_me],
                near_send.at[step],
                near_recv.at[step],
                (z_me * PLANE + target, tp_me),
            )
        )
    near_in[p_me] = near_out[p_me]
    sh_copies = []

    def send_shared(index, source, target, device):
        sh_copies.append(remote(source, target, sh_send.at[index], sh_recv.at[index], device))

    send_shared(0, gu_w.at[0], gu_w.at[1], mate)
    send_shared(1, sd_w.at[pl.ds(0, sd_rows)], sd_w.at[pl.ds(sd_rows, sd_rows)], mate)

    query_f, query_b = [], []

    def within(block):
        rows = pl.ds(block * BLK, BLK)
        queries = rotated(q_ref[rows, :], block) * KEY_CHANNELS ** (-0.5)
        keys = key_ref[rows, :]
        total_f, total_b = cumul_f[block], cumul_b[block]
        middle_f = total_f[BLK // 2 - 1 : BLK // 2]
        middle_b = total_b[BLK // 2 : BLK // 2 + 1]
        scaled_qf = queries * jnp.exp(total_f - middle_f)
        scaled_qb = queries * jnp.exp(total_b - middle_b)
        scaled_kf = (keys * jnp.exp(middle_f - total_f)).astype(jnp.bfloat16)
        scaled_kb = (keys * jnp.exp(middle_b - total_b)).astype(jnp.bfloat16)
        query_f.append((queries * jnp.exp(total_f)).astype(jnp.bfloat16))
        query_b.append((queries * jnp.exp(total_b)).astype(jnp.bfloat16))
        for h in range(heads):
            mine = lane_head == h
            scores_f = dot_nt(jnp.where(mine, scaled_qf, 0.0).astype(jnp.bfloat16), scaled_kf)
            scores_b = dot_nt(jnp.where(mine, scaled_qb, 0.0).astype(jnp.bfloat16), scaled_kb)
            scores = jnp.where(lower, scores_f, 0.0) + jnp.where(upper, scores_b, 0.0)
            within_ref[rows, h * DV : (h + 1) * DV] = jnp.dot(
                scores.astype(jnp.bfloat16),
                v_ref[rows, h * DV : (h + 1) * DV],
                preferred_element_type=jnp.float32,
            )

    third = blocks // 3
    for block in range(third):
        within(block)
    for copy in near_copies:
        copy.wait()

    def fold(orders, visit):
        state = jnp.zeros((piece, lanes), jnp.float32)
        through = jnp.ones((1, lanes), jnp.float32)
        first = orders[0] == 0
        for p in orders:
            visit(p, state, through)
            fwd_state, bwd_state, fwd_through, bwd_through = get_state(near_in, p)
            state = state * (fwd_through if first else bwd_through) + (
                fwd_state if first else bwd_state
            )
            through = through * (fwd_through if first else bwd_through)
        return state, through

    ahead = list(range(PLANE))
    behind = ahead[::-1]
    plane_f, plane_df = fold(ahead, lambda p, state, through: None)
    plane_b, plane_db = fold(behind, lambda p, state, through: None)
    put_state(far_out, plane_f, plane_b, plane_df, plane_db)
    far_copies = []
    for step in range(1, planes):
        target = lax.rem(z_me + step, planes)
        far_copies.append(
            remote(
                far_out,
                far_in.at[z_me],
                far_send.at[step],
                far_recv.at[step],
                (target * PLANE + p_me, tp_me),
            )
        )
    far_in[z_me] = far_out[...]
    for block in range(third, blocks - third):
        within(block)
    for copy in far_copies:
        copy.wait()
    enter_f = jnp.zeros((piece, lanes), jnp.float32)
    enter_b = jnp.zeros((piece, lanes), jnp.float32)
    for z in range(planes):
        plane_state, _, plane_through, _ = get_state(far_in, z)
        enter_f = jnp.where(z < z_me, enter_f * plane_through + plane_state, enter_f)
    for z in range(planes - 1, -1, -1):
        _, plane_state, _, plane_through = get_state(far_in, z)
        enter_b = jnp.where(z > z_me, enter_b * plane_through + plane_state, enter_b)

    def emit_f(p, state, through):
        carry_out[p, 0:piece] = (enter_f * through + state).astype(jnp.bfloat16)

    def emit_b(p, state, through):
        carry_out[p, piece : 2 * piece] = (enter_b * through + state).astype(jnp.bfloat16)

    fold(ahead, emit_f)
    fold(behind, emit_b)
    carry_copies = []
    for step in range(1, PLANE):
        target = lax.rem(p_me + step, PLANE)
        carry_copies.append(
            remote(
                carry_out.at[target],
                carry_in.at[p_me],
                carry_send.at[step],
                carry_recv.at[step],
                (z_me * PLANE + target, tp_me),
            )
        )
    carry_in[p_me] = carry_out[p_me]
    for block in range(blocks - third, blocks):
        within(block)
    for copy in carry_copies:
        copy.wait()

    def unpacked(first):
        carry = jnp.concatenate(
            [carry_in[p, first : first + piece].astype(jnp.float32) for p in range(PLANE)], axis=0
        )
        return jnp.where(own_head, jnp.concatenate([carry] * heads, axis=0), 0.0)

    state = unpacked(0)
    for block in range(blocks):
        rows = pl.ds(block * BLK, BLK)
        within_ref[rows, :] += dot_nt(query_f[block], state.astype(jnp.bfloat16))
        if block < blocks - 1:
            state = state * decay_f[block] + sums_f[block]
    state = unpacked(piece)
    for block in range(blocks - 1, -1, -1):
        rows = pl.ds(block * BLK, BLK)
        attended = within_ref[rows, :] + dot_nt(query_b[block], state.astype(jnp.bfloat16))
        if block > 0:
            state = state * decay_b[block] + sums_b[block]
        for h in range(heads):
            part = attended[:, h * DV : (h + 1) * DV]
            square = jnp.mean(part * part, axis=-1, keepdims=True)
            gate = gate_ref[rows, h * DV : (h + 1) * DV].astype(jnp.float32)
            mixed_ref[rows, h * DV : (h + 1) * DV] = (
                part
                * lax.rsqrt(square + EPS)
                * gain_ref[:, h * DV : (h + 1) * DV]
                * (gate / (1.0 + jnp.exp(-gate)))
            ).astype(jnp.bfloat16)

    row_copies = []
    for step in range(1, tp_count):
        target = lax.rem(tp_me + step, tp_count)
        row_copies.append(
            remote(
                mixed_ref.at[pl.ds(pl.multiple_of(target * rows_out, rows_out), rows_out)],
                land_ref.at[tp_me],
                row_send.at[step],
                row_recv.at[step],
                (sp_me, target),
            )
        )
    send_own(1)
    send_own(2)
    land_ref[tp_me] = mixed_ref[pl.ds(pl.multiple_of(tp_me * rows_out, rows_out), rows_out), :]

    def iota(shape, axis):
        return lax.broadcasted_iota(jnp.int32, shape, axis)

    square_shape = (rows_out, rows_out)
    eye = (iota(square_shape, 0) == iota(square_shape, 1)).astype(jnp.float32)
    columns = lax.dot_general(
        eye,
        jnp.concatenate(
            [
                route_ref[...].astype(jnp.float32),
                weight_ref[...],
                jnp.zeros((8 - 2 * TOPK, rows_out), jnp.float32),
            ],
            axis=0,
        ),
        (((1,), (1,)), ((), ())),
        precision=TOP_PRECISION,
        preferred_element_type=jnp.float32,
    )
    named = [columns[:, k : k + 1] for k in range(TOPK)]
    weights = [columns[:, TOPK + k : TOPK + k + 1] for k in range(TOPK)]
    expert_lane = iota((rows_out, 128), 1).astype(jnp.float32)
    onehot = [(named[k] == expert_lane).astype(jnp.float32) for k in range(TOPK)]
    earlier = (iota(square_shape, 0) > iota(square_shape, 1)).astype(jnp.bfloat16)
    every = jnp.ones(square_shape, jnp.bfloat16)
    slot_lane = iota((rows_out, sp_count * 8), 1).astype(jnp.float32)
    seen = jnp.zeros((rows_out, 128), jnp.float32)
    mains, tails, thirds = [], [], []
    for k in range(TOPK):
        hot = onehot[k].astype(jnp.bfloat16)
        before = seen + jnp.dot(earlier, hot, preferred_element_type=jnp.float32)
        seen = seen + jnp.dot(every, hot, preferred_element_type=jnp.float32)
        rank = jnp.sum(before * onehot[k], axis=1, keepdims=True)
        over = jnp.where(rank >= 3.0, 1.0, 0.0)
        mains.append(named[k] * 8.0 + rank == slot_lane)
        tails.append(named[k] * 8.0 + 6.0 + over == slot_lane)
        thirds.append(rank - 3.0 * over)

    def tail_hit(k, b):
        return jnp.logical_and(tails[k], thirds[k] == b)

    def chosen(first, second):
        return jnp.where(jnp.logical_or(first, second), 1.0, 0.0).astype(jnp.bfloat16)

    local[3].wait()
    for copy in row_copies:
        copy.wait()
    mixed_all = jnp.concatenate([land_ref[source] for source in range(tp_count)], axis=1)
    projected = jnp.dot(mixed_all, proj_w[...], preferred_element_type=jnp.float32)
    residual = (
        stream_ref[...].astype(jnp.float32) + normalize(projected) * mix_gain_ref[...]
    ).astype(jnp.bfloat16)
    resid_ref[...] = residual
    normed = (normalize(residual.astype(jnp.float32)) * ffn_gain_ref[...]).astype(jnp.bfloat16)
    normed_ref[...] = normed
    pick_main = chosen(mains[0], mains[1])
    for b in range(3):
        picks = jnp.concatenate([pick_main, chosen(tail_hit(0, b), tail_hit(1, b))], axis=0)
        source = jnp.concatenate(
            [normed[:, b * quarter : (b + 1) * quarter], normed[:, 3 * quarter :]], axis=0
        )
        outgoing_ref[:, :, b * quarter : (b + 1) * quarter] = (
            dot_tn(picks, source).reshape(sp_count, 8, quarter).astype(jnp.bfloat16)
        )
    def exchange(source_ref, source_of, target_ref, send, recv, way):
        copies = []
        for turn in range(PLANE):
            if way == 0 and turn == 0:
                continue
            target = lax.rem(z_me + way, planes) * PLANE + lax.rem(p_me + turn, PLANE)
            copies.append(
                remote(
                    source_ref.at[source_of(target)],
                    target_ref.at[sp_me],
                    send.at[way, turn],
                    recv.at[way, turn],
                    (target, tp_me),
                )
            )
        return copies

    block_copies = [
        exchange(outgoing_ref, lambda target: target, arrived_ref, block_send, block_recv, way)
        for way in ways
    ]
    arrived_ref[sp_me] = outgoing_ref[sp_me]
    pair_copy = remote(normed_ref, pair_in, pair_send.at[0], pair_recv.at[0], (pair, tp_me))
    sh_copies[0].wait()
    sh_copies[1].wait()
    send_shared(2, gu_w.at[pl.ds(0, 2)], gu_w.at[pl.ds(2, 2)], holder)
    send_shared(
        3, sd_w.at[pl.ds(0, 2 * sd_rows)], sd_w.at[pl.ds(2 * sd_rows, 2 * sd_rows)], holder
    )

    group = PLANE * 8
    spot = iota((group, group), 0)
    origin = iota((group, group), 1)
    same = spot // 8 == origin // 8

    def spread(target, source, b):
        rank = lax.rem(target, 8)
        hit = jnp.logical_and(rank < 6, lax.rem(rank, 3) == b)
        hit = jnp.logical_and(hit, lax.rem(source, 8) == 6 + rank // 3)
        return jnp.where(jnp.logical_and(same, hit), 1.0, 0.0).astype(jnp.bfloat16)

    scatter = [spread(spot, origin, b) for b in range(3)]
    gather = [spread(origin, spot, b) for b in range(3)]

    def sources(index):
        plane = lax.rem(z_me + planes - ways[index], planes)
        return pl.ds(pl.multiple_of(plane * PLANE, PLANE), PLANE)

    def unpack(ref, side, index):
        cut = slice(index * group, (index + 1) * group)
        tail = jnp.zeros((group, quarter), jnp.float32)
        for b in range(3):
            block = ref[sources(index), :, b * quarter : (b + 1) * quarter].reshape(group, quarter)
            rows_ref[side, cut, b * quarter : (b + 1) * quarter] = block
            tail = tail + jnp.dot(scatter[b], block, preferred_element_type=jnp.float32)
        rows_ref[side, cut, 3 * quarter :] = tail.astype(jnp.bfloat16)

    lend_copies = []
    for index in range(planes):
        for copy in block_copies[index]:
            copy.wait()
        lend_copies.append(
            remote(
                arrived_ref.at[sources(index)],
                lent_ref.at[sources(index)],
                lend_send.at[index],
                lend_recv.at[index],
                mate,
            )
        )
        unpack(arrived_ref, 0, index)

    def hidden_of(side, part, shard):
        rows = rows_ref[side, part]
        hidden_ref[side, part, shard * units : (shard + 1) * units] = (
            jax.nn.silu(jnp.dot(rows, gate_w[shard], preferred_element_type=jnp.float32))
            * jnp.dot(rows, up_w[shard], preferred_element_type=jnp.float32)
        ).astype(jnp.bfloat16)

    for copy in local[4:]:
        copy.wait()
    total_rows = sp_count * 8
    whole = slice(0, total_rows)
    halves = [slice(total_rows // 2, total_rows), slice(0, total_rows // 2)]
    hidden_of(0, whole, 0)
    for index, copy in enumerate(lend_copies):
        copy.wait()
        unpack(lent_ref, 1, index)
    hidden_of(1, whole, 0)
    for copy in own_copies:
        copy.wait()

    def finish(side, part, target_ref):
        count = part.stop - part.start
        hidden = hidden_ref[side, part]
        keep = lax.rem(iota((count, quarter), 0), 8) < 6
        last = jnp.dot(
            hidden, down_w[:, 3 * quarter :], preferred_element_type=jnp.float32
        ).astype(jnp.bfloat16)
        for b in range(3):
            value = jnp.dot(
                hidden,
                down_w[:, b * quarter : (b + 1) * quarter],
                preferred_element_type=jnp.float32,
            )
            moved = jnp.concatenate(
                [
                    jnp.dot(
                        gather[b], last[start : start + group], preferred_element_type=jnp.float32
                    )
                    for start in range(0, count, group)
                ],
                axis=0,
            )
            target_ref[part.start // 8 : part.stop // 8, :, b * quarter : (b + 1) * quarter] = (
                jnp.where(keep, value, moved).reshape(count // 8, 8, quarter).astype(jnp.bfloat16)
            )

    give_copies = {}
    for part in halves:
        hidden_of(1, part, 1)
        finish(1, part, lent_out)
        for index in range(part.stop // group - 1, part.start // group - 1, -1):
            cut = pl.ds(index * PLANE, PLANE)
            give_copies[index] = remote(
                lent_out.at[cut],
                lent_back.at[cut],
                give_send.at[index],
                give_recv.at[index],
                mate,
            )
    hidden_of(0, whole, 1)
    finish(0, whole, kept_ref)
    back_copies = []
    for index in range(planes - 1, -1, -1):
        cut = slice(index * PLANE, (index + 1) * PLANE)
        give_copies[index].wait()
        done_ref[sources(index)] = (
            kept_ref[cut].astype(jnp.float32) + lent_back[cut].astype(jnp.float32)
        ).astype(jnp.bfloat16)
        back_copies += exchange(
            done_ref,
            lambda target: target,
            back_ref,
            back_send,
            back_recv,
            (planes - ways[index]) % planes,
        )
    back_ref[sp_me] = done_ref[sp_me]

    sh_copies[2].wait()
    sh_copies[3].wait()
    pair_copy.wait()
    tokens = jnp.concatenate([normed_ref[...], pair_in[...]], axis=0)
    lane = lax.broadcasted_iota(jnp.int32, (2 * rows_out, 2 * sd_rows), 1)
    units_of = []
    for slot in range(tp_count):
        both = jnp.dot(tokens, gu_w[slot], preferred_element_type=jnp.float32)
        units_of.append(jax.nn.silu(both) * pltpu.roll(both, sd_rows, 1))
    hidden = jnp.concatenate(
        [
            jnp.where(lane < sd_rows, units_of[s], pltpu.roll(units_of[s + 1], sd_rows, 1))
            for s in range(0, tp_count, 2)
        ],
        axis=1,
    ).astype(jnp.bfloat16)
    part_out[...] = jnp.dot(
        hidden[rows_out:], sd_w[...], preferred_element_type=jnp.float32
    ).astype(jnp.bfloat16)
    part_copy = remote(part_out, part_in, pair_send.at[1], pair_recv.at[1], (pair, tp_me))
    shared = jnp.dot(hidden[:rows_out], sd_w[...], preferred_element_type=jnp.float32)

    def split(hits):
        full = jnp.where(hits[0], weights[0], 0.0) + jnp.where(hits[1], weights[1], 0.0)
        high = full.astype(jnp.bfloat16)
        return [high, (full - high.astype(jnp.float32)).astype(jnp.bfloat16)]

    main_split = split(mains)
    sides = [
        jnp.concatenate(main_split + split([tail_hit(0, b), tail_hit(1, b)]), axis=0)
        for b in range(3)
    ]
    part_copy.wait()
    for copy in back_copies:
        copy.wait()
    shared = shared + part_in[...].astype(jnp.float32)
    pieces = []
    tail = jnp.zeros((rows_out, quarter), jnp.float32)
    for b in range(3):
        block = back_ref[:, :, b * quarter : (b + 1) * quarter].reshape(sp_count * 8, quarter)
        value = jnp.dot(sides[b], block, preferred_element_type=jnp.float32)
        pieces.append(value[0:rows_out] + value[rows_out : 2 * rows_out])
        tail = tail + value[2 * rows_out : 3 * rows_out] + value[3 * rows_out :]
    mixture = shared + jnp.concatenate(pieces + [tail], axis=1)
    square = jnp.mean(mixture * mixture, axis=-1, keepdims=True)
    out_ref[...] = (
        resid_ref[...].astype(jnp.float32)
        + mixture * lax.rsqrt(square + EPS) * moe_gain_ref[...]
    ).astype(out_ref.dtype)


def fused(vmem_args, hbm_args):
    sp_count = lax.axis_size("sp")
    tp_count = lax.axis_size("tp")
    queries, _, values = vmem_args[:3]
    stream = vmem_args[9]
    _, expert_gate, _, expert_down, shared_gate, _, shared_down = hbm_args
    span, lanes = queries.shape
    width = values.shape[1]
    rows_out = span // tp_count
    blocks = span // BLK
    planes = sp_count // PLANE
    piece = DV // PLANE
    model = stream.shape[1]
    units = expert_gate.shape[2]
    vmem = pl.BlockSpec(memory_space=pltpu.VMEM)
    hbm = pl.BlockSpec(memory_space=pl.ANY)
    bf16, f32 = jnp.bfloat16, jnp.float32
    packets = pltpu.VMEM((sp_count, 8, 3 * model // 4), bf16)
    tokens = pltpu.VMEM(stream.shape, bf16)
    dma = pltpu.SemaphoreType.DMA
    return pl.pallas_call(
        functools.partial(fused_kernel, sp_count, tp_count),
        out_shape=jax.ShapeDtypeStruct(stream.shape, stream.dtype),
        in_specs=[vmem] * len(vmem_args) + [hbm] * len(hbm_args),
        out_specs=vmem,
        scratch_shapes=[
            pltpu.VMEM((span, width), bf16),
            pltpu.VMEM((tp_count, rows_out, width), bf16),
            pltpu.VMEM((span, width), f32),
            pltpu.VMEM((span, lanes), f32),
            pltpu.VMEM((blocks, width, lanes), f32),
            pltpu.VMEM((blocks, width, lanes), f32),
            pltpu.VMEM((PLANE, 2 * piece + 8, lanes), bf16),
            pltpu.VMEM((PLANE, 2 * piece + 8, lanes), bf16),
            pltpu.VMEM((2 * piece + 8, lanes), bf16),
            pltpu.VMEM((planes, 2 * piece + 8, lanes), bf16),
            pltpu.VMEM((PLANE, 2 * piece, lanes), bf16),
            pltpu.VMEM((PLANE, 2 * piece, lanes), bf16),
            pltpu.VMEM((tp_count * width, model), bf16),
            pltpu.VMEM((2, model, units), bf16),
            pltpu.VMEM((2, model, units), bf16),
            pltpu.VMEM((2 * units, model), bf16),
            pltpu.VMEM(shared_gate.shape, bf16),
            pltpu.VMEM(shared_gate.shape, bf16),
            pltpu.VMEM((tp_count,) + shared_gate.shape, bf16),
            pltpu.VMEM((tp_count * shared_down.shape[0] // 2, model), bf16),
            tokens,
            tokens,
            packets,
            packets,
            packets,
            pltpu.VMEM((2, sp_count * 8, model), bf16),
            pltpu.VMEM((2, sp_count * 8, 2 * units), bf16),
            packets,
            packets,
            packets,
            packets,
            packets,
            tokens,
            tokens,
            tokens,
            dma((7,)),
            dma((PLANE,)),
            dma((PLANE,)),
            dma((planes,)),
            dma((planes,)),
            dma((PLANE,)),
            dma((PLANE,)),
            dma((tp_count,)),
            dma((tp_count,)),
            dma((3,)),
            dma((3,)),
            dma((4,)),
            dma((4,)),
            dma((planes,)),
            dma((planes,)),
            dma((planes,)),
            dma((planes,)),
            dma((planes, PLANE)),
            dma((planes, PLANE)),
            dma((planes, PLANE)),
            dma((planes, PLANE)),
            dma((2,)),
            dma((2,)),
        ],
        compiler_params=pltpu.CompilerParams(
            collective_id=0, has_side_effects=True, vmem_limit_bytes=60 * 1024 * 1024
        ),
    )(*vmem_args, *hbm_args)


def body(
    stream,
    queries,
    key_rows,
    values,
    out_gate,
    fwd_decay,
    bwd_decay,
    head_gain,
    out_proj,
    mix_gain,
    ffn_gain,
    moe_gain,
    routes,
    route_weight,
    expert_gate,
    expert_up,
    expert_down,
    shared_gate,
    shared_up,
    shared_down,
):
    span_rows, lanes = queries.shape
    offset = lax.axis_index("sp") * span_rows
    positions = jnp.concatenate(
        [
            offset + jnp.arange(0, span_rows, BLK, dtype=jnp.int32),
            jnp.arange(BLK, dtype=jnp.int32),
        ]
    ).astype(jnp.float32)
    half = KEY_CHANNELS // 2
    lane = jnp.arange(lanes, dtype=jnp.int32) % KEY_CHANNELS
    frequency = ROPE_BASE ** (-(lane % half).astype(jnp.float32) / half)
    angles = positions[:, None] * frequency[None, :]
    return fused(
        (
            queries,
            key_rows,
            values,
            out_gate,
            fwd_decay,
            bwd_decay,
            jnp.cos(angles),
            jnp.sin(angles),
            head_gain.reshape(1, -1),
            stream,
            mix_gain.reshape(1, -1),
            ffn_gain.reshape(1, -1),
            moe_gain.reshape(1, -1),
            routes.T,
            route_weight.T,
        ),
        (out_proj, expert_gate, expert_up, expert_down, shared_gate, shared_up, shared_down),
    )


def solution(mesh):
    return jax.shard_map(
        body,
        mesh=mesh,
        in_specs=(
            P(("sp", "tp"), None),
            P("sp", "tp"),
            P("sp", "tp"),
            P("sp", "tp"),
            P("sp", "tp"),
            P("sp", "tp"),
            P("sp", "tp"),
            P("tp"),
            P(),
            P(),
            P(),
            P(),
            P(("sp", "tp"), None),
            P(("sp", "tp"), None),
            P("sp", None, "tp"),
            P("sp", None, "tp"),
            P("sp", "tp", None),
            P(None, "tp"),
            P(None, "tp"),
            P("tp", None),
        ),
        out_specs=P(("sp", "tp"), None),
        check_vma=False,
    )
```

```python
import functools

import jax
import jax.numpy as jnp
from jax import lax
from jax.experimental import pallas as pl
from jax.experimental.pallas import tpu as pltpu
from jax.sharding import PartitionSpec as P

KEY_CHANNELS = 64
DV = 128
BLK = 64
TOPK = 2
PLANE = 8


EPS = 1e-06
GATE_NORM = 16.0
ROPE_BASE = 10000.0
TOP_PRECISION = lax.Precision.HIGHEST
MESH = pl.DeviceIdType.MESH


def normalize(tensor):
    return tensor * lax.rsqrt(jnp.mean(tensor * tensor, axis=-1, keepdims=True) + EPS)


def dot_nt(left, right):
    return lax.dot_general(
        left, right, (((1,), (1,)), ((), ())), preferred_element_type=jnp.float32
    )


def dot_tn(left, right):
    return lax.dot_general(
        left, right, (((0,), (0,)), ((), ())), preferred_element_type=jnp.float32
    )


def fused_kernel(
    sp_count,
    tp_count,
    q_ref,
    k_ref,
    v_ref,
    gate_ref,
    fwd_ref,
    bwd_ref,
    cos_ref,
    sin_ref,
    gain_ref,
    stream_ref,
    mix_gain_ref,
    ffn_gain_ref,
    moe_gain_ref,
    route_ref,
    weight_ref,
    proj_hbm,
    eg_hbm,
    eu_hbm,
    ed_hbm,
    sg_hbm,
    su_hbm,
    sd_hbm,
    out_ref,
    mixed_ref,
    land_ref,
    within_ref,
    key_ref,
    sums_f,
    sums_b,
    near_out,
    near_in,
    far_out,
    far_in,
    carry_out,
    carry_in,
    proj_w,
    gate_w,
    up_w,
    down_w,
    sg_ref,
    su_ref,
    gu_w,
    sd_w,
    resid_ref,
    normed_ref,
    outgoing_ref,
    arrived_ref,
    lent_ref,
    rows_ref,
    hidden_ref,
    lent_out,
    lent_back,
    kept_ref,
    done_ref,
    back_ref,
    pair_in,
    part_out,
    part_in,
    mixture_ref,
    local_sem,
    near_send,
    near_recv,
    far_send,
    far_recv,
    carry_send,
    carry_recv,
    row_send,
    row_recv,
    own_send,
    own_recv,
    sh_send,
    sh_recv,
    lend_send,
    lend_recv,
    give_send,
    give_recv,
    block_send,
    block_recv,
    back_send,
    back_recv,
    pair_send,
    pair_recv,
):
    span, lanes = q_ref.shape
    width = v_ref.shape[1]
    heads = lanes // KEY_CHANNELS
    blocks = span // BLK
    rows_out = span // tp_count
    planes = sp_count // PLANE
    piece = DV // PLANE
    model = stream_ref.shape[1]
    quarter = model // 4
    units = eg_hbm.shape[2]
    depth = eg_hbm.shape[1]
    sp_me = lax.axis_index("sp")
    tp_me = lax.axis_index("tp")
    z_me = sp_me // PLANE
    p_me = lax.rem(sp_me, PLANE)
    pair = sp_me + 1 - 2 * lax.rem(sp_me, 2)
    core = lax.rem(sp_me, 2)
    flip = tp_me + 1 - 2 * lax.rem(tp_me, 2)
    mirror = tp_count - 1 - tp_me
    holder = (sp_me, jnp.where(core == 0, flip, mirror))
    mate = (sp_me, jnp.where(core == 0, mirror, flip))
    ways = [0, planes // 2, 1, planes - 1]
    for step in range(2, planes // 2):
        ways += [step, planes - step]

    barrier = pltpu.get_barrier_semaphore()
    for step in range(1, sp_count):
        pl.semaphore_signal(
            barrier,
            inc=1,
            device_id=(lax.rem(sp_me + step, sp_count), tp_me),
            device_id_type=MESH,
        )
    for step in range(1, tp_count):
        pl.semaphore_signal(
            barrier,
            inc=1,
            device_id=(sp_me, lax.rem(tp_me + step, tp_count)),
            device_id_type=MESH,
        )

    def remote(source, target, send, recv, device):
        copy = pltpu.make_async_remote_copy(
            src_ref=source,
            dst_ref=target,
            send_sem=send,
            recv_sem=recv,
            device_id=device,
            device_id_type=MESH,
        )
        copy.start()
        return copy

    sd_rows = sd_hbm.shape[0] // 2
    local = []
    for index, (source, target) in enumerate(
        (
            (sg_hbm, sg_ref),
            (su_hbm, su_ref),
            (
                sd_hbm.at[pl.ds(pl.multiple_of(core * sd_rows, sd_rows), sd_rows)],
                sd_w.at[pl.ds(0, sd_rows)],
            ),
            (proj_hbm, proj_w),
            (eg_hbm.at[0], gate_w.at[0]),
            (eu_hbm.at[0], up_w.at[0]),
            (ed_hbm.at[0], down_w.at[pl.ds(0, units)]),
        )
    ):
        copy = pltpu.make_async_copy(source, target, local_sem.at[index])
        copy.start()
        local.append(copy)

    row = lax.broadcasted_iota(jnp.int32, (BLK, BLK), 0)
    column = lax.broadcasted_iota(jnp.int32, (BLK, BLK), 1)
    lower = row >= column
    upper = row <= column
    lower_ones = lower.astype(jnp.float32)
    upper_ones = upper.astype(jnp.float32)
    from_lane = lax.broadcasted_iota(jnp.int32, (lanes, lanes), 0)
    to_lane = lax.broadcasted_iota(jnp.int32, (lanes, lanes), 1)
    half = KEY_CHANNELS // 2
    partner = jnp.where(lax.rem(to_lane, KEY_CHANNELS) < half, to_lane + half, to_lane - half)
    swap = (from_lane == partner).astype(jnp.bfloat16)
    own_head = (
        lax.broadcasted_iota(jnp.int32, (width, lanes), 0) // DV
        == lax.broadcasted_iota(jnp.int32, (width, lanes), 1) // KEY_CHANNELS
    )
    lane_head = lax.broadcasted_iota(jnp.int32, (BLK, lanes), 1) // KEY_CHANNELS

    lane_low = lax.rem(lax.broadcasted_iota(jnp.int32, (BLK, lanes), 1), KEY_CHANNELS) < half

    def rotated(tensor, block):
        swapped = jnp.dot(tensor, swap, preferred_element_type=jnp.float32)
        cos_block, sin_block = cos_ref[block : block + 1], sin_ref[block : block + 1]
        cos_row, sin_row = cos_ref[blocks : blocks + BLK], sin_ref[blocks : blocks + BLK]
        cosine = cos_block * cos_row - sin_block * sin_row
        sine = sin_block * cos_row + cos_block * sin_row
        return tensor.astype(jnp.float32) * cosine + swapped * jnp.where(lane_low, -sine, sine)

    cumul_f, cumul_b, decay_f, decay_b = [], [], [], []
    for block in range(blocks):
        rows = pl.ds(block * BLK, BLK)
        total_f = jnp.dot(
            lower_ones,
            jax.nn.log_sigmoid(fwd_ref[rows, :]) / GATE_NORM,
            precision=TOP_PRECISION,
            preferred_element_type=jnp.float32,
        )
        total_b = jnp.dot(
            upper_ones,
            jax.nn.log_sigmoid(bwd_ref[rows, :]) / GATE_NORM,
            precision=TOP_PRECISION,
            preferred_element_type=jnp.float32,
        )
        last_f = total_f[BLK - 1 : BLK]
        last_b = total_b[0:1]
        keys = rotated(k_ref[rows, :], block)
        key_ref[rows, :] = keys
        value_rows = v_ref[rows, :]
        out_f = (keys * jnp.exp(last_f - total_f)).astype(jnp.bfloat16)
        out_b = (keys * jnp.exp(last_b - total_b)).astype(jnp.bfloat16)
        sums_f[block] = jnp.where(own_head, dot_tn(value_rows, out_f), 0.0)
        sums_b[block] = jnp.where(own_head, dot_tn(value_rows, out_b), 0.0)
        cumul_f.append(total_f)
        cumul_b.append(total_b)
        decay_f.append(jnp.exp(last_f))
        decay_b.append(jnp.exp(last_b))

    local[0].wait()
    local[1].wait()
    local[2].wait()
    shared_low = lax.broadcasted_iota(jnp.int32, sg_ref.shape, 1) < sd_rows
    gate_rows = sg_ref[...].astype(jnp.float32)
    up_rows = su_ref[...].astype(jnp.float32)
    first = jnp.where(core == 0, gate_rows, pltpu.roll(gate_rows, sd_rows, 1))
    second = jnp.where(core == 0, pltpu.roll(up_rows, sd_rows, 1), up_rows)
    gu_w[0] = jnp.where(shared_low, first, second).astype(jnp.bfloat16)

    pl.semaphore_wait(barrier, sp_count - 1 + tp_count - 1)
    own_copies = []
    early = depth // 4

    def send_own(item):
        source, target = (
            (eg_hbm.at[0], gate_w.at[1]),
            (eu_hbm.at[0, pl.ds(0, early)], up_w.at[1, pl.ds(0, early)]),
            (eu_hbm.at[0, pl.ds(early, depth - early)], up_w.at[1, pl.ds(early, depth - early)]),
            (ed_hbm.at[0], down_w.at[pl.ds(units, units)]),
        )[item]
        own_copies.append(remote(source, target, own_send.at[item], own_recv.at[item], holder))

    send_own(0)
    send_own(1)
    sh_copies = []
    middle = depth // 2

    def send_shared(item):
        source, target, device = (
            (gu_w.at[0, pl.ds(0, middle)], gu_w.at[1, pl.ds(0, middle)], mate),
            (gu_w.at[0, pl.ds(middle, middle)], gu_w.at[1, pl.ds(middle, middle)], mate),
            (sd_w.at[pl.ds(0, sd_rows)], sd_w.at[pl.ds(sd_rows, sd_rows)], mate),
            (gu_w.at[0], gu_w.at[2], holder),
            (gu_w.at[1], gu_w.at[3], holder),
            (sd_w.at[pl.ds(0, 2 * sd_rows)], sd_w.at[pl.ds(2 * sd_rows, 2 * sd_rows)], holder),
        )[item]
        sh_copies.append(remote(source, target, sh_send.at[item], sh_recv.at[item], device))

    def packed(total):
        return sum(total[h * DV : (h + 1) * DV] for h in range(heads))

    total = sums_f[0]
    through_f = decay_f[0]
    for block in range(1, blocks):
        total = total * decay_f[block] + sums_f[block]
        through_f = through_f * decay_f[block]
    state_f = packed(total)
    total = sums_b[blocks - 1]
    through_b = decay_b[blocks - 1]
    for block in range(blocks - 2, -1, -1):
        total = total * decay_b[block] + sums_b[block]
        through_b = through_b * decay_b[block]
    state_b = packed(total)

    def put_state(ref, first, second, through_first, through_second):
        ref[0:piece] = first.astype(jnp.bfloat16)
        ref[piece : 2 * piece] = second.astype(jnp.bfloat16)
        high = [t.astype(jnp.bfloat16).astype(jnp.float32) for t in (through_first, through_second)]
        ref[2 * piece : 2 * piece + 8] = jnp.concatenate(
            [
                high[0],
                through_first - high[0],
                high[1],
                through_second - high[1],
                jnp.zeros((4, lanes), jnp.float32),
            ],
            axis=0,
        ).astype(jnp.bfloat16)

    def get_state(ref, index):
        block = ref[index].astype(jnp.float32)
        cut = 2 * piece
        return (
            block[0:piece],
            block[piece:cut],
            block[cut : cut + 1] + block[cut + 1 : cut + 2],
            block[cut + 2 : cut + 3] + block[cut + 3 : cut + 4],
        )

    for p in range(PLANE):
        cut = slice(p * piece, (p + 1) * piece)
        put_state(near_out.at[p], state_f[cut], state_b[cut], through_f, through_b)
    near_copies = []
    for step in range(1, PLANE):
        target = lax.rem(p_me + step, PLANE)
        near_copies.append(
            remote(
                near_out.at[target],
                near_in.at[p_me],
                near_send.at[step],
                near_recv.at[step],
                (z_me * PLANE + target, tp_me),
            )
        )
    near_in[p_me] = near_out[p_me]

    query_f, query_b = [], []

    def within(block):
        rows = pl.ds(block * BLK, BLK)
        queries = rotated(q_ref[rows, :], block) * KEY_CHANNELS ** (-0.5)
        keys = key_ref[rows, :]
        total_f, total_b = cumul_f[block], cumul_b[block]
        middle_f = total_f[BLK // 2 - 1 : BLK // 2]
        middle_b = total_b[BLK // 2 : BLK // 2 + 1]
        scaled_qf = queries * jnp.exp(total_f - middle_f)
        scaled_qb = queries * jnp.exp(total_b - middle_b)
        scaled_kf = (keys * jnp.exp(middle_f - total_f)).astype(jnp.bfloat16)
        scaled_kb = (keys * jnp.exp(middle_b - total_b)).astype(jnp.bfloat16)
        query_f.append((queries * jnp.exp(total_f)).astype(jnp.bfloat16))
        query_b.append((queries * jnp.exp(total_b)).astype(jnp.bfloat16))
        for h in range(heads):
            mine = lane_head == h
            scores_f = dot_nt(jnp.where(mine, scaled_qf, 0.0).astype(jnp.bfloat16), scaled_kf)
            scores_b = dot_nt(jnp.where(mine, scaled_qb, 0.0).astype(jnp.bfloat16), scaled_kb)
            scores = jnp.where(lower, scores_f, 0.0) + jnp.where(upper, scores_b, 0.0)
            within_ref[rows, h * DV : (h + 1) * DV] = jnp.dot(
                scores.astype(jnp.bfloat16),
                v_ref[rows, h * DV : (h + 1) * DV],
                preferred_element_type=jnp.float32,
            )

    third = blocks // 3
    for block in range(third):
        within(block)
    for copy in near_copies:
        copy.wait()

    def fold(orders, visit):
        state = jnp.zeros((piece, lanes), jnp.float32)
        through = jnp.ones((1, lanes), jnp.float32)
        first = orders[0] == 0
        for p in orders:
            visit(p, state, through)
            fwd_state, bwd_state, fwd_through, bwd_through = get_state(near_in, p)
            state = state * (fwd_through if first else bwd_through) + (
                fwd_state if first else bwd_state
            )
            through = through * (fwd_through if first else bwd_through)
        return state, through

    ahead = list(range(PLANE))
    behind = ahead[::-1]
    plane_f, plane_df = fold(ahead, lambda p, state, through: None)
    plane_b, plane_db = fold(behind, lambda p, state, through: None)
    put_state(far_out, plane_f, plane_b, plane_df, plane_db)
    far_copies = []
    for step in range(1, planes):
        target = lax.rem(z_me + step, planes)
        far_copies.append(
            remote(
                far_out,
                far_in.at[z_me],
                far_send.at[step],
                far_recv.at[step],
                (target * PLANE + p_me, tp_me),
            )
        )
    far_in[z_me] = far_out[...]
    for block in range(third, blocks - third):
        within(block)
    for copy in far_copies:
        copy.wait()
    enter_f = jnp.zeros((piece, lanes), jnp.float32)
    enter_b = jnp.zeros((piece, lanes), jnp.float32)
    for z in range(planes):
        plane_state, _, plane_through, _ = get_state(far_in, z)
        enter_f = jnp.where(z < z_me, enter_f * plane_through + plane_state, enter_f)
    for z in range(planes - 1, -1, -1):
        _, plane_state, _, plane_through = get_state(far_in, z)
        enter_b = jnp.where(z > z_me, enter_b * plane_through + plane_state, enter_b)

    def emit_f(p, state, through):
        carry_out[p, 0:piece] = (enter_f * through + state).astype(jnp.bfloat16)

    def emit_b(p, state, through):
        carry_out[p, piece : 2 * piece] = (enter_b * through + state).astype(jnp.bfloat16)

    fold(ahead, emit_f)
    fold(behind, emit_b)
    carry_copies = []
    for step in range(1, PLANE):
        target = lax.rem(p_me + step, PLANE)
        carry_copies.append(
            remote(
                carry_out.at[target],
                carry_in.at[p_me],
                carry_send.at[step],
                carry_recv.at[step],
                (z_me * PLANE + target, tp_me),
            )
        )
    carry_in[p_me] = carry_out[p_me]
    for block in range(blocks - third, blocks):
        within(block)
    for copy in carry_copies:
        copy.wait()

    def unpacked(first):
        carry = jnp.concatenate(
            [carry_in[p, first : first + piece].astype(jnp.float32) for p in range(PLANE)], axis=0
        )
        return jnp.where(own_head, jnp.concatenate([carry] * heads, axis=0), 0.0)

    state = unpacked(0)
    for block in range(blocks):
        rows = pl.ds(block * BLK, BLK)
        within_ref[rows, :] += dot_nt(query_f[block], state.astype(jnp.bfloat16))
        if block < blocks - 1:
            state = state * decay_f[block] + sums_f[block]
    state = unpacked(piece)
    for block in range(blocks - 1, -1, -1):
        rows = pl.ds(block * BLK, BLK)
        attended = within_ref[rows, :] + dot_nt(query_b[block], state.astype(jnp.bfloat16))
        if block > 0:
            state = state * decay_b[block] + sums_b[block]
        for h in range(heads):
            part = attended[:, h * DV : (h + 1) * DV]
            square = jnp.mean(part * part, axis=-1, keepdims=True)
            gate = gate_ref[rows, h * DV : (h + 1) * DV].astype(jnp.float32)
            mixed_ref[rows, h * DV : (h + 1) * DV] = (
                part
                * lax.rsqrt(square + EPS)
                * gain_ref[:, h * DV : (h + 1) * DV]
                * (gate / (1.0 + jnp.exp(-gate)))
            ).astype(jnp.bfloat16)

    row_copies = []
    for step in range(1, tp_count):
        target = lax.rem(tp_me + step, tp_count)
        row_copies.append(
            remote(
                mixed_ref.at[pl.ds(pl.multiple_of(target * rows_out, rows_out), rows_out)],
                land_ref.at[tp_me],
                row_send.at[step],
                row_recv.at[step],
                (sp_me, target),
            )
        )
    send_own(2)
    send_own(3)
    land_ref[tp_me] = mixed_ref[pl.ds(pl.multiple_of(tp_me * rows_out, rows_out), rows_out), :]

    def iota(shape, axis):
        return lax.broadcasted_iota(jnp.int32, shape, axis)

    square_shape = (rows_out, rows_out)
    eye = (iota(square_shape, 0) == iota(square_shape, 1)).astype(jnp.float32)
    columns = lax.dot_general(
        eye,
        jnp.concatenate(
            [
                route_ref[...].astype(jnp.float32),
                weight_ref[...],
                jnp.zeros((8 - 2 * TOPK, rows_out), jnp.float32),
            ],
            axis=0,
        ),
        (((1,), (1,)), ((), ())),
        precision=TOP_PRECISION,
        preferred_element_type=jnp.float32,
    )
    named = [columns[:, k : k + 1] for k in range(TOPK)]
    weights = [columns[:, TOPK + k : TOPK + k + 1] for k in range(TOPK)]
    expert_lane = iota((rows_out, 128), 1).astype(jnp.float32)
    onehot = [(named[k] == expert_lane).astype(jnp.float32) for k in range(TOPK)]
    earlier = (iota(square_shape, 0) > iota(square_shape, 1)).astype(jnp.bfloat16)
    every = jnp.ones(square_shape, jnp.bfloat16)
    slot_lane = iota((rows_out, sp_count * 8), 1).astype(jnp.float32)
    seen = jnp.zeros((rows_out, 128), jnp.float32)
    mains, tails, thirds = [], [], []
    for k in range(TOPK):
        hot = onehot[k].astype(jnp.bfloat16)
        before = seen + jnp.dot(earlier, hot, preferred_element_type=jnp.float32)
        seen = seen + jnp.dot(every, hot, preferred_element_type=jnp.float32)
        rank = jnp.sum(before * onehot[k], axis=1, keepdims=True)
        over = jnp.where(rank >= 3.0, 1.0, 0.0)
        mains.append(named[k] * 8.0 + rank == slot_lane)
        tails.append(named[k] * 8.0 + 6.0 + over == slot_lane)
        thirds.append(rank - 3.0 * over)

    def tail_hit(k, b):
        return jnp.logical_and(tails[k], thirds[k] == b)

    def chosen(first, second):
        return jnp.where(jnp.logical_or(first, second), 1.0, 0.0).astype(jnp.bfloat16)

    local[3].wait()
    for copy in row_copies:
        copy.wait()
    mixed_all = jnp.concatenate([land_ref[source] for source in range(tp_count)], axis=1)
    projected = jnp.dot(mixed_all, proj_w[...], preferred_element_type=jnp.float32)
    residual = (
        stream_ref[...].astype(jnp.float32) + normalize(projected) * mix_gain_ref[...]
    ).astype(jnp.bfloat16)
    resid_ref[...] = residual
    normed = (normalize(residual.astype(jnp.float32)) * ffn_gain_ref[...]).astype(jnp.bfloat16)
    normed_ref[...] = normed
    pick_main = chosen(mains[0], mains[1])
    for b in range(3):
        picks = jnp.concatenate([pick_main, chosen(tail_hit(0, b), tail_hit(1, b))], axis=0)
        source = jnp.concatenate(
            [normed[:, b * quarter : (b + 1) * quarter], normed[:, 3 * quarter :]], axis=0
        )
        outgoing_ref[:, :, b * quarter : (b + 1) * quarter] = (
            dot_tn(picks, source).reshape(sp_count, 8, quarter).astype(jnp.bfloat16)
        )
    def exchange(source_ref, source_of, target_ref, send, recv, way):
        copies = []
        for turn in range(PLANE):
            if way == 0 and turn == 0:
                continue
            target = lax.rem(z_me + way, planes) * PLANE + lax.rem(p_me + turn, PLANE)
            copies.append(
                remote(
                    source_ref.at[source_of(target)],
                    target_ref.at[sp_me],
                    send.at[way, turn],
                    recv.at[way, turn],
                    (target, tp_me),
                )
            )
        return copies

    block_copies = [
        exchange(outgoing_ref, lambda target: target, arrived_ref, block_send, block_recv, way)
        for way in ways
    ]
    arrived_ref[sp_me] = outgoing_ref[sp_me]
    pair_copy = remote(normed_ref, pair_in, pair_send.at[0], pair_recv.at[0], (pair, tp_me))

    group = PLANE * 8
    spot = iota((group, group), 0)
    origin = iota((group, group), 1)
    same = spot // 8 == origin // 8

    def spread(target, source, b):
        rank = lax.rem(target, 8)
        hit = jnp.logical_and(rank < 6, lax.rem(rank, 3) == b)
        hit = jnp.logical_and(hit, lax.rem(source, 8) == 6 + rank // 3)
        return jnp.where(jnp.logical_and(same, hit), 1.0, 0.0).astype(jnp.bfloat16)

    scatter = [spread(spot, origin, b) for b in range(3)]
    gather = [spread(origin, spot, b) for b in range(3)]

    def sources(index):
        plane = lax.rem(z_me + planes - ways[index], planes)
        return pl.ds(pl.multiple_of(plane * PLANE, PLANE), PLANE)

    def unpack(ref, side, index):
        cut = slice(index * group, (index + 1) * group)
        tail = jnp.zeros((group, quarter), jnp.float32)
        for b in range(3):
            block = ref[sources(index), :, b * quarter : (b + 1) * quarter].reshape(group, quarter)
            rows_ref[side, cut, b * quarter : (b + 1) * quarter] = block
            tail = tail + jnp.dot(scatter[b], block, preferred_element_type=jnp.float32)
        rows_ref[side, cut, 3 * quarter :] = tail.astype(jnp.bfloat16)

    total_rows = sp_count * 8

    def hidden_of(side, part, shard):
        rows = rows_ref[side, part]
        hidden_ref[side, part, shard * units : (shard + 1) * units] = (
            jax.nn.silu(jnp.dot(rows, gate_w[shard], preferred_element_type=jnp.float32))
            * jnp.dot(rows, up_w[shard], preferred_element_type=jnp.float32)
        ).astype(jnp.bfloat16)

    def finish(side, part, target_ref):
        count = part.stop - part.start
        hidden = hidden_ref[side, part]
        keep = lax.rem(iota((count, quarter), 0), 8) < 6
        last = jnp.dot(
            hidden, down_w[:, 3 * quarter :], preferred_element_type=jnp.float32
        ).astype(jnp.bfloat16)
        for b in range(3):
            value = jnp.dot(
                hidden,
                down_w[:, b * quarter : (b + 1) * quarter],
                preferred_element_type=jnp.float32,
            )
            moved = jnp.concatenate(
                [
                    jnp.dot(
                        gather[b], last[start : start + group], preferred_element_type=jnp.float32
                    )
                    for start in range(0, count, group)
                ],
                axis=0,
            )
            target_ref[part.start // 8 : part.stop // 8, :, b * quarter : (b + 1) * quarter] = (
                jnp.where(keep, value, moved).reshape(count // 8, 8, quarter).astype(jnp.bfloat16)
            )

    back_copies, lend_copies, give_copies = [], [], []
    batches = [slice(0, total_rows // 2), slice(total_rows // 2, total_rows)]

    def lend(chunks):
        for index in chunks:
            for copy in block_copies[index]:
                copy.wait()
            lend_copies.append(
                remote(
                    arrived_ref.at[sources(index)],
                    lent_ref.at[sources(index)],
                    lend_send.at[index],
                    lend_recv.at[index],
                    mate,
                )
            )
            unpack(arrived_ref, 0, index)

    def work_lent(chunks, part, spare):
        for index in chunks:
            lend_copies[index].wait()
            unpack(lent_ref, 1, index)
        send_shared(spare)
        hidden_of(1, part, 0)
        hidden_of(1, part, 1)
        finish(1, part, lent_out)
        for index in chunks:
            cut = pl.ds(index * PLANE, PLANE)
            give_copies.append(
                remote(
                    lent_out.at[cut],
                    lent_back.at[cut],
                    give_send.at[index],
                    give_recv.at[index],
                    mate,
                )
            )

    def work_kept(part):
        hidden_of(0, part, 0)
        hidden_of(0, part, 1)
        finish(0, part, kept_ref)

    def give_back(chunks):
        for index in chunks:
            cut = slice(index * PLANE, (index + 1) * PLANE)
            give_copies[index].wait()
            done_ref[sources(index)] = (
                kept_ref[cut].astype(jnp.float32) + lent_back[cut].astype(jnp.float32)
            ).astype(jnp.bfloat16)
            back_copies.extend(
                exchange(
                    done_ref,
                    lambda target: target,
                    back_ref,
                    back_send,
                    back_recv,
                    (planes - ways[index]) % planes,
                )
            )

    near_half, far_half = range(planes // 2), range(planes // 2, planes)
    lend(near_half)
    for copy in local[4:] + own_copies:
        copy.wait()
    work_lent(near_half, batches[0], 0)
    lend(far_half[:2])
    work_kept(batches[0])
    lend(far_half[2:])
    give_back(near_half)
    work_lent(far_half, batches[1], 1)
    send_shared(2)
    work_kept(batches[1])
    give_back(far_half)
    send_shared(3)
    for copy in sh_copies[:3]:
        copy.wait()
    send_shared(4)
    send_shared(5)
    back_ref[sp_me] = done_ref[sp_me]

    def split(hits):
        full = jnp.where(hits[0], weights[0], 0.0) + jnp.where(hits[1], weights[1], 0.0)
        high = full.astype(jnp.bfloat16)
        return [high, (full - high.astype(jnp.float32)).astype(jnp.bfloat16)]

    main_split = split(mains)
    sides = [
        jnp.concatenate(main_split + split([tail_hit(0, b), tail_hit(1, b)]), axis=0)
        for b in range(3)
    ]
    for copy in back_copies:
        copy.wait()
    tail = jnp.zeros((rows_out, quarter), jnp.float32)
    for b in range(3):
        block = back_ref[:, :, b * quarter : (b + 1) * quarter].reshape(sp_count * 8, quarter)
        value = jnp.dot(sides[b], block, preferred_element_type=jnp.float32)
        mixture_ref[:, b * quarter : (b + 1) * quarter] = (
            value[0:rows_out] + value[rows_out : 2 * rows_out]
        )
        tail = tail + value[2 * rows_out : 3 * rows_out] + value[3 * rows_out :]
    mixture_ref[:, 3 * quarter :] = tail

    pair_copy.wait()
    sh_copies[3].wait()
    sh_copies[4].wait()
    tokens = jnp.concatenate([normed_ref[...], pair_in[...]], axis=0)
    lane = iota((2 * rows_out, 2 * sd_rows), 1)
    units_of = []
    for slot in range(tp_count):
        both = jnp.dot(tokens, gu_w[slot], preferred_element_type=jnp.float32)
        units_of.append(jax.nn.silu(both) * pltpu.roll(both, sd_rows, 1))
    hidden = jnp.concatenate(
        [
            jnp.where(lane < sd_rows, units_of[s], pltpu.roll(units_of[s + 1], sd_rows, 1))
            for s in range(0, tp_count, 2)
        ],
        axis=1,
    ).astype(jnp.bfloat16)
    sh_copies[5].wait()
    part_out[...] = jnp.dot(
        hidden[rows_out:], sd_w[...], preferred_element_type=jnp.float32
    ).astype(jnp.bfloat16)
    part_copy = remote(part_out, part_in, pair_send.at[1], pair_recv.at[1], (pair, tp_me))
    mixture_ref[...] += jnp.dot(hidden[:rows_out], sd_w[...], preferred_element_type=jnp.float32)
    part_copy.wait()
    mixture = mixture_ref[...] + part_in[...].astype(jnp.float32)
    square = jnp.mean(mixture * mixture, axis=-1, keepdims=True)
    out_ref[...] = (
        resid_ref[...].astype(jnp.float32)
        + mixture * lax.rsqrt(square + EPS) * moe_gain_ref[...]
    ).astype(out_ref.dtype)


def fused(vmem_args, hbm_args):
    sp_count = lax.axis_size("sp")
    tp_count = lax.axis_size("tp")
    queries, _, values = vmem_args[:3]
    stream = vmem_args[9]
    _, expert_gate, _, expert_down, shared_gate, _, shared_down = hbm_args
    span, lanes = queries.shape
    width = values.shape[1]
    rows_out = span // tp_count
    blocks = span // BLK
    planes = sp_count // PLANE
    piece = DV // PLANE
    model = stream.shape[1]
    units = expert_gate.shape[2]
    vmem = pl.BlockSpec(memory_space=pltpu.VMEM)
    hbm = pl.BlockSpec(memory_space=pl.ANY)
    bf16, f32 = jnp.bfloat16, jnp.float32
    packets = pltpu.VMEM((sp_count, 8, 3 * model // 4), bf16)
    tokens = pltpu.VMEM(stream.shape, bf16)
    dma = pltpu.SemaphoreType.DMA
    return pl.pallas_call(
        functools.partial(fused_kernel, sp_count, tp_count),
        out_shape=jax.ShapeDtypeStruct(stream.shape, stream.dtype),
        in_specs=[vmem] * len(vmem_args) + [hbm] * len(hbm_args),
        out_specs=vmem,
        scratch_shapes=[
            pltpu.VMEM((span, width), bf16),
            pltpu.VMEM((tp_count, rows_out, width), bf16),
            pltpu.VMEM((span, width), f32),
            pltpu.VMEM((span, lanes), f32),
            pltpu.VMEM((blocks, width, lanes), f32),
            pltpu.VMEM((blocks, width, lanes), f32),
            pltpu.VMEM((PLANE, 2 * piece + 8, lanes), bf16),
            pltpu.VMEM((PLANE, 2 * piece + 8, lanes), bf16),
            pltpu.VMEM((2 * piece + 8, lanes), bf16),
            pltpu.VMEM((planes, 2 * piece + 8, lanes), bf16),
            pltpu.VMEM((PLANE, 2 * piece, lanes), bf16),
            pltpu.VMEM((PLANE, 2 * piece, lanes), bf16),
            pltpu.VMEM((tp_count * width, model), bf16),
            pltpu.VMEM((2, model, units), bf16),
            pltpu.VMEM((2, model, units), bf16),
            pltpu.VMEM((2 * units, model), bf16),
            pltpu.VMEM(shared_gate.shape, bf16),
            pltpu.VMEM(shared_gate.shape, bf16),
            pltpu.VMEM((tp_count,) + shared_gate.shape, bf16),
            pltpu.VMEM((tp_count * shared_down.shape[0] // 2, model), bf16),
            tokens,
            tokens,
            packets,
            packets,
            packets,
            pltpu.VMEM((2, sp_count * 8, model), bf16),
            pltpu.VMEM((2, sp_count * 8, 2 * units), bf16),
            packets,
            packets,
            packets,
            packets,
            packets,
            tokens,
            tokens,
            tokens,
            pltpu.VMEM(stream.shape, f32),
            dma((7,)),
            dma((PLANE,)),
            dma((PLANE,)),
            dma((planes,)),
            dma((planes,)),
            dma((PLANE,)),
            dma((PLANE,)),
            dma((tp_count,)),
            dma((tp_count,)),
            dma((4,)),
            dma((4,)),
            dma((6,)),
            dma((6,)),
            dma((planes,)),
            dma((planes,)),
            dma((planes,)),
            dma((planes,)),
            dma((planes, PLANE)),
            dma((planes, PLANE)),
            dma((planes, PLANE)),
            dma((planes, PLANE)),
            dma((2,)),
            dma((2,)),
        ],
        compiler_params=pltpu.CompilerParams(
            collective_id=0, has_side_effects=True, vmem_limit_bytes=60 * 1024 * 1024
        ),
    )(*vmem_args, *hbm_args)


def body(
    stream,
    queries,
    key_rows,
    values,
    out_gate,
    fwd_decay,
    bwd_decay,
    head_gain,
    out_proj,
    mix_gain,
    ffn_gain,
    moe_gain,
    routes,
    route_weight,
    expert_gate,
    expert_up,
    expert_down,
    shared_gate,
    shared_up,
    shared_down,
):
    span_rows, lanes = queries.shape
    offset = lax.axis_index("sp") * span_rows
    positions = jnp.concatenate(
        [
            offset + jnp.arange(0, span_rows, BLK, dtype=jnp.int32),
            jnp.arange(BLK, dtype=jnp.int32),
        ]
    ).astype(jnp.float32)
    half = KEY_CHANNELS // 2
    lane = jnp.arange(lanes, dtype=jnp.int32) % KEY_CHANNELS
    frequency = ROPE_BASE ** (-(lane % half).astype(jnp.float32) / half)
    angles = positions[:, None] * frequency[None, :]
    return fused(
        (
            queries,
            key_rows,
            values,
            out_gate,
            fwd_decay,
            bwd_decay,
            jnp.cos(angles),
            jnp.sin(angles),
            head_gain.reshape(1, -1),
            stream,
            mix_gain.reshape(1, -1),
            ffn_gain.reshape(1, -1),
            moe_gain.reshape(1, -1),
            routes.T,
            route_weight.T,
        ),
        (out_proj, expert_gate, expert_up, expert_down, shared_gate, shared_up, shared_down),
    )


def solution(mesh):
    return jax.shard_map(
        body,
        mesh=mesh,
        in_specs=(
            P(("sp", "tp"), None),
            P("sp", "tp"),
            P("sp", "tp"),
            P("sp", "tp"),
            P("sp", "tp"),
            P("sp", "tp"),
            P("sp", "tp"),
            P("tp"),
            P(),
            P(),
            P(),
            P(),
            P(("sp", "tp"), None),
            P(("sp", "tp"), None),
            P("sp", None, "tp"),
            P("sp", None, "tp"),
            P("sp", "tp", None),
            P(None, "tp"),
            P(None, "tp"),
            P("tp", None),
        ),
        out_specs=P(("sp", "tp"), None),
        check_vma=False,
    )
```

```python
import functools

import jax
import jax.numpy as jnp
import numpy as np
from jax import lax
from jax.experimental import pallas as pl
from jax.experimental.pallas import tpu as pltpu
from jax.sharding import PartitionSpec as P

KEY_CHANNELS = 64
DV = 128
BLK = 64
TOPK = 2
PLANE = 8


EPS = 1e-06
GATE_NORM = 16.0
ROPE_BASE = 10000.0
TOP_PRECISION = lax.Precision.HIGHEST
MESH = pl.DeviceIdType.MESH


def normalize(tensor):
    return tensor * lax.rsqrt(jnp.mean(tensor * tensor, axis=-1, keepdims=True) + EPS)


def dot_nt(left, right):
    return lax.dot_general(
        left, right, (((1,), (1,)), ((), ())), preferred_element_type=jnp.float32
    )


def dot_tn(left, right):
    return lax.dot_general(
        left, right, (((0,), (0,)), ((), ())), preferred_element_type=jnp.float32
    )


def fused_kernel(
    sp_count,
    tp_count,
    rate_ref,
    gain_ref,
    mix_gain_ref,
    ffn_gain_ref,
    moe_gain_ref,
    route_ref,
    weight_ref,
    k_hbm,
    v_hbm,
    fwd_hbm,
    bwd_hbm,
    q_hbm,
    gate_hbm,
    stream_hbm,
    proj_hbm,
    eg_hbm,
    eu_hbm,
    ed_hbm,
    sg_hbm,
    su_hbm,
    sd_hbm,
    out_ref,
    mixed_ref,
    land_ref,
    within_ref,
    key_ref,
    sums_f,
    sums_b,
    near_out,
    near_in,
    far_out,
    far_in,
    carry_out,
    carry_in,
    proj_w,
    gate_w,
    up_w,
    down_w,
    sg_ref,
    su_ref,
    gu_w,
    sd_w,
    resid_ref,
    normed_ref,
    outgoing_ref,
    arrived_ref,
    lent_ref,
    rows_ref,
    hidden_ref,
    lent_out,
    lent_back,
    kept_ref,
    done_ref,
    back_ref,
    pair_in,
    part_out,
    part_in,
    mixture_ref,
    cos_ref,
    sin_ref,
    k_ref,
    v_ref,
    fwd_ref,
    bwd_ref,
    q_ref,
    gate_ref,
    stream_ref,
    input_sem,
    local_sem,
    near_send,
    near_recv,
    far_send,
    far_recv,
    carry_send,
    carry_recv,
    row_send,
    row_recv,
    own_send,
    own_recv,
    sh_send,
    sh_recv,
    lend_send,
    lend_recv,
    give_send,
    give_recv,
    block_send,
    block_recv,
    back_send,
    back_recv,
    pair_send,
    pair_recv,
):
    span, lanes = q_ref.shape
    width = v_ref.shape[1]
    heads = lanes // KEY_CHANNELS
    blocks = span // BLK
    rows_out = span // tp_count
    planes = sp_count // PLANE
    piece = DV // PLANE
    model = stream_ref.shape[1]
    quarter = model // 4
    units = eg_hbm.shape[2]
    depth = eg_hbm.shape[1]
    sp_me = lax.axis_index("sp")
    tp_me = lax.axis_index("tp")
    z_me = sp_me // PLANE
    p_me = lax.rem(sp_me, PLANE)
    pair = sp_me + 1 - 2 * lax.rem(sp_me, 2)
    core = lax.rem(sp_me, 2)
    flip = tp_me + 1 - 2 * lax.rem(tp_me, 2)
    mirror = tp_count - 1 - tp_me
    holder = (sp_me, jnp.where(core == 0, flip, mirror))
    mate = (sp_me, jnp.where(core == 0, mirror, flip))
    ways = [0, planes // 2, 1, planes - 1]
    for step in range(planes // 2 - 1, 1, -1):
        ways += [step, planes - step]

    inputs = []
    for index, (source, target) in enumerate(
        (
            (k_hbm, k_ref),
            (v_hbm, v_ref),
            (fwd_hbm, fwd_ref),
            (bwd_hbm, bwd_ref),
            (q_hbm, q_ref),
            (gate_hbm, gate_ref),
            (stream_hbm, stream_ref),
        )
    ):
        copy = pltpu.make_async_copy(source, target, input_sem.at[index])
        copy.start()
        inputs.append(copy)

    barrier = pltpu.get_barrier_semaphore()
    for step in range(1, sp_count):
        pl.semaphore_signal(
            barrier,
            inc=1,
            device_id=(lax.rem(sp_me + step, sp_count), tp_me),
            device_id_type=MESH,
        )
    for step in range(1, tp_count):
        pl.semaphore_signal(
            barrier,
            inc=1,
            device_id=(sp_me, lax.rem(tp_me + step, tp_count)),
            device_id_type=MESH,
        )

    def remote(source, target, send, recv, device):
        copy = pltpu.make_async_remote_copy(
            src_ref=source,
            dst_ref=target,
            send_sem=send,
            recv_sem=recv,
            device_id=device,
            device_id_type=MESH,
        )
        copy.start()
        return copy

    sd_rows = sd_hbm.shape[0] // 2
    local = []
    for index, (source, target) in enumerate(
        (
            (sg_hbm, sg_ref),
            (su_hbm, su_ref),
            (
                sd_hbm.at[pl.ds(pl.multiple_of(core * sd_rows, sd_rows), sd_rows)],
                sd_w.at[pl.ds(0, sd_rows)],
            ),
            (proj_hbm, proj_w),
            (eg_hbm.at[0], gate_w.at[0]),
            (eu_hbm.at[0], up_w.at[0]),
            (ed_hbm.at[0], down_w.at[pl.ds(0, units)]),
        )
    ):
        copy = pltpu.make_async_copy(source, target, local_sem.at[index])
        copy.start()
        local.append(copy)

    row = lax.broadcasted_iota(jnp.int32, (BLK, BLK), 0)
    column = lax.broadcasted_iota(jnp.int32, (BLK, BLK), 1)
    lower = row >= column
    upper = row <= column
    lower_ones = lower.astype(jnp.float32)
    upper_ones = upper.astype(jnp.float32)
    from_lane = lax.broadcasted_iota(jnp.int32, (lanes, lanes), 0)
    to_lane = lax.broadcasted_iota(jnp.int32, (lanes, lanes), 1)
    half = KEY_CHANNELS // 2
    partner = jnp.where(lax.rem(to_lane, KEY_CHANNELS) < half, to_lane + half, to_lane - half)
    swap = (from_lane == partner).astype(jnp.bfloat16)
    own_head = (
        lax.broadcasted_iota(jnp.int32, (width, lanes), 0) // DV
        == lax.broadcasted_iota(jnp.int32, (width, lanes), 1) // KEY_CHANNELS
    )
    lane_head = lax.broadcasted_iota(jnp.int32, (BLK, lanes), 1) // KEY_CHANNELS

    lane_low = lax.rem(lax.broadcasted_iota(jnp.int32, (BLK, lanes), 1), KEY_CHANNELS) < half

    table = (blocks + BLK, lanes)
    place = lax.broadcasted_iota(jnp.int32, table, 0)
    position = jnp.where(place < blocks, sp_me * span + place * BLK, place - blocks)
    angles = position.astype(jnp.float32) * rate_ref[...]
    cos_ref[...] = jnp.cos(angles)
    sin_ref[...] = jnp.sin(angles)

    def rotated(tensor, block):
        swapped = jnp.dot(tensor, swap, preferred_element_type=jnp.float32)
        cos_block, sin_block = cos_ref[block : block + 1], sin_ref[block : block + 1]
        cos_row, sin_row = cos_ref[blocks : blocks + BLK], sin_ref[blocks : blocks + BLK]
        cosine = cos_block * cos_row - sin_block * sin_row
        sine = sin_block * cos_row + cos_block * sin_row
        return tensor.astype(jnp.float32) * cosine + swapped * jnp.where(lane_low, -sine, sine)

    for copy in inputs[:4]:
        copy.wait()
    cumul_f, cumul_b, decay_f, decay_b = [], [], [], []
    for block in range(blocks):
        rows = pl.ds(block * BLK, BLK)
        total_f = jnp.dot(
            lower_ones,
            jax.nn.log_sigmoid(fwd_ref[rows, :]) / GATE_NORM,
            precision=TOP_PRECISION,
            preferred_element_type=jnp.float32,
        )
        total_b = jnp.dot(
            upper_ones,
            jax.nn.log_sigmoid(bwd_ref[rows, :]) / GATE_NORM,
            precision=TOP_PRECISION,
            preferred_element_type=jnp.float32,
        )
        last_f = total_f[BLK - 1 : BLK]
        last_b = total_b[0:1]
        keys = rotated(k_ref[rows, :], block)
        key_ref[rows, :] = keys
        value_rows = v_ref[rows, :]
        out_f = (keys * jnp.exp(last_f - total_f)).astype(jnp.bfloat16)
        out_b = (keys * jnp.exp(last_b - total_b)).astype(jnp.bfloat16)
        sums_f[block] = jnp.where(own_head, dot_tn(value_rows, out_f), 0.0)
        sums_b[block] = jnp.where(own_head, dot_tn(value_rows, out_b), 0.0)
        cumul_f.append(total_f)
        cumul_b.append(total_b)
        decay_f.append(jnp.exp(last_f))
        decay_b.append(jnp.exp(last_b))

    local[0].wait()
    local[1].wait()
    local[2].wait()
    shared_low = lax.broadcasted_iota(jnp.int32, sg_ref.shape, 1) < sd_rows
    gate_rows = sg_ref[...].astype(jnp.float32)
    up_rows = su_ref[...].astype(jnp.float32)
    first = jnp.where(core == 0, gate_rows, pltpu.roll(gate_rows, sd_rows, 1))
    second = jnp.where(core == 0, pltpu.roll(up_rows, sd_rows, 1), up_rows)
    gu_w[0] = jnp.where(shared_low, first, second).astype(jnp.bfloat16)

    pl.semaphore_wait(barrier, sp_count - 1 + tp_count - 1)
    own_copies = []
    early = depth // 4

    def send_own(item):
        source, target = (
            (eg_hbm.at[0], gate_w.at[1]),
            (eu_hbm.at[0, pl.ds(0, early)], up_w.at[1, pl.ds(0, early)]),
            (eu_hbm.at[0, pl.ds(early, depth - early)], up_w.at[1, pl.ds(early, depth - early)]),
            (ed_hbm.at[0], down_w.at[pl.ds(units, units)]),
        )[item]
        own_copies.append(remote(source, target, own_send.at[item], own_recv.at[item], holder))

    send_own(0)
    send_own(1)
    sh_copies = []
    middle = depth // 2

    def send_shared(item):
        source, target, device = (
            (gu_w.at[0, pl.ds(0, middle)], gu_w.at[1, pl.ds(0, middle)], mate),
            (gu_w.at[0, pl.ds(middle, middle)], gu_w.at[1, pl.ds(middle, middle)], mate),
            (sd_w.at[pl.ds(0, sd_rows)], sd_w.at[pl.ds(sd_rows, sd_rows)], mate),
            (gu_w.at[0], gu_w.at[2], holder),
            (gu_w.at[1], gu_w.at[3], holder),
            (sd_w.at[pl.ds(0, 2 * sd_rows)], sd_w.at[pl.ds(2 * sd_rows, 2 * sd_rows)], holder),
        )[item]
        sh_copies.append(remote(source, target, sh_send.at[item], sh_recv.at[item], device))

    def packed(total):
        return sum(total[h * DV : (h + 1) * DV] for h in range(heads))

    total = sums_f[0]
    through_f = decay_f[0]
    for block in range(1, blocks):
        total = total * decay_f[block] + sums_f[block]
        through_f = through_f * decay_f[block]
    state_f = packed(total)
    total = sums_b[blocks - 1]
    through_b = decay_b[blocks - 1]
    for block in range(blocks - 2, -1, -1):
        total = total * decay_b[block] + sums_b[block]
        through_b = through_b * decay_b[block]
    state_b = packed(total)

    def put_state(ref, first, second, through_first, through_second):
        ref[0:piece] = first.astype(jnp.bfloat16)
        ref[piece : 2 * piece] = second.astype(jnp.bfloat16)
        high = [t.astype(jnp.bfloat16).astype(jnp.float32) for t in (through_first, through_second)]
        ref[2 * piece : 2 * piece + 8] = jnp.concatenate(
            [
                high[0],
                through_first - high[0],
                high[1],
                through_second - high[1],
                jnp.zeros((4, lanes), jnp.float32),
            ],
            axis=0,
        ).astype(jnp.bfloat16)

    def get_state(ref, index):
        block = ref[index].astype(jnp.float32)
        cut = 2 * piece
        return (
            block[0:piece],
            block[piece:cut],
            block[cut : cut + 1] + block[cut + 1 : cut + 2],
            block[cut + 2 : cut + 3] + block[cut + 3 : cut + 4],
        )

    for p in range(PLANE):
        cut = slice(p * piece, (p + 1) * piece)
        put_state(near_out.at[p], state_f[cut], state_b[cut], through_f, through_b)
    near_copies = []
    for step in range(1, PLANE):
        target = lax.rem(p_me + step, PLANE)
        near_copies.append(
            remote(
                near_out.at[target],
                near_in.at[p_me],
                near_send.at[step],
                near_recv.at[step],
                (z_me * PLANE + target, tp_me),
            )
        )
    near_in[p_me] = near_out[p_me]

    query_f, query_b = [], []

    def within(block):
        rows = pl.ds(block * BLK, BLK)
        queries = rotated(q_ref[rows, :], block) * KEY_CHANNELS ** (-0.5)
        keys = key_ref[rows, :]
        total_f, total_b = cumul_f[block], cumul_b[block]
        middle_f = total_f[BLK // 2 - 1 : BLK // 2]
        middle_b = total_b[BLK // 2 : BLK // 2 + 1]
        scaled_qf = queries * jnp.exp(total_f - middle_f)
        scaled_qb = queries * jnp.exp(total_b - middle_b)
        scaled_kf = (keys * jnp.exp(middle_f - total_f)).astype(jnp.bfloat16)
        scaled_kb = (keys * jnp.exp(middle_b - total_b)).astype(jnp.bfloat16)
        query_f.append((queries * jnp.exp(total_f)).astype(jnp.bfloat16))
        query_b.append((queries * jnp.exp(total_b)).astype(jnp.bfloat16))
        for h in range(heads):
            mine = lane_head == h
            scores_f = dot_nt(jnp.where(mine, scaled_qf, 0.0).astype(jnp.bfloat16), scaled_kf)
            scores_b = dot_nt(jnp.where(mine, scaled_qb, 0.0).astype(jnp.bfloat16), scaled_kb)
            scores = jnp.where(lower, scores_f, 0.0) + jnp.where(upper, scores_b, 0.0)
            within_ref[rows, h * DV : (h + 1) * DV] = jnp.dot(
                scores.astype(jnp.bfloat16),
                v_ref[rows, h * DV : (h + 1) * DV],
                preferred_element_type=jnp.float32,
            )

    for copy in inputs[4:]:
        copy.wait()
    third = blocks // 3
    for block in range(third):
        within(block)
    for copy in near_copies:
        copy.wait()

    def fold(orders, visit):
        state = jnp.zeros((piece, lanes), jnp.float32)
        through = jnp.ones((1, lanes), jnp.float32)
        first = orders[0] == 0
        for p in orders:
            visit(p, state, through)
            fwd_state, bwd_state, fwd_through, bwd_through = get_state(near_in, p)
            state = state * (fwd_through if first else bwd_through) + (
                fwd_state if first else bwd_state
            )
            through = through * (fwd_through if first else bwd_through)
        return state, through

    ahead = list(range(PLANE))
    behind = ahead[::-1]
    plane_f, plane_df = fold(ahead, lambda p, state, through: None)
    plane_b, plane_db = fold(behind, lambda p, state, through: None)
    put_state(far_out, plane_f, plane_b, plane_df, plane_db)
    far_copies = []
    for step in range(1, planes):
        target = lax.rem(z_me + step, planes)
        far_copies.append(
            remote(
                far_out,
                far_in.at[z_me],
                far_send.at[step],
                far_recv.at[step],
                (target * PLANE + p_me, tp_me),
            )
        )
    far_in[z_me] = far_out[...]
    for block in range(third, blocks - third):
        within(block)
    for copy in far_copies:
        copy.wait()
    enter_f = jnp.zeros((piece, lanes), jnp.float32)
    enter_b = jnp.zeros((piece, lanes), jnp.float32)
    for z in range(planes):
        plane_state, _, plane_through, _ = get_state(far_in, z)
        enter_f = jnp.where(z < z_me, enter_f * plane_through + plane_state, enter_f)
    for z in range(planes - 1, -1, -1):
        _, plane_state, _, plane_through = get_state(far_in, z)
        enter_b = jnp.where(z > z_me, enter_b * plane_through + plane_state, enter_b)

    def emit_f(p, state, through):
        carry_out[p, 0:piece] = (enter_f * through + state).astype(jnp.bfloat16)

    def emit_b(p, state, through):
        carry_out[p, piece : 2 * piece] = (enter_b * through + state).astype(jnp.bfloat16)

    fold(ahead, emit_f)
    fold(behind, emit_b)
    carry_copies = []
    for step in range(1, PLANE):
        target = lax.rem(p_me + step, PLANE)
        carry_copies.append(
            remote(
                carry_out.at[target],
                carry_in.at[p_me],
                carry_send.at[step],
                carry_recv.at[step],
                (z_me * PLANE + target, tp_me),
            )
        )
    carry_in[p_me] = carry_out[p_me]
    for block in range(blocks - third, blocks):
        within(block)
    for copy in carry_copies:
        copy.wait()

    def unpacked(first):
        carry = jnp.concatenate(
            [carry_in[p, first : first + piece].astype(jnp.float32) for p in range(PLANE)], axis=0
        )
        return jnp.where(own_head, jnp.concatenate([carry] * heads, axis=0), 0.0)

    state = unpacked(0)
    for block in range(blocks):
        rows = pl.ds(block * BLK, BLK)
        within_ref[rows, :] += dot_nt(query_f[block], state.astype(jnp.bfloat16))
        if block < blocks - 1:
            state = state * decay_f[block] + sums_f[block]
    state = unpacked(piece)
    for block in range(blocks - 1, -1, -1):
        rows = pl.ds(block * BLK, BLK)
        attended = within_ref[rows, :] + dot_nt(query_b[block], state.astype(jnp.bfloat16))
        if block > 0:
            state = state * decay_b[block] + sums_b[block]
        for h in range(heads):
            part = attended[:, h * DV : (h + 1) * DV]
            square = jnp.mean(part * part, axis=-1, keepdims=True)
            gate = gate_ref[rows, h * DV : (h + 1) * DV].astype(jnp.float32)
            mixed_ref[rows, h * DV : (h + 1) * DV] = (
                part
                * lax.rsqrt(square + EPS)
                * gain_ref[:, h * DV : (h + 1) * DV]
                * (gate / (1.0 + jnp.exp(-gate)))
            ).astype(jnp.bfloat16)

    row_copies = []
    for step in range(1, tp_count):
        target = lax.rem(tp_me + step, tp_count)
        row_copies.append(
            remote(
                mixed_ref.at[pl.ds(pl.multiple_of(target * rows_out, rows_out), rows_out)],
                land_ref.at[tp_me],
                row_send.at[step],
                row_recv.at[step],
                (sp_me, target),
            )
        )
    send_own(2)
    send_own(3)
    land_ref[tp_me] = mixed_ref[pl.ds(pl.multiple_of(tp_me * rows_out, rows_out), rows_out), :]

    def iota(shape, axis):
        return lax.broadcasted_iota(jnp.int32, shape, axis)

    square_shape = (rows_out, rows_out)
    eye = (iota(square_shape, 0) == iota(square_shape, 1)).astype(jnp.float32)
    columns = lax.dot_general(
        eye,
        jnp.concatenate(
            [
                route_ref[...].astype(jnp.float32),
                weight_ref[...],
                jnp.zeros((8 - 2 * TOPK, rows_out), jnp.float32),
            ],
            axis=0,
        ),
        (((1,), (1,)), ((), ())),
        precision=TOP_PRECISION,
        preferred_element_type=jnp.float32,
    )
    named = [columns[:, k : k + 1] for k in range(TOPK)]
    weights = [columns[:, TOPK + k : TOPK + k + 1] for k in range(TOPK)]
    expert_lane = iota((rows_out, 128), 1).astype(jnp.float32)
    onehot = [(named[k] == expert_lane).astype(jnp.float32) for k in range(TOPK)]
    earlier = (iota(square_shape, 0) > iota(square_shape, 1)).astype(jnp.bfloat16)
    every = jnp.ones(square_shape, jnp.bfloat16)
    slot_lane = iota((rows_out, sp_count * 8), 1).astype(jnp.float32)
    seen = jnp.zeros((rows_out, 128), jnp.float32)
    mains, tails, thirds = [], [], []
    for k in range(TOPK):
        hot = onehot[k].astype(jnp.bfloat16)
        before = seen + jnp.dot(earlier, hot, preferred_element_type=jnp.float32)
        seen = seen + jnp.dot(every, hot, preferred_element_type=jnp.float32)
        rank = jnp.sum(before * onehot[k], axis=1, keepdims=True)
        over = jnp.where(rank >= 3.0, 1.0, 0.0)
        mains.append(named[k] * 8.0 + rank == slot_lane)
        tails.append(named[k] * 8.0 + 6.0 + over == slot_lane)
        thirds.append(rank - 3.0 * over)

    def tail_hit(k, b):
        return jnp.logical_and(tails[k], thirds[k] == b)

    def chosen(first, second):
        return jnp.where(jnp.logical_or(first, second), 1.0, 0.0).astype(jnp.bfloat16)

    local[3].wait()
    for copy in row_copies:
        copy.wait()
    mixed_all = jnp.concatenate([land_ref[source] for source in range(tp_count)], axis=1)
    projected = jnp.dot(mixed_all, proj_w[...], preferred_element_type=jnp.float32)
    residual = (
        stream_ref[...].astype(jnp.float32) + normalize(projected) * mix_gain_ref[...]
    ).astype(jnp.bfloat16)
    resid_ref[...] = residual
    normed = (normalize(residual.astype(jnp.float32)) * ffn_gain_ref[...]).astype(jnp.bfloat16)
    normed_ref[...] = normed
    pick_main = chosen(mains[0], mains[1])
    for b in range(3):
        picks = jnp.concatenate([pick_main, chosen(tail_hit(0, b), tail_hit(1, b))], axis=0)
        source = jnp.concatenate(
            [normed[:, b * quarter : (b + 1) * quarter], normed[:, 3 * quarter :]], axis=0
        )
        outgoing_ref[:, :, b * quarter : (b + 1) * quarter] = (
            dot_tn(picks, source).reshape(sp_count, 8, quarter).astype(jnp.bfloat16)
        )
    def exchange(source_ref, source_of, target_ref, send, recv, way):
        copies = []
        for turn in range(PLANE):
            if way == 0 and turn == 0:
                continue
            target = lax.rem(z_me + way, planes) * PLANE + lax.rem(p_me + turn, PLANE)
            copies.append(
                remote(
                    source_ref.at[source_of(target)],
                    target_ref.at[sp_me],
                    send.at[way, turn],
                    recv.at[way, turn],
                    (target, tp_me),
                )
            )
        return copies

    block_copies = [
        exchange(outgoing_ref, lambda target: target, arrived_ref, block_send, block_recv, way)
        for way in ways
    ]
    arrived_ref[sp_me] = outgoing_ref[sp_me]
    pair_copy = remote(normed_ref, pair_in, pair_send.at[0], pair_recv.at[0], (pair, tp_me))

    group = PLANE * 8
    spot = iota((group, group), 0)
    origin = iota((group, group), 1)
    same = spot // 8 == origin // 8

    def spread(target, source, b):
        rank = lax.rem(target, 8)
        hit = jnp.logical_and(rank < 6, lax.rem(rank, 3) == b)
        hit = jnp.logical_and(hit, lax.rem(source, 8) == 6 + rank // 3)
        return jnp.where(jnp.logical_and(same, hit), 1.0, 0.0).astype(jnp.bfloat16)

    scatter = [spread(spot, origin, b) for b in range(3)]
    gather = [spread(origin, spot, b) for b in range(3)]

    def sources(index):
        plane = lax.rem(z_me + planes - ways[index], planes)
        return pl.ds(pl.multiple_of(plane * PLANE, PLANE), PLANE)

    def unpack(ref, side, index):
        cut = slice(index * group, (index + 1) * group)
        tail = jnp.zeros((group, quarter), jnp.float32)
        for b in range(3):
            block = ref[sources(index), :, b * quarter : (b + 1) * quarter].reshape(group, quarter)
            rows_ref[side, cut, b * quarter : (b + 1) * quarter] = block
            tail = tail + jnp.dot(scatter[b], block, preferred_element_type=jnp.float32)
        rows_ref[side, cut, 3 * quarter :] = tail.astype(jnp.bfloat16)

    total_rows = sp_count * 8

    def hidden_of(side, part, shard):
        rows = rows_ref[side, part]
        hidden_ref[side, part, shard * units : (shard + 1) * units] = (
            jax.nn.silu(jnp.dot(rows, gate_w[shard], preferred_element_type=jnp.float32))
            * jnp.dot(rows, up_w[shard], preferred_element_type=jnp.float32)
        ).astype(jnp.bfloat16)

    def finish(side, part, target_ref):
        count = part.stop - part.start
        hidden = hidden_ref[side, part]
        keep = lax.rem(iota((count, quarter), 0), 8) < 6
        last = jnp.dot(
            hidden, down_w[:, 3 * quarter :], preferred_element_type=jnp.float32
        ).astype(jnp.bfloat16)
        for b in range(3):
            value = jnp.dot(
                hidden,
                down_w[:, b * quarter : (b + 1) * quarter],
                preferred_element_type=jnp.float32,
            )
            moved = jnp.concatenate(
                [
                    jnp.dot(
                        gather[b], last[start : start + group], preferred_element_type=jnp.float32
                    )
                    for start in range(0, count, group)
                ],
                axis=0,
            )
            target_ref[part.start // 8 : part.stop // 8, :, b * quarter : (b + 1) * quarter] = (
                jnp.where(keep, value, moved).reshape(count // 8, 8, quarter).astype(jnp.bfloat16)
            )

    back_copies, lend_copies, give_copies = [], [], []
    batches = [slice(0, total_rows // 2), slice(total_rows // 2, total_rows)]

    def lend(chunks):
        for index in chunks:
            for copy in block_copies[index]:
                copy.wait()
            lend_copies.append(
                remote(
                    arrived_ref.at[sources(index)],
                    lent_ref.at[sources(index)],
                    lend_send.at[index],
                    lend_recv.at[index],
                    mate,
                )
            )
            unpack(arrived_ref, 0, index)

    def take_lent(chunks):
        for index in chunks:
            lend_copies[index].wait()
            unpack(lent_ref, 1, index)

    def give(chunks, part):
        finish(1, part, lent_out)
        for index in chunks:
            cut = pl.ds(index * PLANE, PLANE)
            give_copies.append(
                remote(
                    lent_out.at[cut],
                    lent_back.at[cut],
                    give_send.at[index],
                    give_recv.at[index],
                    mate,
                )
            )

    def give_back(chunks):
        for index in chunks:
            cut = slice(index * PLANE, (index + 1) * PLANE)
            give_copies[index].wait()
            done_ref[sources(index)] = (
                kept_ref[cut].astype(jnp.float32) + lent_back[cut].astype(jnp.float32)
            ).astype(jnp.bfloat16)
            back_copies.extend(
                exchange(
                    done_ref,
                    lambda target: target,
                    back_ref,
                    back_send,
                    back_recv,
                    (planes - ways[index]) % planes,
                )
            )

    near_half, far_half = range(planes // 2), range(planes // 2, planes)
    lend(near_half)
    send_shared(0)
    for copy in local[4:]:
        copy.wait()
    hidden_of(0, batches[0], 0)
    take_lent(near_half)
    hidden_of(1, batches[0], 0)
    for copy in own_copies[:3]:
        copy.wait()
    hidden_of(1, batches[0], 1)
    own_copies[3].wait()
    give(near_half, batches[0])
    lend(far_half[:2])
    hidden_of(0, batches[0], 1)
    finish(0, batches[0], kept_ref)
    lend(far_half[2:])
    send_shared(1)
    give_back(near_half)
    for step in range(2):
        chunks = far_half[2 * step : 2 * step + 2]
        part = slice(chunks[0] * group, (chunks[-1] + 1) * group)
        take_lent(chunks)
        hidden_of(1, part, 0)
        hidden_of(1, part, 1)
        give(chunks, part)
    send_shared(2)
    hidden_of(0, batches[1], 0)
    hidden_of(0, batches[1], 1)
    finish(0, batches[1], kept_ref)
    give_back(far_half)
    send_shared(3)
    for copy in sh_copies[:3]:
        copy.wait()
    send_shared(4)
    send_shared(5)
    back_ref[sp_me] = done_ref[sp_me]

    def split(hits):
        full = jnp.where(hits[0], weights[0], 0.0) + jnp.where(hits[1], weights[1], 0.0)
        high = full.astype(jnp.bfloat16)
        return [high, (full - high.astype(jnp.float32)).astype(jnp.bfloat16)]

    main_split = split(mains)
    sides = [
        jnp.concatenate(main_split + split([tail_hit(0, b), tail_hit(1, b)]), axis=0)
        for b in range(3)
    ]
    for copy in back_copies:
        copy.wait()
    tail = jnp.zeros((rows_out, quarter), jnp.float32)
    for b in range(3):
        block = back_ref[:, :, b * quarter : (b + 1) * quarter].reshape(sp_count * 8, quarter)
        value = jnp.dot(sides[b], block, preferred_element_type=jnp.float32)
        mixture_ref[:, b * quarter : (b + 1) * quarter] = (
            value[0:rows_out] + value[rows_out : 2 * rows_out]
        )
        tail = tail + value[2 * rows_out : 3 * rows_out] + value[3 * rows_out :]
    mixture_ref[:, 3 * quarter :] = tail

    pair_copy.wait()
    sh_copies[3].wait()
    sh_copies[4].wait()
    tokens = jnp.concatenate([normed_ref[...], pair_in[...]], axis=0)
    lane = iota((2 * rows_out, 2 * sd_rows), 1)
    units_of = []
    for slot in range(tp_count):
        both = jnp.dot(tokens, gu_w[slot], preferred_element_type=jnp.float32)
        units_of.append(jax.nn.silu(both) * pltpu.roll(both, sd_rows, 1))
    hidden = jnp.concatenate(
        [
            jnp.where(lane < sd_rows, units_of[s], pltpu.roll(units_of[s + 1], sd_rows, 1))
            for s in range(0, tp_count, 2)
        ],
        axis=1,
    ).astype(jnp.bfloat16)
    sh_copies[5].wait()
    part_out[...] = jnp.dot(
        hidden[rows_out:], sd_w[...], preferred_element_type=jnp.float32
    ).astype(jnp.bfloat16)
    part_copy = remote(part_out, part_in, pair_send.at[1], pair_recv.at[1], (pair, tp_me))
    mixture_ref[...] += jnp.dot(hidden[:rows_out], sd_w[...], preferred_element_type=jnp.float32)
    part_copy.wait()
    mixture = mixture_ref[...] + part_in[...].astype(jnp.float32)
    square = jnp.mean(mixture * mixture, axis=-1, keepdims=True)
    out_ref[...] = (
        resid_ref[...].astype(jnp.float32)
        + mixture * lax.rsqrt(square + EPS) * moe_gain_ref[...]
    ).astype(out_ref.dtype)


def fused(vmem_args, hbm_args):
    sp_count = lax.axis_size("sp")
    tp_count = lax.axis_size("tp")
    queries, values, stream = hbm_args[4], hbm_args[1], hbm_args[6]
    expert_gate, expert_down, shared_gate, shared_down = (hbm_args[i] for i in (8, 10, 11, 13))
    span, lanes = queries.shape
    width = values.shape[1]
    rows_out = span // tp_count
    blocks = span // BLK
    planes = sp_count // PLANE
    piece = DV // PLANE
    model = stream.shape[1]
    units = expert_gate.shape[2]
    vmem = pl.BlockSpec(memory_space=pltpu.VMEM)
    hbm = pl.BlockSpec(memory_space=pl.ANY)
    bf16, f32 = jnp.bfloat16, jnp.float32
    packets = pltpu.VMEM((sp_count, 8, 3 * model // 4), bf16)
    tokens = pltpu.VMEM(stream.shape, bf16)
    dma = pltpu.SemaphoreType.DMA
    return pl.pallas_call(
        functools.partial(fused_kernel, sp_count, tp_count),
        out_shape=jax.ShapeDtypeStruct(stream.shape, stream.dtype),
        in_specs=[vmem] * len(vmem_args) + [hbm] * len(hbm_args),
        out_specs=vmem,
        scratch_shapes=[
            pltpu.VMEM((span, width), bf16),
            pltpu.VMEM((tp_count, rows_out, width), bf16),
            pltpu.VMEM((span, width), f32),
            pltpu.VMEM((span, lanes), f32),
            pltpu.VMEM((blocks, width, lanes), f32),
            pltpu.VMEM((blocks, width, lanes), f32),
            pltpu.VMEM((PLANE, 2 * piece + 8, lanes), bf16),
            pltpu.VMEM((PLANE, 2 * piece + 8, lanes), bf16),
            pltpu.VMEM((2 * piece + 8, lanes), bf16),
            pltpu.VMEM((planes, 2 * piece + 8, lanes), bf16),
            pltpu.VMEM((PLANE, 2 * piece, lanes), bf16),
            pltpu.VMEM((PLANE, 2 * piece, lanes), bf16),
            pltpu.VMEM((tp_count * width, model), bf16),
            pltpu.VMEM((2, model, units), bf16),
            pltpu.VMEM((2, model, units), bf16),
            pltpu.VMEM((2 * units, model), bf16),
            pltpu.VMEM(shared_gate.shape, bf16),
            pltpu.VMEM(shared_gate.shape, bf16),
            pltpu.VMEM((tp_count,) + shared_gate.shape, bf16),
            pltpu.VMEM((tp_count * shared_down.shape[0] // 2, model), bf16),
            tokens,
            tokens,
            packets,
            packets,
            packets,
            pltpu.VMEM((2, sp_count * 8, model), bf16),
            pltpu.VMEM((2, sp_count * 8, 2 * units), bf16),
            packets,
            packets,
            packets,
            packets,
            packets,
            tokens,
            tokens,
            tokens,
            pltpu.VMEM(stream.shape, f32),
            pltpu.VMEM((blocks + BLK, lanes), f32),
            pltpu.VMEM((blocks + BLK, lanes), f32),
            pltpu.VMEM(queries.shape, bf16),
            pltpu.VMEM(values.shape, bf16),
            pltpu.VMEM(queries.shape, f32),
            pltpu.VMEM(queries.shape, f32),
            pltpu.VMEM(queries.shape, bf16),
            pltpu.VMEM(values.shape, bf16),
            tokens,
            dma((7,)),
            dma((7,)),
            dma((PLANE,)),
            dma((PLANE,)),
            dma((planes,)),
            dma((planes,)),
            dma((PLANE,)),
            dma((PLANE,)),
            dma((tp_count,)),
            dma((tp_count,)),
            dma((4,)),
            dma((4,)),
            dma((6,)),
            dma((6,)),
            dma((planes,)),
            dma((planes,)),
            dma((planes,)),
            dma((planes,)),
            dma((planes, PLANE)),
            dma((planes, PLANE)),
            dma((planes, PLANE)),
            dma((planes, PLANE)),
            dma((2,)),
            dma((2,)),
        ],
        compiler_params=pltpu.CompilerParams(
            collective_id=0, has_side_effects=True, vmem_limit_bytes=60 * 1024 * 1024
        ),
    )(*vmem_args, *hbm_args)


def body(
    stream,
    queries,
    key_rows,
    values,
    out_gate,
    fwd_decay,
    bwd_decay,
    head_gain,
    out_proj,
    mix_gain,
    ffn_gain,
    moe_gain,
    routes,
    route_weight,
    expert_gate,
    expert_up,
    expert_down,
    shared_gate,
    shared_up,
    shared_down,
):
    half = KEY_CHANNELS // 2
    rates = ROPE_BASE ** (-(np.arange(queries.shape[1]) % half) / half)
    return fused(
        (
            jnp.asarray(rates.astype(np.float32).reshape(1, -1)),
            head_gain.reshape(1, -1),
            mix_gain.reshape(1, -1),
            ffn_gain.reshape(1, -1),
            moe_gain.reshape(1, -1),
            routes.T,
            route_weight.T,
        ),
        (
            key_rows,
            values,
            fwd_decay,
            bwd_decay,
            queries,
            out_gate,
            stream,
            out_proj,
            expert_gate,
            expert_up,
            expert_down,
            shared_gate,
            shared_up,
            shared_down,
        ),
    )


def solution(mesh):
    return jax.shard_map(
        body,
        mesh=mesh,
        in_specs=(
            P(("sp", "tp"), None),
            P("sp", "tp"),
            P("sp", "tp"),
            P("sp", "tp"),
            P("sp", "tp"),
            P("sp", "tp"),
            P("sp", "tp"),
            P("tp"),
            P(),
            P(),
            P(),
            P(),
            P(("sp", "tp"), None),
            P(("sp", "tp"), None),
            P("sp", None, "tp"),
            P("sp", None, "tp"),
            P("sp", "tp", None),
            P(None, "tp"),
            P(None, "tp"),
            P("tp", None),
        ),
        out_specs=P(("sp", "tp"), None),
        check_vma=False,
    )
```

```python
import functools

import jax
import jax.numpy as jnp
import numpy as np
from jax import lax
from jax.experimental import pallas as pl
from jax.experimental.pallas import tpu as pltpu
from jax.sharding import PartitionSpec as P

KEY_CHANNELS = 64
DV = 128
BLK = 64
TOPK = 2
PLANE = 8


EPS = 1e-06
GATE_NORM = 16.0
ROPE_BASE = 10000.0
TOP_PRECISION = lax.Precision.HIGHEST
MESH = pl.DeviceIdType.MESH


def normalize(tensor):
    return tensor * lax.rsqrt(jnp.mean(tensor * tensor, axis=-1, keepdims=True) + EPS)


def dot_nt(left, right):
    return lax.dot_general(
        left, right, (((1,), (1,)), ((), ())), preferred_element_type=jnp.float32
    )


def dot_tn(left, right):
    return lax.dot_general(
        left, right, (((0,), (0,)), ((), ())), preferred_element_type=jnp.float32
    )


def fused_kernel(
    sp_count,
    tp_count,
    rate_ref,
    gain_ref,
    mix_gain_ref,
    ffn_gain_ref,
    moe_gain_ref,
    route_ref,
    weight_ref,
    k_hbm,
    v_hbm,
    fwd_hbm,
    bwd_hbm,
    q_hbm,
    gate_hbm,
    stream_hbm,
    proj_hbm,
    eg_hbm,
    eu_hbm,
    ed_hbm,
    sg_hbm,
    su_hbm,
    sd_hbm,
    out_ref,
    mixed_ref,
    land_ref,
    within_ref,
    key_ref,
    sums_f,
    sums_b,
    near_out,
    near_in,
    far_out,
    far_in,
    carry_out,
    carry_in,
    proj_w,
    gate_w,
    up_w,
    down_w,
    sg_ref,
    su_ref,
    gu_w,
    sd_w,
    resid_ref,
    normed_ref,
    outgoing_ref,
    arrived_ref,
    lent_ref,
    rows_ref,
    hidden_ref,
    lent_out,
    lent_back,
    kept_ref,
    done_ref,
    back_ref,
    pair_in,
    part_out,
    part_in,
    mixture_ref,
    cos_ref,
    sin_ref,
    k_ref,
    v_ref,
    fwd_ref,
    bwd_ref,
    q_ref,
    gate_ref,
    stream_ref,
    input_sem,
    local_sem,
    near_send,
    near_recv,
    far_send,
    far_recv,
    carry_send,
    carry_recv,
    row_send,
    row_recv,
    own_send,
    own_recv,
    sh_send,
    sh_recv,
    lend_send,
    lend_recv,
    give_send,
    give_recv,
    block_send,
    block_recv,
    back_send,
    back_recv,
    pair_send,
    pair_recv,
):
    span, lanes = q_ref.shape
    width = v_ref.shape[1]
    heads = lanes // KEY_CHANNELS
    blocks = span // BLK
    rows_out = span // tp_count
    planes = sp_count // PLANE
    piece = DV // PLANE
    model = stream_ref.shape[1]
    quarter = model // 4
    units = eg_hbm.shape[2]
    depth = eg_hbm.shape[1]
    sp_me = lax.axis_index("sp")
    tp_me = lax.axis_index("tp")
    z_me = sp_me // PLANE
    p_me = lax.rem(sp_me, PLANE)
    pair = sp_me + 1 - 2 * lax.rem(sp_me, 2)
    core = lax.rem(sp_me, 2)
    flip = tp_me + 1 - 2 * lax.rem(tp_me, 2)
    mirror = tp_count - 1 - tp_me
    holder = (sp_me, jnp.where(core == 0, flip, mirror))
    mate = (sp_me, jnp.where(core == 0, mirror, flip))
    ways = [0, planes // 2, 1, planes - 1]
    for step in range(planes // 2 - 1, 1, -1):
        ways += [step, planes - step]

    inputs = []
    for index, (source, target) in enumerate(
        (
            (k_hbm, k_ref),
            (v_hbm, v_ref),
            (fwd_hbm, fwd_ref),
            (bwd_hbm, bwd_ref),
            (q_hbm, q_ref),
            (gate_hbm, gate_ref),
            (stream_hbm, stream_ref),
        )
    ):
        copy = pltpu.make_async_copy(source, target, input_sem.at[index])
        copy.start()
        inputs.append(copy)

    barrier = pltpu.get_barrier_semaphore()
    for step in range(1, sp_count):
        pl.semaphore_signal(
            barrier,
            inc=1,
            device_id=(lax.rem(sp_me + step, sp_count), tp_me),
            device_id_type=MESH,
        )
    for step in range(1, tp_count):
        pl.semaphore_signal(
            barrier,
            inc=1,
            device_id=(sp_me, lax.rem(tp_me + step, tp_count)),
            device_id_type=MESH,
        )

    def remote(source, target, send, recv, device):
        copy = pltpu.make_async_remote_copy(
            src_ref=source,
            dst_ref=target,
            send_sem=send,
            recv_sem=recv,
            device_id=device,
            device_id_type=MESH,
        )
        copy.start()
        return copy

    sd_rows = sd_hbm.shape[0] // 2
    local = []
    for index, (source, target) in enumerate(
        (
            (sg_hbm, sg_ref),
            (su_hbm, su_ref),
            (
                sd_hbm.at[pl.ds(pl.multiple_of(core * sd_rows, sd_rows), sd_rows)],
                sd_w.at[pl.ds(0, sd_rows)],
            ),
            (proj_hbm, proj_w),
            (eg_hbm.at[0], gate_w.at[0]),
            (eu_hbm.at[0], up_w.at[0]),
            (ed_hbm.at[0], down_w.at[pl.ds(0, units)]),
        )
    ):
        copy = pltpu.make_async_copy(source, target, local_sem.at[index])
        copy.start()
        local.append(copy)

    row = lax.broadcasted_iota(jnp.int32, (BLK, BLK), 0)
    column = lax.broadcasted_iota(jnp.int32, (BLK, BLK), 1)
    lower = row >= column
    upper = row <= column
    lower_ones = lower.astype(jnp.float32)
    upper_ones = upper.astype(jnp.float32)
    from_lane = lax.broadcasted_iota(jnp.int32, (lanes, lanes), 0)
    to_lane = lax.broadcasted_iota(jnp.int32, (lanes, lanes), 1)
    half = KEY_CHANNELS // 2
    partner = jnp.where(lax.rem(to_lane, KEY_CHANNELS) < half, to_lane + half, to_lane - half)
    swap = (from_lane == partner).astype(jnp.bfloat16)
    own_head = (
        lax.broadcasted_iota(jnp.int32, (width, lanes), 0) // DV
        == lax.broadcasted_iota(jnp.int32, (width, lanes), 1) // KEY_CHANNELS
    )
    lane_head = lax.broadcasted_iota(jnp.int32, (BLK, lanes), 1) // KEY_CHANNELS

    lane_low = lax.rem(lax.broadcasted_iota(jnp.int32, (BLK, lanes), 1), KEY_CHANNELS) < half

    table = (blocks + BLK, lanes)
    place = lax.broadcasted_iota(jnp.int32, table, 0)
    position = jnp.where(place < blocks, sp_me * span + place * BLK, place - blocks)
    angles = position.astype(jnp.float32) * rate_ref[...]
    cos_ref[...] = jnp.cos(angles)
    sin_ref[...] = jnp.sin(angles)

    def rotated(tensor, block):
        swapped = jnp.dot(tensor, swap, preferred_element_type=jnp.float32)
        cos_block, sin_block = cos_ref[block : block + 1], sin_ref[block : block + 1]
        cos_row, sin_row = cos_ref[blocks : blocks + BLK], sin_ref[blocks : blocks + BLK]
        cosine = cos_block * cos_row - sin_block * sin_row
        sine = sin_block * cos_row + cos_block * sin_row
        return tensor.astype(jnp.float32) * cosine + swapped * jnp.where(lane_low, -sine, sine)

    for copy in inputs[:4]:
        copy.wait()
    cumul_f, cumul_b, decay_f, decay_b = [], [], [], []
    for block in range(blocks):
        rows = pl.ds(block * BLK, BLK)
        total_f = jnp.dot(
            lower_ones,
            jax.nn.log_sigmoid(fwd_ref[rows, :]) / GATE_NORM,
            precision=TOP_PRECISION,
            preferred_element_type=jnp.float32,
        )
        total_b = jnp.dot(
            upper_ones,
            jax.nn.log_sigmoid(bwd_ref[rows, :]) / GATE_NORM,
            precision=TOP_PRECISION,
            preferred_element_type=jnp.float32,
        )
        last_f = total_f[BLK - 1 : BLK]
        last_b = total_b[0:1]
        keys = rotated(k_ref[rows, :], block)
        key_ref[rows, :] = keys
        value_rows = v_ref[rows, :]
        out_f = (keys * jnp.exp(last_f - total_f)).astype(jnp.bfloat16)
        out_b = (keys * jnp.exp(last_b - total_b)).astype(jnp.bfloat16)
        sums_f[block] = jnp.where(own_head, dot_tn(value_rows, out_f), 0.0)
        sums_b[block] = jnp.where(own_head, dot_tn(value_rows, out_b), 0.0)
        cumul_f.append(total_f)
        cumul_b.append(total_b)
        decay_f.append(jnp.exp(last_f))
        decay_b.append(jnp.exp(last_b))

    local[0].wait()
    local[1].wait()
    local[2].wait()
    shared_low = lax.broadcasted_iota(jnp.int32, sg_ref.shape, 1) < sd_rows
    gate_rows = sg_ref[...].astype(jnp.float32)
    up_rows = su_ref[...].astype(jnp.float32)
    first = jnp.where(core == 0, gate_rows, pltpu.roll(gate_rows, sd_rows, 1))
    second = jnp.where(core == 0, pltpu.roll(up_rows, sd_rows, 1), up_rows)
    gu_w[0] = jnp.where(shared_low, first, second).astype(jnp.bfloat16)

    pl.semaphore_wait(barrier, sp_count - 1 + tp_count - 1)
    own_copies = []
    early = depth // 4

    def send_own(item):
        source, target = (
            (eg_hbm.at[0], gate_w.at[1]),
            (eu_hbm.at[0, pl.ds(0, early)], up_w.at[1, pl.ds(0, early)]),
            (eu_hbm.at[0, pl.ds(early, depth - early)], up_w.at[1, pl.ds(early, depth - early)]),
            (ed_hbm.at[0], down_w.at[pl.ds(units, units)]),
        )[item]
        own_copies.append(remote(source, target, own_send.at[item], own_recv.at[item], holder))

    send_own(0)
    send_own(1)
    sh_copies = []
    middle = depth // 2

    def send_shared(item):
        source, target, device = (
            (gu_w.at[0, pl.ds(0, middle)], gu_w.at[1, pl.ds(0, middle)], mate),
            (gu_w.at[0, pl.ds(middle, middle)], gu_w.at[1, pl.ds(middle, middle)], mate),
            (sd_w.at[pl.ds(0, sd_rows)], sd_w.at[pl.ds(sd_rows, sd_rows)], mate),
            (gu_w.at[0], gu_w.at[2], holder),
            (gu_w.at[1], gu_w.at[3], holder),
            (sd_w.at[pl.ds(0, 2 * sd_rows)], sd_w.at[pl.ds(2 * sd_rows, 2 * sd_rows)], holder),
        )[item]
        sh_copies.append(remote(source, target, sh_send.at[item], sh_recv.at[item], device))

    def packed(total):
        return sum(total[h * DV : (h + 1) * DV] for h in range(heads))

    total = sums_f[0]
    through_f = decay_f[0]
    for block in range(1, blocks):
        total = total * decay_f[block] + sums_f[block]
        through_f = through_f * decay_f[block]
    state_f = packed(total)
    total = sums_b[blocks - 1]
    through_b = decay_b[blocks - 1]
    for block in range(blocks - 2, -1, -1):
        total = total * decay_b[block] + sums_b[block]
        through_b = through_b * decay_b[block]
    state_b = packed(total)

    def put_state(ref, first, second, through_first, through_second):
        ref[0:piece] = first.astype(jnp.bfloat16)
        ref[piece : 2 * piece] = second.astype(jnp.bfloat16)
        high = [t.astype(jnp.bfloat16).astype(jnp.float32) for t in (through_first, through_second)]
        ref[2 * piece : 2 * piece + 8] = jnp.concatenate(
            [
                high[0],
                through_first - high[0],
                high[1],
                through_second - high[1],
                jnp.zeros((4, lanes), jnp.float32),
            ],
            axis=0,
        ).astype(jnp.bfloat16)

    def get_state(ref, index):
        block = ref[index].astype(jnp.float32)
        cut = 2 * piece
        return (
            block[0:piece],
            block[piece:cut],
            block[cut : cut + 1] + block[cut + 1 : cut + 2],
            block[cut + 2 : cut + 3] + block[cut + 3 : cut + 4],
        )

    for p in range(PLANE):
        cut = slice(p * piece, (p + 1) * piece)
        put_state(near_out.at[p], state_f[cut], state_b[cut], through_f, through_b)
    near_copies = []
    for step in range(1, PLANE):
        target = lax.rem(p_me + step, PLANE)
        near_copies.append(
            remote(
                near_out.at[target],
                near_in.at[p_me],
                near_send.at[step],
                near_recv.at[step],
                (z_me * PLANE + target, tp_me),
            )
        )
    near_in[p_me] = near_out[p_me]

    query_f, query_b = [], []

    def within(block):
        rows = pl.ds(block * BLK, BLK)
        queries = rotated(q_ref[rows, :], block) * KEY_CHANNELS ** (-0.5)
        keys = key_ref[rows, :]
        total_f, total_b = cumul_f[block], cumul_b[block]
        middle_f = total_f[BLK // 2 - 1 : BLK // 2]
        middle_b = total_b[BLK // 2 : BLK // 2 + 1]
        scaled_qf = queries * jnp.exp(total_f - middle_f)
        scaled_qb = queries * jnp.exp(total_b - middle_b)
        scaled_kf = (keys * jnp.exp(middle_f - total_f)).astype(jnp.bfloat16)
        scaled_kb = (keys * jnp.exp(middle_b - total_b)).astype(jnp.bfloat16)
        query_f.append((queries * jnp.exp(total_f)).astype(jnp.bfloat16))
        query_b.append((queries * jnp.exp(total_b)).astype(jnp.bfloat16))
        for h in range(heads):
            mine = lane_head == h
            scores_f = dot_nt(jnp.where(mine, scaled_qf, 0.0).astype(jnp.bfloat16), scaled_kf)
            scores_b = dot_nt(jnp.where(mine, scaled_qb, 0.0).astype(jnp.bfloat16), scaled_kb)
            scores = jnp.where(lower, scores_f, 0.0) + jnp.where(upper, scores_b, 0.0)
            within_ref[rows, h * DV : (h + 1) * DV] = jnp.dot(
                scores.astype(jnp.bfloat16),
                v_ref[rows, h * DV : (h + 1) * DV],
                preferred_element_type=jnp.float32,
            )

    for copy in inputs[4:]:
        copy.wait()
    third = blocks // 3
    for block in range(third):
        within(block)
    for copy in near_copies:
        copy.wait()

    def fold(orders, visit):
        state = jnp.zeros((piece, lanes), jnp.float32)
        through = jnp.ones((1, lanes), jnp.float32)
        first = orders[0] == 0
        for p in orders:
            visit(p, state, through)
            fwd_state, bwd_state, fwd_through, bwd_through = get_state(near_in, p)
            state = state * (fwd_through if first else bwd_through) + (
                fwd_state if first else bwd_state
            )
            through = through * (fwd_through if first else bwd_through)
        return state, through

    ahead = list(range(PLANE))
    behind = ahead[::-1]
    plane_f, plane_df = fold(ahead, lambda p, state, through: None)
    plane_b, plane_db = fold(behind, lambda p, state, through: None)
    put_state(far_out, plane_f, plane_b, plane_df, plane_db)
    far_copies = []
    for step in range(1, planes):
        target = lax.rem(z_me + step, planes)
        far_copies.append(
            remote(
                far_out,
                far_in.at[z_me],
                far_send.at[step],
                far_recv.at[step],
                (target * PLANE + p_me, tp_me),
            )
        )
    far_in[z_me] = far_out[...]
    for block in range(third, blocks - third):
        within(block)
    for copy in far_copies:
        copy.wait()
    enter_f = jnp.zeros((piece, lanes), jnp.float32)
    enter_b = jnp.zeros((piece, lanes), jnp.float32)
    for z in range(planes):
        plane_state, _, plane_through, _ = get_state(far_in, z)
        enter_f = jnp.where(z < z_me, enter_f * plane_through + plane_state, enter_f)
    for z in range(planes - 1, -1, -1):
        _, plane_state, _, plane_through = get_state(far_in, z)
        enter_b = jnp.where(z > z_me, enter_b * plane_through + plane_state, enter_b)

    def emit_f(p, state, through):
        carry_out[p, 0:piece] = (enter_f * through + state).astype(jnp.bfloat16)

    def emit_b(p, state, through):
        carry_out[p, piece : 2 * piece] = (enter_b * through + state).astype(jnp.bfloat16)

    fold(ahead, emit_f)
    fold(behind, emit_b)
    carry_copies = []
    for step in range(1, PLANE):
        target = lax.rem(p_me + step, PLANE)
        carry_copies.append(
            remote(
                carry_out.at[target],
                carry_in.at[p_me],
                carry_send.at[step],
                carry_recv.at[step],
                (z_me * PLANE + target, tp_me),
            )
        )
    carry_in[p_me] = carry_out[p_me]
    for block in range(blocks - third, blocks):
        within(block)
    for copy in carry_copies:
        copy.wait()

    def unpacked(first):
        carry = jnp.concatenate(
            [carry_in[p, first : first + piece].astype(jnp.float32) for p in range(PLANE)], axis=0
        )
        return jnp.where(own_head, jnp.concatenate([carry] * heads, axis=0), 0.0)

    state = unpacked(0)
    for block in range(blocks):
        rows = pl.ds(block * BLK, BLK)
        within_ref[rows, :] += dot_nt(query_f[block], state.astype(jnp.bfloat16))
        if block < blocks - 1:
            state = state * decay_f[block] + sums_f[block]
    state = unpacked(piece)
    for block in range(blocks - 1, -1, -1):
        rows = pl.ds(block * BLK, BLK)
        attended = within_ref[rows, :] + dot_nt(query_b[block], state.astype(jnp.bfloat16))
        if block > 0:
            state = state * decay_b[block] + sums_b[block]
        for h in range(heads):
            part = attended[:, h * DV : (h + 1) * DV]
            square = jnp.mean(part * part, axis=-1, keepdims=True)
            gate = gate_ref[rows, h * DV : (h + 1) * DV].astype(jnp.float32)
            mixed_ref[rows, h * DV : (h + 1) * DV] = (
                part
                * lax.rsqrt(square + EPS)
                * gain_ref[:, h * DV : (h + 1) * DV]
                * (gate / (1.0 + jnp.exp(-gate)))
            ).astype(jnp.bfloat16)

    row_copies = []
    for step in (2, 1, 3):
        target = lax.rem(tp_me + step, tp_count)
        row_copies.append(
            remote(
                mixed_ref.at[pl.ds(pl.multiple_of(target * rows_out, rows_out), rows_out)],
                land_ref.at[tp_me],
                row_send.at[step],
                row_recv.at[step],
                (sp_me, target),
            )
        )
    send_own(2)
    send_own(3)
    land_ref[tp_me] = mixed_ref[pl.ds(pl.multiple_of(tp_me * rows_out, rows_out), rows_out), :]

    def iota(shape, axis):
        return lax.broadcasted_iota(jnp.int32, shape, axis)

    square_shape = (rows_out, rows_out)
    eye = (iota(square_shape, 0) == iota(square_shape, 1)).astype(jnp.float32)
    columns = lax.dot_general(
        eye,
        jnp.concatenate(
            [
                route_ref[...].astype(jnp.float32),
                weight_ref[...],
                jnp.zeros((8 - 2 * TOPK, rows_out), jnp.float32),
            ],
            axis=0,
        ),
        (((1,), (1,)), ((), ())),
        precision=TOP_PRECISION,
        preferred_element_type=jnp.float32,
    )
    named = [columns[:, k : k + 1] for k in range(TOPK)]
    weights = [columns[:, TOPK + k : TOPK + k + 1] for k in range(TOPK)]
    expert_lane = iota((rows_out, 128), 1).astype(jnp.float32)
    onehot = [(named[k] == expert_lane).astype(jnp.float32) for k in range(TOPK)]
    earlier = (iota(square_shape, 0) > iota(square_shape, 1)).astype(jnp.bfloat16)
    every = jnp.ones(square_shape, jnp.bfloat16)
    slot_lane = iota((rows_out, sp_count * 8), 1).astype(jnp.float32)
    seen = jnp.zeros((rows_out, 128), jnp.float32)
    mains, tails, thirds = [], [], []
    for k in range(TOPK):
        hot = onehot[k].astype(jnp.bfloat16)
        before = seen + jnp.dot(earlier, hot, preferred_element_type=jnp.float32)
        seen = seen + jnp.dot(every, hot, preferred_element_type=jnp.float32)
        rank = jnp.sum(before * onehot[k], axis=1, keepdims=True)
        over = jnp.where(rank >= 3.0, 1.0, 0.0)
        mains.append(named[k] * 8.0 + rank == slot_lane)
        tails.append(named[k] * 8.0 + 6.0 + over == slot_lane)
        thirds.append(rank - 3.0 * over)

    def tail_hit(k, b):
        return jnp.logical_and(tails[k], thirds[k] == b)

    def chosen(first, second):
        return jnp.where(jnp.logical_or(first, second), 1.0, 0.0).astype(jnp.bfloat16)

    local[3].wait()
    for copy in row_copies:
        copy.wait()
    mixed_all = jnp.concatenate([land_ref[source] for source in range(tp_count)], axis=1)
    projected = jnp.dot(mixed_all, proj_w[...], preferred_element_type=jnp.float32)
    residual = (
        stream_ref[...].astype(jnp.float32) + normalize(projected) * mix_gain_ref[...]
    ).astype(jnp.bfloat16)
    resid_ref[...] = residual
    normed = (normalize(residual.astype(jnp.float32)) * ffn_gain_ref[...]).astype(jnp.bfloat16)
    normed_ref[...] = normed
    pick_main = chosen(mains[0], mains[1])
    for b in range(3):
        picks = jnp.concatenate([pick_main, chosen(tail_hit(0, b), tail_hit(1, b))], axis=0)
        source = jnp.concatenate(
            [normed[:, b * quarter : (b + 1) * quarter], normed[:, 3 * quarter :]], axis=0
        )
        outgoing_ref[:, :, b * quarter : (b + 1) * quarter] = (
            dot_tn(picks, source).reshape(sp_count, 8, quarter).astype(jnp.bfloat16)
        )
    def exchange(source_ref, source_of, target_ref, send, recv, way):
        copies = []
        for turn in range(PLANE):
            if way == 0 and turn == 0:
                continue
            target = lax.rem(z_me + way, planes) * PLANE + lax.rem(p_me + turn, PLANE)
            copies.append(
                remote(
                    source_ref.at[source_of(target)],
                    target_ref.at[sp_me],
                    send.at[way, turn],
                    recv.at[way, turn],
                    (target, tp_me),
                )
            )
        return copies

    block_copies = [
        exchange(outgoing_ref, lambda target: target, arrived_ref, block_send, block_recv, way)
        for way in ways
    ]
    arrived_ref[sp_me] = outgoing_ref[sp_me]
    pair_copy = remote(normed_ref, pair_in, pair_send.at[0], pair_recv.at[0], (pair, tp_me))

    group = PLANE * 8
    spot = iota((group, group), 0)
    origin = iota((group, group), 1)
    same = spot // 8 == origin // 8

    def spread(target, source, b):
        rank = lax.rem(target, 8)
        hit = jnp.logical_and(rank < 6, lax.rem(rank, 3) == b)
        hit = jnp.logical_and(hit, lax.rem(source, 8) == 6 + rank // 3)
        return jnp.where(jnp.logical_and(same, hit), 1.0, 0.0).astype(jnp.bfloat16)

    scatter = [spread(spot, origin, b) for b in range(3)]
    gather = [spread(origin, spot, b) for b in range(3)]

    def sources(index):
        plane = lax.rem(z_me + planes - ways[index], planes)
        return pl.ds(pl.multiple_of(plane * PLANE, PLANE), PLANE)

    def unpack(ref, side, index):
        cut = slice(index * group, (index + 1) * group)
        tail = jnp.zeros((group, quarter), jnp.float32)
        for b in range(3):
            block = ref[sources(index), :, b * quarter : (b + 1) * quarter].reshape(group, quarter)
            rows_ref[side, cut, b * quarter : (b + 1) * quarter] = block
            tail = tail + jnp.dot(scatter[b], block, preferred_element_type=jnp.float32)
        rows_ref[side, cut, 3 * quarter :] = tail.astype(jnp.bfloat16)

    total_rows = sp_count * 8

    def hidden_of(side, part, shard):
        rows = rows_ref[side, part]
        hidden_ref[side, part, shard * units : (shard + 1) * units] = (
            jax.nn.silu(jnp.dot(rows, gate_w[shard], preferred_element_type=jnp.float32))
            * jnp.dot(rows, up_w[shard], preferred_element_type=jnp.float32)
        ).astype(jnp.bfloat16)

    def finish(side, part, target_ref):
        count = part.stop - part.start
        hidden = hidden_ref[side, part]
        keep = lax.rem(iota((count, quarter), 0), 8) < 6
        last = jnp.dot(
            hidden, down_w[:, 3 * quarter :], preferred_element_type=jnp.float32
        ).astype(jnp.bfloat16)
        for b in range(3):
            value = jnp.dot(
                hidden,
                down_w[:, b * quarter : (b + 1) * quarter],
                preferred_element_type=jnp.float32,
            )
            moved = jnp.concatenate(
                [
                    jnp.dot(
                        gather[b], last[start : start + group], preferred_element_type=jnp.float32
                    )
                    for start in range(0, count, group)
                ],
                axis=0,
            )
            target_ref[part.start // 8 : part.stop // 8, :, b * quarter : (b + 1) * quarter] = (
                jnp.where(keep, value, moved).reshape(count // 8, 8, quarter).astype(jnp.bfloat16)
            )

    back_copies, lend_copies, give_copies = [], [], []
    batches = [slice(0, total_rows // 2), slice(total_rows // 2, total_rows)]

    def lend(chunks):
        for index in chunks:
            for copy in block_copies[index]:
                copy.wait()
            lend_copies.append(
                remote(
                    arrived_ref.at[sources(index)],
                    lent_ref.at[sources(index)],
                    lend_send.at[index],
                    lend_recv.at[index],
                    mate,
                )
            )
            unpack(arrived_ref, 0, index)

    def take_lent(chunks):
        for index in chunks:
            lend_copies[index].wait()
            unpack(lent_ref, 1, index)

    def give(chunks, part):
        finish(1, part, lent_out)
        for index in chunks:
            cut = pl.ds(index * PLANE, PLANE)
            give_copies.append(
                remote(
                    lent_out.at[cut],
                    lent_back.at[cut],
                    give_send.at[index],
                    give_recv.at[index],
                    mate,
                )
            )

    def give_back(chunks):
        for index in chunks:
            cut = slice(index * PLANE, (index + 1) * PLANE)
            give_copies[index].wait()
            done_ref[sources(index)] = (
                kept_ref[cut].astype(jnp.float32) + lent_back[cut].astype(jnp.float32)
            ).astype(jnp.bfloat16)
            back_copies.extend(
                exchange(
                    done_ref,
                    lambda target: target,
                    back_ref,
                    back_send,
                    back_recv,
                    (planes - ways[index]) % planes,
                )
            )

    near_half, far_half = range(planes // 2), range(planes // 2, planes)
    lend(near_half)
    send_shared(0)
    for copy in local[4:]:
        copy.wait()
    hidden_of(0, batches[0], 0)
    take_lent(near_half)
    hidden_of(1, batches[0], 0)
    for copy in own_copies[:3]:
        copy.wait()
    hidden_of(1, batches[0], 1)
    own_copies[3].wait()
    give(near_half, batches[0])
    lend(far_half[:2])
    hidden_of(0, batches[0], 1)
    finish(0, batches[0], kept_ref)
    lend(far_half[2:])
    send_shared(1)
    give_back(near_half)
    for step in range(2):
        chunks = far_half[2 * step : 2 * step + 2]
        part = slice(chunks[0] * group, (chunks[-1] + 1) * group)
        take_lent(chunks)
        hidden_of(1, part, 0)
        hidden_of(1, part, 1)
        give(chunks, part)
    send_shared(2)
    hidden_of(0, batches[1], 0)
    hidden_of(0, batches[1], 1)
    finish(0, batches[1], kept_ref)
    give_back(far_half)
    send_shared(3)
    for copy in sh_copies[:3]:
        copy.wait()
    send_shared(4)
    send_shared(5)
    back_ref[sp_me] = done_ref[sp_me]

    def split(hits):
        full = jnp.where(hits[0], weights[0], 0.0) + jnp.where(hits[1], weights[1], 0.0)
        high = full.astype(jnp.bfloat16)
        return [high, (full - high.astype(jnp.float32)).astype(jnp.bfloat16)]

    main_split = split(mains)
    sides = [
        jnp.concatenate(main_split + split([tail_hit(0, b), tail_hit(1, b)]), axis=0)
        for b in range(3)
    ]
    for copy in back_copies:
        copy.wait()
    tail = jnp.zeros((rows_out, quarter), jnp.float32)
    for b in range(3):
        block = back_ref[:, :, b * quarter : (b + 1) * quarter].reshape(sp_count * 8, quarter)
        value = jnp.dot(sides[b], block, preferred_element_type=jnp.float32)
        mixture_ref[:, b * quarter : (b + 1) * quarter] = (
            value[0:rows_out] + value[rows_out : 2 * rows_out]
        )
        tail = tail + value[2 * rows_out : 3 * rows_out] + value[3 * rows_out :]
    mixture_ref[:, 3 * quarter :] = tail

    pair_copy.wait()
    sh_copies[3].wait()
    sh_copies[4].wait()
    tokens = jnp.concatenate([normed_ref[...], pair_in[...]], axis=0)
    lane = iota((2 * rows_out, 2 * sd_rows), 1)
    units_of = []
    for slot in range(tp_count):
        both = jnp.dot(tokens, gu_w[slot], preferred_element_type=jnp.float32)
        units_of.append(jax.nn.silu(both) * pltpu.roll(both, sd_rows, 1))
    hidden = jnp.concatenate(
        [
            jnp.where(lane < sd_rows, units_of[s], pltpu.roll(units_of[s + 1], sd_rows, 1))
            for s in range(0, tp_count, 2)
        ],
        axis=1,
    ).astype(jnp.bfloat16)
    sh_copies[5].wait()
    part_out[...] = jnp.dot(
        hidden[rows_out:], sd_w[...], preferred_element_type=jnp.float32
    ).astype(jnp.bfloat16)
    part_copy = remote(part_out, part_in, pair_send.at[1], pair_recv.at[1], (pair, tp_me))
    mixture_ref[...] += jnp.dot(hidden[:rows_out], sd_w[...], preferred_element_type=jnp.float32)
    part_copy.wait()
    mixture = mixture_ref[...] + part_in[...].astype(jnp.float32)
    square = jnp.mean(mixture * mixture, axis=-1, keepdims=True)
    out_ref[...] = (
        resid_ref[...].astype(jnp.float32)
        + mixture * lax.rsqrt(square + EPS) * moe_gain_ref[...]
    ).astype(out_ref.dtype)


def fused(vmem_args, hbm_args):
    sp_count = lax.axis_size("sp")
    tp_count = lax.axis_size("tp")
    queries, values, stream = hbm_args[4], hbm_args[1], hbm_args[6]
    expert_gate, expert_down, shared_gate, shared_down = (hbm_args[i] for i in (8, 10, 11, 13))
    span, lanes = queries.shape
    width = values.shape[1]
    rows_out = span // tp_count
    blocks = span // BLK
    planes = sp_count // PLANE
    piece = DV // PLANE
    model = stream.shape[1]
    units = expert_gate.shape[2]
    vmem = pl.BlockSpec(memory_space=pltpu.VMEM)
    hbm = pl.BlockSpec(memory_space=pl.ANY)
    bf16, f32 = jnp.bfloat16, jnp.float32
    packets = pltpu.VMEM((sp_count, 8, 3 * model // 4), bf16)
    tokens = pltpu.VMEM(stream.shape, bf16)
    dma = pltpu.SemaphoreType.DMA
    return pl.pallas_call(
        functools.partial(fused_kernel, sp_count, tp_count),
        out_shape=jax.ShapeDtypeStruct(stream.shape, stream.dtype),
        in_specs=[vmem] * len(vmem_args) + [hbm] * len(hbm_args),
        out_specs=vmem,
        scratch_shapes=[
            pltpu.VMEM((span, width), bf16),
            pltpu.VMEM((tp_count, rows_out, width), bf16),
            pltpu.VMEM((span, width), f32),
            pltpu.VMEM((span, lanes), f32),
            pltpu.VMEM((blocks, width, lanes), f32),
            pltpu.VMEM((blocks, width, lanes), f32),
            pltpu.VMEM((PLANE, 2 * piece + 8, lanes), bf16),
            pltpu.VMEM((PLANE, 2 * piece + 8, lanes), bf16),
            pltpu.VMEM((2 * piece + 8, lanes), bf16),
            pltpu.VMEM((planes, 2 * piece + 8, lanes), bf16),
            pltpu.VMEM((PLANE, 2 * piece, lanes), bf16),
            pltpu.VMEM((PLANE, 2 * piece, lanes), bf16),
            pltpu.VMEM((tp_count * width, model), bf16),
            pltpu.VMEM((2, model, units), bf16),
            pltpu.VMEM((2, model, units), bf16),
            pltpu.VMEM((2 * units, model), bf16),
            pltpu.VMEM(shared_gate.shape, bf16),
            pltpu.VMEM(shared_gate.shape, bf16),
            pltpu.VMEM((tp_count,) + shared_gate.shape, bf16),
            pltpu.VMEM((tp_count * shared_down.shape[0] // 2, model), bf16),
            tokens,
            tokens,
            packets,
            packets,
            packets,
            pltpu.VMEM((2, sp_count * 8, model), bf16),
            pltpu.VMEM((2, sp_count * 8, 2 * units), bf16),
            packets,
            packets,
            packets,
            packets,
            packets,
            tokens,
            tokens,
            tokens,
            pltpu.VMEM(stream.shape, f32),
            pltpu.VMEM((blocks + BLK, lanes), f32),
            pltpu.VMEM((blocks + BLK, lanes), f32),
            pltpu.VMEM(queries.shape, bf16),
            pltpu.VMEM(values.shape, bf16),
            pltpu.VMEM(queries.shape, f32),
            pltpu.VMEM(queries.shape, f32),
            pltpu.VMEM(queries.shape, bf16),
            pltpu.VMEM(values.shape, bf16),
            tokens,
            dma((7,)),
            dma((7,)),
            dma((PLANE,)),
            dma((PLANE,)),
            dma((planes,)),
            dma((planes,)),
            dma((PLANE,)),
            dma((PLANE,)),
            dma((tp_count,)),
            dma((tp_count,)),
            dma((4,)),
            dma((4,)),
            dma((6,)),
            dma((6,)),
            dma((planes,)),
            dma((planes,)),
            dma((planes,)),
            dma((planes,)),
            dma((planes, PLANE)),
            dma((planes, PLANE)),
            dma((planes, PLANE)),
            dma((planes, PLANE)),
            dma((2,)),
            dma((2,)),
        ],
        compiler_params=pltpu.CompilerParams(
            collective_id=0, has_side_effects=True, vmem_limit_bytes=60 * 1024 * 1024
        ),
    )(*vmem_args, *hbm_args)


def body(
    stream,
    queries,
    key_rows,
    values,
    out_gate,
    fwd_decay,
    bwd_decay,
    head_gain,
    out_proj,
    mix_gain,
    ffn_gain,
    moe_gain,
    routes,
    route_weight,
    expert_gate,
    expert_up,
    expert_down,
    shared_gate,
    shared_up,
    shared_down,
):
    half = KEY_CHANNELS // 2
    rates = ROPE_BASE ** (-(np.arange(queries.shape[1]) % half) / half)
    return fused(
        (
            jnp.asarray(rates.astype(np.float32).reshape(1, -1)),
            head_gain.reshape(1, -1),
            mix_gain.reshape(1, -1),
            ffn_gain.reshape(1, -1),
            moe_gain.reshape(1, -1),
            routes.T,
            route_weight.T,
        ),
        (
            key_rows,
            values,
            fwd_decay,
            bwd_decay,
            queries,
            out_gate,
            stream,
            out_proj,
            expert_gate,
            expert_up,
            expert_down,
            shared_gate,
            shared_up,
            shared_down,
        ),
    )


def solution(mesh):
    return jax.shard_map(
        body,
        mesh=mesh,
        in_specs=(
            P(("sp", "tp"), None),
            P("sp", "tp"),
            P("sp", "tp"),
            P("sp", "tp"),
            P("sp", "tp"),
            P("sp", "tp"),
            P("sp", "tp"),
            P("tp"),
            P(),
            P(),
            P(),
            P(),
            P(("sp", "tp"), None),
            P(("sp", "tp"), None),
            P("sp", None, "tp"),
            P("sp", None, "tp"),
            P("sp", "tp", None),
            P(None, "tp"),
            P(None, "tp"),
            P("tp", None),
        ),
        out_specs=P(("sp", "tp"), None),
        check_vma=False,
    )
```

```python
import functools

import jax
import jax.numpy as jnp
import numpy as np
from jax import lax
from jax.experimental import pallas as pl
from jax.experimental.pallas import tpu as pltpu
from jax.sharding import PartitionSpec as P

KEY_CHANNELS = 64
DV = 128
BLK = 64
TOPK = 2
PLANE = 8


EPS = 1e-06
GATE_NORM = 16.0
ROPE_BASE = 10000.0
TOP_PRECISION = lax.Precision.HIGHEST
MESH = pl.DeviceIdType.MESH


def normalize(tensor):
    return tensor * lax.rsqrt(jnp.mean(tensor * tensor, axis=-1, keepdims=True) + EPS)


def dot_nt(left, right):
    return lax.dot_general(
        left, right, (((1,), (1,)), ((), ())), preferred_element_type=jnp.float32
    )


def dot_tn(left, right):
    return lax.dot_general(
        left, right, (((0,), (0,)), ((), ())), preferred_element_type=jnp.float32
    )


def fused_kernel(
    sp_count,
    tp_count,
    rate_ref,
    gain_ref,
    mix_gain_ref,
    ffn_gain_ref,
    moe_gain_ref,
    route_ref,
    weight_ref,
    k_hbm,
    v_hbm,
    fwd_hbm,
    bwd_hbm,
    q_hbm,
    gate_hbm,
    stream_hbm,
    proj_hbm,
    eg_hbm,
    eu_hbm,
    ed_hbm,
    sg_hbm,
    su_hbm,
    sd_hbm,
    out_ref,
    mixed_ref,
    land_ref,
    within_ref,
    key_ref,
    sums_f,
    sums_b,
    near_out,
    near_in,
    far_out,
    far_in,
    carry_out,
    carry_in,
    proj_w,
    gate_w,
    up_w,
    down_w,
    sg_ref,
    su_ref,
    gu_w,
    sd_w,
    resid_ref,
    normed_ref,
    outgoing_ref,
    arrived_ref,
    lent_ref,
    rows_ref,
    hidden_ref,
    lent_out,
    lent_back,
    kept_ref,
    done_ref,
    back_ref,
    pair_in,
    part_out,
    part_in,
    mixture_ref,
    cos_ref,
    sin_ref,
    k_ref,
    v_ref,
    fwd_ref,
    bwd_ref,
    q_ref,
    gate_ref,
    stream_ref,
    input_sem,
    local_sem,
    near_send,
    near_recv,
    far_send,
    far_recv,
    carry_send,
    carry_recv,
    row_send,
    row_recv,
    own_send,
    own_recv,
    sh_send,
    sh_recv,
    lend_send,
    lend_recv,
    give_send,
    give_recv,
    block_send,
    block_recv,
    back_send,
    back_recv,
    pair_send,
    pair_recv,
):
    span, lanes = q_ref.shape
    width = v_ref.shape[1]
    heads = lanes // KEY_CHANNELS
    blocks = span // BLK
    rows_out = span // tp_count
    planes = sp_count // PLANE
    piece = DV // PLANE
    model = stream_ref.shape[1]
    quarter = model // 4
    units = eg_hbm.shape[2]
    depth = eg_hbm.shape[1]
    sp_me = lax.axis_index("sp")
    tp_me = lax.axis_index("tp")
    z_me = sp_me // PLANE
    p_me = lax.rem(sp_me, PLANE)
    pair = sp_me + 1 - 2 * lax.rem(sp_me, 2)
    core = lax.rem(sp_me, 2)
    flip = tp_me + 1 - 2 * lax.rem(tp_me, 2)
    mirror = tp_count - 1 - tp_me
    holder = (sp_me, jnp.where(core == 0, flip, mirror))
    mate = (sp_me, jnp.where(core == 0, mirror, flip))
    ways = [0, planes // 2, 1, planes - 1]
    for step in range(planes // 2 - 1, 1, -1):
        ways += [step, planes - step]

    inputs = []
    for index, (source, target) in enumerate(
        (
            (k_hbm, k_ref),
            (v_hbm, v_ref),
            (fwd_hbm, fwd_ref),
            (bwd_hbm, bwd_ref),
            (q_hbm, q_ref),
            (gate_hbm, gate_ref),
            (stream_hbm, stream_ref),
        )
    ):
        copy = pltpu.make_async_copy(source, target, input_sem.at[index])
        copy.start()
        inputs.append(copy)

    barrier = pltpu.get_barrier_semaphore()
    for step in range(1, sp_count):
        pl.semaphore_signal(
            barrier,
            inc=1,
            device_id=(lax.rem(sp_me + step, sp_count), tp_me),
            device_id_type=MESH,
        )
    for step in range(1, tp_count):
        pl.semaphore_signal(
            barrier,
            inc=1,
            device_id=(sp_me, lax.rem(tp_me + step, tp_count)),
            device_id_type=MESH,
        )

    def remote(source, target, send, recv, device):
        copy = pltpu.make_async_remote_copy(
            src_ref=source,
            dst_ref=target,
            send_sem=send,
            recv_sem=recv,
            device_id=device,
            device_id_type=MESH,
        )
        copy.start()
        return copy

    sd_rows = sd_hbm.shape[0] // 2
    local = []
    for index, (source, target) in enumerate(
        (
            (sg_hbm, sg_ref),
            (su_hbm, su_ref),
            (
                sd_hbm.at[pl.ds(pl.multiple_of(core * sd_rows, sd_rows), sd_rows)],
                sd_w.at[pl.ds(0, sd_rows)],
            ),
            (proj_hbm, proj_w),
            (eg_hbm.at[0], gate_w.at[0]),
            (eu_hbm.at[0], up_w.at[0]),
            (ed_hbm.at[0], down_w.at[pl.ds(0, units)]),
        )
    ):
        copy = pltpu.make_async_copy(source, target, local_sem.at[index])
        copy.start()
        local.append(copy)

    row = lax.broadcasted_iota(jnp.int32, (BLK, BLK), 0)
    column = lax.broadcasted_iota(jnp.int32, (BLK, BLK), 1)
    lower = row >= column
    upper = row <= column
    lower_ones = lower.astype(jnp.float32)
    upper_ones = upper.astype(jnp.float32)
    from_lane = lax.broadcasted_iota(jnp.int32, (lanes, lanes), 0)
    to_lane = lax.broadcasted_iota(jnp.int32, (lanes, lanes), 1)
    half = KEY_CHANNELS // 2
    partner = jnp.where(lax.rem(to_lane, KEY_CHANNELS) < half, to_lane + half, to_lane - half)
    swap = (from_lane == partner).astype(jnp.bfloat16)
    own_head = (
        lax.broadcasted_iota(jnp.int32, (width, lanes), 0) // DV
        == lax.broadcasted_iota(jnp.int32, (width, lanes), 1) // KEY_CHANNELS
    )
    lane_head = lax.broadcasted_iota(jnp.int32, (BLK, lanes), 1) // KEY_CHANNELS

    lane_low = lax.rem(lax.broadcasted_iota(jnp.int32, (BLK, lanes), 1), KEY_CHANNELS) < half

    table = (blocks + BLK, lanes)
    place = lax.broadcasted_iota(jnp.int32, table, 0)
    position = jnp.where(place < blocks, sp_me * span + place * BLK, place - blocks)
    angles = position.astype(jnp.float32) * rate_ref[...]
    cos_ref[...] = jnp.cos(angles)
    sin_ref[...] = jnp.sin(angles)

    def rotated(tensor, block):
        swapped = jnp.dot(tensor, swap, preferred_element_type=jnp.float32)
        cos_block, sin_block = cos_ref[block : block + 1], sin_ref[block : block + 1]
        cos_row, sin_row = cos_ref[blocks : blocks + BLK], sin_ref[blocks : blocks + BLK]
        cosine = cos_block * cos_row - sin_block * sin_row
        sine = sin_block * cos_row + cos_block * sin_row
        return tensor.astype(jnp.float32) * cosine + swapped * jnp.where(lane_low, -sine, sine)

    for copy in inputs[:4]:
        copy.wait()
    cumul_f, cumul_b, decay_f, decay_b = [], [], [], []
    for block in range(blocks):
        rows = pl.ds(block * BLK, BLK)
        total_f = jnp.dot(
            lower_ones,
            jax.nn.log_sigmoid(fwd_ref[rows, :]) / GATE_NORM,
            precision=TOP_PRECISION,
            preferred_element_type=jnp.float32,
        )
        total_b = jnp.dot(
            upper_ones,
            jax.nn.log_sigmoid(bwd_ref[rows, :]) / GATE_NORM,
            precision=TOP_PRECISION,
            preferred_element_type=jnp.float32,
        )
        last_f = total_f[BLK - 1 : BLK]
        last_b = total_b[0:1]
        keys = rotated(k_ref[rows, :], block)
        key_ref[rows, :] = keys
        value_rows = v_ref[rows, :]
        out_f = (keys * jnp.exp(last_f - total_f)).astype(jnp.bfloat16)
        out_b = (keys * jnp.exp(last_b - total_b)).astype(jnp.bfloat16)
        sums_f[block] = jnp.where(own_head, dot_tn(value_rows, out_f), 0.0)
        sums_b[block] = jnp.where(own_head, dot_tn(value_rows, out_b), 0.0)
        cumul_f.append(total_f)
        cumul_b.append(total_b)
        decay_f.append(jnp.exp(last_f))
        decay_b.append(jnp.exp(last_b))

    local[0].wait()
    local[1].wait()
    local[2].wait()
    shared_low = lax.broadcasted_iota(jnp.int32, sg_ref.shape, 1) < sd_rows
    gate_rows = sg_ref[...].astype(jnp.float32)
    up_rows = su_ref[...].astype(jnp.float32)
    first = jnp.where(core == 0, gate_rows, pltpu.roll(gate_rows, sd_rows, 1))
    second = jnp.where(core == 0, pltpu.roll(up_rows, sd_rows, 1), up_rows)
    gu_w[0] = jnp.where(shared_low, first, second).astype(jnp.bfloat16)

    pl.semaphore_wait(barrier, sp_count - 1 + tp_count - 1)
    own_copies = []
    early = depth // 4

    def send_own(item):
        source, target = (
            (eg_hbm.at[0], gate_w.at[1]),
            (eu_hbm.at[0, pl.ds(0, early)], up_w.at[1, pl.ds(0, early)]),
            (eu_hbm.at[0, pl.ds(early, depth - early)], up_w.at[1, pl.ds(early, depth - early)]),
            (ed_hbm.at[0], down_w.at[pl.ds(units, units)]),
        )[item]
        own_copies.append(remote(source, target, own_send.at[item], own_recv.at[item], holder))

    send_own(0)
    send_own(1)
    sh_copies = []
    middle = depth // 2

    def send_shared(item):
        source, target, device = (
            (gu_w.at[0, pl.ds(0, middle)], gu_w.at[1, pl.ds(0, middle)], mate),
            (gu_w.at[0, pl.ds(middle, middle)], gu_w.at[1, pl.ds(middle, middle)], mate),
            (sd_w.at[pl.ds(0, sd_rows)], sd_w.at[pl.ds(sd_rows, sd_rows)], mate),
            (gu_w.at[0], gu_w.at[2], holder),
            (gu_w.at[1], gu_w.at[3], holder),
            (sd_w.at[pl.ds(0, 2 * sd_rows)], sd_w.at[pl.ds(2 * sd_rows, 2 * sd_rows)], holder),
        )[item]
        sh_copies.append(remote(source, target, sh_send.at[item], sh_recv.at[item], device))

    def packed(total):
        return sum(total[h * DV : (h + 1) * DV] for h in range(heads))

    total = sums_f[0]
    through_f = decay_f[0]
    for block in range(1, blocks):
        total = total * decay_f[block] + sums_f[block]
        through_f = through_f * decay_f[block]
    state_f = packed(total)
    total = sums_b[blocks - 1]
    through_b = decay_b[blocks - 1]
    for block in range(blocks - 2, -1, -1):
        total = total * decay_b[block] + sums_b[block]
        through_b = through_b * decay_b[block]
    state_b = packed(total)

    def put_state(ref, first, second, through_first, through_second):
        ref[0:piece] = first.astype(jnp.bfloat16)
        ref[piece : 2 * piece] = second.astype(jnp.bfloat16)
        high = [t.astype(jnp.bfloat16).astype(jnp.float32) for t in (through_first, through_second)]
        ref[2 * piece : 2 * piece + 8] = jnp.concatenate(
            [
                high[0],
                through_first - high[0],
                high[1],
                through_second - high[1],
                jnp.zeros((4, lanes), jnp.float32),
            ],
            axis=0,
        ).astype(jnp.bfloat16)

    def get_state(ref, index):
        block = ref[index].astype(jnp.float32)
        cut = 2 * piece
        return (
            block[0:piece],
            block[piece:cut],
            block[cut : cut + 1] + block[cut + 1 : cut + 2],
            block[cut + 2 : cut + 3] + block[cut + 3 : cut + 4],
        )

    for p in range(PLANE):
        cut = slice(p * piece, (p + 1) * piece)
        put_state(near_out.at[p], state_f[cut], state_b[cut], through_f, through_b)
    near_copies = []
    for step in range(1, PLANE):
        target = lax.rem(p_me + step, PLANE)
        near_copies.append(
            remote(
                near_out.at[target],
                near_in.at[p_me],
                near_send.at[step],
                near_recv.at[step],
                (z_me * PLANE + target, tp_me),
            )
        )
    near_in[p_me] = near_out[p_me]

    query_f, query_b = [], []

    def within(block):
        rows = pl.ds(block * BLK, BLK)
        queries = rotated(q_ref[rows, :], block) * KEY_CHANNELS ** (-0.5)
        keys = key_ref[rows, :]
        total_f, total_b = cumul_f[block], cumul_b[block]
        middle_f = total_f[BLK // 2 - 1 : BLK // 2]
        middle_b = total_b[BLK // 2 : BLK // 2 + 1]
        scaled_qf = queries * jnp.exp(total_f - middle_f)
        scaled_qb = queries * jnp.exp(total_b - middle_b)
        scaled_kf = (keys * jnp.exp(middle_f - total_f)).astype(jnp.bfloat16)
        scaled_kb = (keys * jnp.exp(middle_b - total_b)).astype(jnp.bfloat16)
        query_f.append((queries * jnp.exp(total_f)).astype(jnp.bfloat16))
        query_b.append((queries * jnp.exp(total_b)).astype(jnp.bfloat16))
        for h in range(heads):
            mine = lane_head == h
            scores_f = dot_nt(jnp.where(mine, scaled_qf, 0.0).astype(jnp.bfloat16), scaled_kf)
            scores_b = dot_nt(jnp.where(mine, scaled_qb, 0.0).astype(jnp.bfloat16), scaled_kb)
            scores = jnp.where(lower, scores_f, 0.0) + jnp.where(upper, scores_b, 0.0)
            within_ref[rows, h * DV : (h + 1) * DV] = jnp.dot(
                scores.astype(jnp.bfloat16),
                v_ref[rows, h * DV : (h + 1) * DV],
                preferred_element_type=jnp.float32,
            )

    for copy in inputs[4:]:
        copy.wait()
    third = blocks // 3
    for block in range(third):
        within(block)
    for copy in near_copies:
        copy.wait()

    def fold(orders, visit):
        state = jnp.zeros((piece, lanes), jnp.float32)
        through = jnp.ones((1, lanes), jnp.float32)
        first = orders[0] == 0
        for p in orders:
            visit(p, state, through)
            fwd_state, bwd_state, fwd_through, bwd_through = get_state(near_in, p)
            state = state * (fwd_through if first else bwd_through) + (
                fwd_state if first else bwd_state
            )
            through = through * (fwd_through if first else bwd_through)
        return state, through

    ahead = list(range(PLANE))
    behind = ahead[::-1]
    plane_f, plane_df = fold(ahead, lambda p, state, through: None)
    plane_b, plane_db = fold(behind, lambda p, state, through: None)
    put_state(far_out, plane_f, plane_b, plane_df, plane_db)
    far_copies = []
    for step in range(1, planes):
        target = lax.rem(z_me + step, planes)
        far_copies.append(
            remote(
                far_out,
                far_in.at[z_me],
                far_send.at[step],
                far_recv.at[step],
                (target * PLANE + p_me, tp_me),
            )
        )
    far_in[z_me] = far_out[...]
    for block in range(third, blocks - third):
        within(block)
    for copy in far_copies:
        copy.wait()
    enter_f = jnp.zeros((piece, lanes), jnp.float32)
    enter_b = jnp.zeros((piece, lanes), jnp.float32)
    for z in range(planes):
        plane_state, _, plane_through, _ = get_state(far_in, z)
        enter_f = jnp.where(z < z_me, enter_f * plane_through + plane_state, enter_f)
    for z in range(planes - 1, -1, -1):
        _, plane_state, _, plane_through = get_state(far_in, z)
        enter_b = jnp.where(z > z_me, enter_b * plane_through + plane_state, enter_b)

    def emit_f(p, state, through):
        carry_out[p, 0:piece] = (enter_f * through + state).astype(jnp.bfloat16)

    def emit_b(p, state, through):
        carry_out[p, piece : 2 * piece] = (enter_b * through + state).astype(jnp.bfloat16)

    fold(ahead, emit_f)
    fold(behind, emit_b)
    carry_copies = []
    for step in range(1, PLANE):
        target = lax.rem(p_me + step, PLANE)
        carry_copies.append(
            remote(
                carry_out.at[target],
                carry_in.at[p_me],
                carry_send.at[step],
                carry_recv.at[step],
                (z_me * PLANE + target, tp_me),
            )
        )
    carry_in[p_me] = carry_out[p_me]
    for block in range(blocks - third, blocks):
        within(block)
    for copy in carry_copies:
        copy.wait()

    def unpacked(first):
        carry = jnp.concatenate(
            [carry_in[p, first : first + piece].astype(jnp.float32) for p in range(PLANE)], axis=0
        )
        return jnp.where(own_head, jnp.concatenate([carry] * heads, axis=0), 0.0)

    state = unpacked(0)
    for block in range(blocks):
        rows = pl.ds(block * BLK, BLK)
        within_ref[rows, :] += dot_nt(query_f[block], state.astype(jnp.bfloat16))
        if block < blocks - 1:
            state = state * decay_f[block] + sums_f[block]
    state = unpacked(piece)
    for block in range(blocks - 1, -1, -1):
        rows = pl.ds(block * BLK, BLK)
        attended = within_ref[rows, :] + dot_nt(query_b[block], state.astype(jnp.bfloat16))
        if block > 0:
            state = state * decay_b[block] + sums_b[block]
        for h in range(heads):
            part = attended[:, h * DV : (h + 1) * DV]
            square = jnp.mean(part * part, axis=-1, keepdims=True)
            gate = gate_ref[rows, h * DV : (h + 1) * DV].astype(jnp.float32)
            mixed_ref[rows, h * DV : (h + 1) * DV] = (
                part
                * lax.rsqrt(square + EPS)
                * gain_ref[:, h * DV : (h + 1) * DV]
                * (gate / (1.0 + jnp.exp(-gate)))
            ).astype(jnp.bfloat16)

    row_copies = []
    for step in (2, 1, 3):
        target = lax.rem(tp_me + step, tp_count)
        row_copies.append(
            remote(
                mixed_ref.at[pl.ds(pl.multiple_of(target * rows_out, rows_out), rows_out)],
                land_ref.at[tp_me],
                row_send.at[step],
                row_recv.at[step],
                (sp_me, target),
            )
        )
    send_own(2)
    send_own(3)
    land_ref[tp_me] = mixed_ref[pl.ds(pl.multiple_of(tp_me * rows_out, rows_out), rows_out), :]

    def iota(shape, axis):
        return lax.broadcasted_iota(jnp.int32, shape, axis)

    square_shape = (rows_out, rows_out)
    eye = (iota(square_shape, 0) == iota(square_shape, 1)).astype(jnp.float32)
    columns = lax.dot_general(
        eye,
        jnp.concatenate(
            [
                route_ref[...].astype(jnp.float32),
                weight_ref[...],
                jnp.zeros((8 - 2 * TOPK, rows_out), jnp.float32),
            ],
            axis=0,
        ),
        (((1,), (1,)), ((), ())),
        precision=TOP_PRECISION,
        preferred_element_type=jnp.float32,
    )
    named = [columns[:, k : k + 1] for k in range(TOPK)]
    weights = [columns[:, TOPK + k : TOPK + k + 1] for k in range(TOPK)]
    expert_lane = iota((rows_out, 128), 1).astype(jnp.float32)
    onehot = [(named[k] == expert_lane).astype(jnp.float32) for k in range(TOPK)]
    earlier = (iota(square_shape, 0) > iota(square_shape, 1)).astype(jnp.bfloat16)
    every = jnp.ones(square_shape, jnp.bfloat16)
    slot_lane = iota((rows_out, sp_count * 8), 1).astype(jnp.float32)
    seen = jnp.zeros((rows_out, 128), jnp.float32)
    mains, tails, thirds = [], [], []
    for k in range(TOPK):
        hot = onehot[k].astype(jnp.bfloat16)
        before = seen + jnp.dot(earlier, hot, preferred_element_type=jnp.float32)
        seen = seen + jnp.dot(every, hot, preferred_element_type=jnp.float32)
        rank = jnp.sum(before * onehot[k], axis=1, keepdims=True)
        over = jnp.where(rank >= 3.0, 1.0, 0.0)
        mains.append(named[k] * 8.0 + rank == slot_lane)
        tails.append(named[k] * 8.0 + 6.0 + over == slot_lane)
        thirds.append(rank - 3.0 * over)

    def tail_hit(k, b):
        return jnp.logical_and(tails[k], thirds[k] == b)

    def chosen(first, second):
        return jnp.where(jnp.logical_or(first, second), 1.0, 0.0).astype(jnp.bfloat16)

    local[3].wait()
    for copy in row_copies:
        copy.wait()
    mixed_all = jnp.concatenate([land_ref[source] for source in range(tp_count)], axis=1)
    projected = jnp.dot(mixed_all, proj_w[...], preferred_element_type=jnp.float32)
    residual = (
        stream_ref[...].astype(jnp.float32) + normalize(projected) * mix_gain_ref[...]
    ).astype(jnp.bfloat16)
    resid_ref[...] = residual
    normed = (normalize(residual.astype(jnp.float32)) * ffn_gain_ref[...]).astype(jnp.bfloat16)
    normed_ref[...] = normed
    pick_main = chosen(mains[0], mains[1])
    for b in range(3):
        picks = jnp.concatenate([pick_main, chosen(tail_hit(0, b), tail_hit(1, b))], axis=0)
        source = jnp.concatenate(
            [normed[:, b * quarter : (b + 1) * quarter], normed[:, 3 * quarter :]], axis=0
        )
        outgoing_ref[:, :, b * quarter : (b + 1) * quarter] = (
            dot_tn(picks, source).reshape(sp_count, 8, quarter).astype(jnp.bfloat16)
        )
    def exchange(source_ref, source_of, target_ref, send, recv, way):
        copies = []
        for turn in range(PLANE):
            if way == 0 and turn == 0:
                continue
            target = lax.rem(z_me + way, planes) * PLANE + lax.rem(p_me + turn, PLANE)
            copies.append(
                remote(
                    source_ref.at[source_of(target)],
                    target_ref.at[sp_me],
                    send.at[way, turn],
                    recv.at[way, turn],
                    (target, tp_me),
                )
            )
        return copies

    block_copies = [
        exchange(outgoing_ref, lambda target: target, arrived_ref, block_send, block_recv, way)
        for way in ways
    ]
    arrived_ref[sp_me] = outgoing_ref[sp_me]
    pair_copy = remote(normed_ref, pair_in, pair_send.at[0], pair_recv.at[0], (pair, tp_me))

    group = PLANE * 8
    spot = iota((group, group), 0)
    origin = iota((group, group), 1)
    same = spot // 8 == origin // 8

    def spread(target, source, b):
        rank = lax.rem(target, 8)
        hit = jnp.logical_and(rank < 6, lax.rem(rank, 3) == b)
        hit = jnp.logical_and(hit, lax.rem(source, 8) == 6 + rank // 3)
        return jnp.where(jnp.logical_and(same, hit), 1.0, 0.0).astype(jnp.bfloat16)

    scatter = [spread(spot, origin, b) for b in range(3)]
    gather = [spread(origin, spot, b) for b in range(3)]

    def sources(index):
        plane = lax.rem(z_me + planes - ways[index], planes)
        return pl.ds(pl.multiple_of(plane * PLANE, PLANE), PLANE)

    def unpack(ref, side, index):
        cut = slice(index * group, (index + 1) * group)
        tail = jnp.zeros((group, quarter), jnp.float32)
        for b in range(3):
            block = ref[sources(index), :, b * quarter : (b + 1) * quarter].reshape(group, quarter)
            rows_ref[side, cut, b * quarter : (b + 1) * quarter] = block
            tail = tail + jnp.dot(scatter[b], block, preferred_element_type=jnp.float32)
        rows_ref[side, cut, 3 * quarter :] = tail.astype(jnp.bfloat16)

    total_rows = sp_count * 8

    def hidden_of(side, part, shard):
        rows = rows_ref[side, part]
        hidden_ref[side, part, shard * units : (shard + 1) * units] = (
            jax.nn.silu(jnp.dot(rows, gate_w[shard], preferred_element_type=jnp.float32))
            * jnp.dot(rows, up_w[shard], preferred_element_type=jnp.float32)
        ).astype(jnp.bfloat16)

    def finish(side, part, target_ref):
        count = part.stop - part.start
        hidden = hidden_ref[side, part]
        keep = lax.rem(iota((count, quarter), 0), 8) < 6
        last = jnp.dot(
            hidden, down_w[:, 3 * quarter :], preferred_element_type=jnp.float32
        ).astype(jnp.bfloat16)
        for b in range(3):
            value = jnp.dot(
                hidden,
                down_w[:, b * quarter : (b + 1) * quarter],
                preferred_element_type=jnp.float32,
            )
            moved = jnp.concatenate(
                [
                    jnp.dot(
                        gather[b], last[start : start + group], preferred_element_type=jnp.float32
                    )
                    for start in range(0, count, group)
                ],
                axis=0,
            )
            target_ref[part.start // 8 : part.stop // 8, :, b * quarter : (b + 1) * quarter] = (
                jnp.where(keep, value, moved).reshape(count // 8, 8, quarter).astype(jnp.bfloat16)
            )

    back_copies, lend_copies, give_copies = [], [], []
    batches = [slice(0, total_rows // 2), slice(total_rows // 2, total_rows)]

    def lend(chunks):
        for index in chunks:
            for copy in block_copies[index]:
                copy.wait()
            lend_copies.append(
                remote(
                    arrived_ref.at[sources(index)],
                    lent_ref.at[sources(index)],
                    lend_send.at[index],
                    lend_recv.at[index],
                    mate,
                )
            )
            unpack(arrived_ref, 0, index)

    def take_lent(chunks):
        for index in chunks:
            lend_copies[index].wait()
            unpack(lent_ref, 1, index)

    def give(chunks, part):
        finish(1, part, lent_out)
        for index in chunks:
            cut = pl.ds(index * PLANE, PLANE)
            give_copies.append(
                remote(
                    lent_out.at[cut],
                    lent_back.at[cut],
                    give_send.at[index],
                    give_recv.at[index],
                    mate,
                )
            )

    def give_back(chunks):
        for index in chunks:
            cut = slice(index * PLANE, (index + 1) * PLANE)
            give_copies[index].wait()
            done_ref[sources(index)] = (
                kept_ref[cut].astype(jnp.float32) + lent_back[cut].astype(jnp.float32)
            ).astype(jnp.bfloat16)
            back_copies.extend(
                exchange(
                    done_ref,
                    lambda target: target,
                    back_ref,
                    back_send,
                    back_recv,
                    (planes - ways[index]) % planes,
                )
            )

    near_half, far_half = range(planes // 2), range(planes // 2, planes)
    lend(near_half)
    send_shared(0)
    for copy in local[4:]:
        copy.wait()
    hidden_of(0, batches[0], 0)
    take_lent(near_half)
    hidden_of(1, batches[0], 0)
    for copy in own_copies[:3]:
        copy.wait()
    hidden_of(1, batches[0], 1)
    own_copies[3].wait()
    give(near_half, batches[0])
    lend(far_half[:2])
    hidden_of(0, batches[0], 1)
    finish(0, batches[0], kept_ref)
    lend(far_half[2:])
    send_shared(1)
    give_back(near_half)
    for step in range(2):
        chunks = far_half[2 * step : 2 * step + 2]
        part = slice(chunks[0] * group, (chunks[-1] + 1) * group)
        take_lent(chunks)
        hidden_of(1, part, 0)
        hidden_of(1, part, 1)
        give(chunks, part)
    send_shared(2)
    hidden_of(0, batches[1], 0)
    hidden_of(0, batches[1], 1)
    finish(0, batches[1], kept_ref)
    give_back(far_half)
    send_shared(3)
    for copy in sh_copies[:2]:
        copy.wait()
    send_shared(4)
    sh_copies[2].wait()
    send_shared(5)
    back_ref[sp_me] = done_ref[sp_me]

    def split(hits):
        full = jnp.where(hits[0], weights[0], 0.0) + jnp.where(hits[1], weights[1], 0.0)
        high = full.astype(jnp.bfloat16)
        return [high, (full - high.astype(jnp.float32)).astype(jnp.bfloat16)]

    main_split = split(mains)
    sides = [
        jnp.concatenate(main_split + split([tail_hit(0, b), tail_hit(1, b)]), axis=0)
        for b in range(3)
    ]
    for copy in back_copies:
        copy.wait()
    tail = jnp.zeros((rows_out, quarter), jnp.float32)
    for b in range(3):
        block = back_ref[:, :, b * quarter : (b + 1) * quarter].reshape(sp_count * 8, quarter)
        value = jnp.dot(sides[b], block, preferred_element_type=jnp.float32)
        mixture_ref[:, b * quarter : (b + 1) * quarter] = (
            value[0:rows_out] + value[rows_out : 2 * rows_out]
        )
        tail = tail + value[2 * rows_out : 3 * rows_out] + value[3 * rows_out :]
    mixture_ref[:, 3 * quarter :] = tail

    pair_copy.wait()
    sh_copies[3].wait()
    sh_copies[4].wait()
    tokens = jnp.concatenate([normed_ref[...], pair_in[...]], axis=0)
    lane = iota((2 * rows_out, 2 * sd_rows), 1)
    units_of = []
    for slot in range(tp_count):
        both = jnp.dot(tokens, gu_w[slot], preferred_element_type=jnp.float32)
        units_of.append(jax.nn.silu(both) * pltpu.roll(both, sd_rows, 1))
    hidden = jnp.concatenate(
        [
            jnp.where(lane < sd_rows, units_of[s], pltpu.roll(units_of[s + 1], sd_rows, 1))
            for s in range(0, tp_count, 2)
        ],
        axis=1,
    ).astype(jnp.bfloat16)
    sh_copies[5].wait()
    part_out[...] = jnp.dot(
        hidden[rows_out:], sd_w[...], preferred_element_type=jnp.float32
    ).astype(jnp.bfloat16)
    part_copy = remote(part_out, part_in, pair_send.at[1], pair_recv.at[1], (pair, tp_me))
    mixture_ref[...] += jnp.dot(hidden[:rows_out], sd_w[...], preferred_element_type=jnp.float32)
    part_copy.wait()
    mixture = mixture_ref[...] + part_in[...].astype(jnp.float32)
    square = jnp.mean(mixture * mixture, axis=-1, keepdims=True)
    out_ref[...] = (
        resid_ref[...].astype(jnp.float32)
        + mixture * lax.rsqrt(square + EPS) * moe_gain_ref[...]
    ).astype(out_ref.dtype)


def fused(vmem_args, hbm_args):
    sp_count = lax.axis_size("sp")
    tp_count = lax.axis_size("tp")
    queries, values, stream = hbm_args[4], hbm_args[1], hbm_args[6]
    expert_gate, expert_down, shared_gate, shared_down = (hbm_args[i] for i in (8, 10, 11, 13))
    span, lanes = queries.shape
    width = values.shape[1]
    rows_out = span // tp_count
    blocks = span // BLK
    planes = sp_count // PLANE
    piece = DV // PLANE
    model = stream.shape[1]
    units = expert_gate.shape[2]
    vmem = pl.BlockSpec(memory_space=pltpu.VMEM)
    hbm = pl.BlockSpec(memory_space=pl.ANY)
    bf16, f32 = jnp.bfloat16, jnp.float32
    packets = pltpu.VMEM((sp_count, 8, 3 * model // 4), bf16)
    tokens = pltpu.VMEM(stream.shape, bf16)
    dma = pltpu.SemaphoreType.DMA
    return pl.pallas_call(
        functools.partial(fused_kernel, sp_count, tp_count),
        out_shape=jax.ShapeDtypeStruct(stream.shape, stream.dtype),
        in_specs=[vmem] * len(vmem_args) + [hbm] * len(hbm_args),
        out_specs=vmem,
        scratch_shapes=[
            pltpu.VMEM((span, width), bf16),
            pltpu.VMEM((tp_count, rows_out, width), bf16),
            pltpu.VMEM((span, width), f32),
            pltpu.VMEM((span, lanes), f32),
            pltpu.VMEM((blocks, width, lanes), f32),
            pltpu.VMEM((blocks, width, lanes), f32),
            pltpu.VMEM((PLANE, 2 * piece + 8, lanes), bf16),
            pltpu.VMEM((PLANE, 2 * piece + 8, lanes), bf16),
            pltpu.VMEM((2 * piece + 8, lanes), bf16),
            pltpu.VMEM((planes, 2 * piece + 8, lanes), bf16),
            pltpu.VMEM((PLANE, 2 * piece, lanes), bf16),
            pltpu.VMEM((PLANE, 2 * piece, lanes), bf16),
            pltpu.VMEM((tp_count * width, model), bf16),
            pltpu.VMEM((2, model, units), bf16),
            pltpu.VMEM((2, model, units), bf16),
            pltpu.VMEM((2 * units, model), bf16),
            pltpu.VMEM(shared_gate.shape, bf16),
            pltpu.VMEM(shared_gate.shape, bf16),
            pltpu.VMEM((tp_count,) + shared_gate.shape, bf16),
            pltpu.VMEM((tp_count * shared_down.shape[0] // 2, model), bf16),
            tokens,
            tokens,
            packets,
            packets,
            packets,
            pltpu.VMEM((2, sp_count * 8, model), bf16),
            pltpu.VMEM((2, sp_count * 8, 2 * units), bf16),
            packets,
            packets,
            packets,
            packets,
            packets,
            tokens,
            tokens,
            tokens,
            pltpu.VMEM(stream.shape, f32),
            pltpu.VMEM((blocks + BLK, lanes), f32),
            pltpu.VMEM((blocks + BLK, lanes), f32),
            pltpu.VMEM(queries.shape, bf16),
            pltpu.VMEM(values.shape, bf16),
            pltpu.VMEM(queries.shape, f32),
            pltpu.VMEM(queries.shape, f32),
            pltpu.VMEM(queries.shape, bf16),
            pltpu.VMEM(values.shape, bf16),
            tokens,
            dma((7,)),
            dma((7,)),
            dma((PLANE,)),
            dma((PLANE,)),
            dma((planes,)),
            dma((planes,)),
            dma((PLANE,)),
            dma((PLANE,)),
            dma((tp_count,)),
            dma((tp_count,)),
            dma((4,)),
            dma((4,)),
            dma((6,)),
            dma((6,)),
            dma((planes,)),
            dma((planes,)),
            dma((planes,)),
            dma((planes,)),
            dma((planes, PLANE)),
            dma((planes, PLANE)),
            dma((planes, PLANE)),
            dma((planes, PLANE)),
            dma((2,)),
            dma((2,)),
        ],
        compiler_params=pltpu.CompilerParams(
            collective_id=0, has_side_effects=True, vmem_limit_bytes=60 * 1024 * 1024
        ),
    )(*vmem_args, *hbm_args)


def body(
    stream,
    queries,
    key_rows,
    values,
    out_gate,
    fwd_decay,
    bwd_decay,
    head_gain,
    out_proj,
    mix_gain,
    ffn_gain,
    moe_gain,
    routes,
    route_weight,
    expert_gate,
    expert_up,
    expert_down,
    shared_gate,
    shared_up,
    shared_down,
):
    half = KEY_CHANNELS // 2
    rates = ROPE_BASE ** (-(np.arange(queries.shape[1]) % half) / half)
    return fused(
        (
            jnp.asarray(rates.astype(np.float32).reshape(1, -1)),
            head_gain.reshape(1, -1),
            mix_gain.reshape(1, -1),
            ffn_gain.reshape(1, -1),
            moe_gain.reshape(1, -1),
            routes.T,
            route_weight.T,
        ),
        (
            key_rows,
            values,
            fwd_decay,
            bwd_decay,
            queries,
            out_gate,
            stream,
            out_proj,
            expert_gate,
            expert_up,
            expert_down,
            shared_gate,
            shared_up,
            shared_down,
        ),
    )


def solution(mesh):
    return jax.shard_map(
        body,
        mesh=mesh,
        in_specs=(
            P(("sp", "tp"), None),
            P("sp", "tp"),
            P("sp", "tp"),
            P("sp", "tp"),
            P("sp", "tp"),
            P("sp", "tp"),
            P("sp", "tp"),
            P("tp"),
            P(),
            P(),
            P(),
            P(),
            P(("sp", "tp"), None),
            P(("sp", "tp"), None),
            P("sp", None, "tp"),
            P("sp", None, "tp"),
            P("sp", "tp", None),
            P(None, "tp"),
            P(None, "tp"),
            P("tp", None),
        ),
        out_specs=P(("sp", "tp"), None),
        check_vma=False,
    )
```
